32 devices in a mesh: sp: 8 (over z, x), tp: 4 (over y, core).
Axes of the slice: x: 2, y: 2, z: 4, core: 2. Of those that a mesh axis runs over, the one named last changes fastest.
Arguments:
- cotangent: bfloat16 [1024, 2048], P('sp'), may hold values from -6 to 6
- mixer_out: bfloat16 [1024, 2048], P('sp'), may hold values from -6 to 6
- expert_ids: int32 [1024, 2], P('sp'), may hold values from 0 to 7, all different within a row; in each aligned block of 128 rows (0 to 127, 128 to 255, ...) at most 64 rows name the same one
- route_weight: float32 [1024, 2], P('sp'), may hold values from 0.3 to 1.5
- saved_normalized: bfloat16 [1024, 2048], P('sp', 'tp'), may hold values from -6 to 6
- inverse_deviation: float32 [1024], P('sp'), may hold values from 0.3 to 3
- channel_norm_gain: float32 [2048], P('tp'), may hold values from 0.1 to 1.9
- taps: float32 [31, 2048], P(None, 'tp'), may hold values from -1 to 1
- proj_weight: bfloat16 [2048, 2048], P('tp'), may hold values from -0.125 to 0.125
- gate_weight: bfloat16 [8, 2048, 2048], P('sp', None, 'tp'), may hold values from -0.125 to 0.125
- up_weight: bfloat16 [8, 2048, 2048], P('sp', None, 'tp'), may hold values from -0.125 to 0.125
- down_weight: bfloat16 [8, 2048, 2048], P('sp', 'tp'), may hold values from -0.125 to 0.125
Outputs:
- grad_mixer_in: bfloat16 [1024, 2048], P('sp', 'tp')
- grad_proj: float32 [2048, 2048], P('sp', 'tp')
- grad_gate: bfloat16 [8, 2048, 2048], P('sp', None, 'tp')
- grad_up: bfloat16 [8, 2048, 2048], P('sp', None, 'tp')
- grad_down: bfloat16 [8, 2048, 2048], P('sp', 'tp')
The draws below stay inside these ranges and needn't reach their ends.
Inputs may be any that keep to these rules, and one draw needn't show every extreme that they name: `expert_ids`: each row names 2 different experts. Within the rows of one index of sp no expert is named more than 64 times, a bound that some block reaches.
All inputs are finite; a program needn't handle non-finite values.
Results may differ from the reference program's by a relative error of at most 0.02.
Values may be sent and summed in bfloat16 or wider, within the bound.
A program may use at most 64 MiB of HBM per device.

```python
import math
import jax
import jax.numpy as jnp
import numpy as np
from jax import lax

D = 2048
CHANNELS = 2048
EXPERT_FF = 2048
WIDTH = 31
TOPK = 2
TOK_DEV = 128
TOKENS = 1024
EXPERTS = 8
CAP = 64
FFD = 512
N_SP = 8
N_TP = 4


def spiked(drawn, own_key, source, target, blocks, factor):
    def block_of(dim):
        return (jnp.arange(drawn.shape[dim]) // (drawn.shape[dim] // blocks)).reshape((-1,) + (1,) * (drawn.ndim - 1 - dim))

    near = jax.random.permutation(own_key, blocks)[block_of(target)]
    second = (block_of(target) + blocks // 2) % blocks
    return jnp.where((block_of(source) == near) | (block_of(source) == second), factor * drawn, drawn)


def block_scale(rng, extent, split, smallest, high):
    def one(axis_at, blocks):
        draws = jax.random.uniform(jax.random.fold_in(jax.random.fold_in(rng, 6), axis_at), (blocks,), jnp.float32, smallest / len(split), high / len(split))
        return jnp.repeat(jnp.exp(draws), extent[axis_at] // blocks).reshape((-1,) + (1,) * (len(extent) - axis_at - 1))

    loudness = one(*split[0])
    for cut in split[1:]:
        loudness = loudness * one(*cut)
    return loudness


def deal_out(stream_key, own, number, rows, amount, top, reach, skew):
    sequence = jax.random.permutation(stream_key, amount)
    crowded, usual = portions_of(amount, rows * top, reach, skew, True), portions_of(amount, rows * top, reach, skew, False)
    places = jnp.arange(amount)

    def named(lengths, offset_by):
        used = int((lengths > 0).sum())
        fixed = max(1, used // 4)
        shifted = fixed + (places - fixed + offset_by * (used - fixed)) % max(1, amount - fixed)
        return jnp.zeros((amount,), jnp.int32).at[sequence[jnp.where(places < fixed, places, shifted)]].set(jnp.asarray(lengths, jnp.int32))

    lengths = jnp.where(number % 4 == 0, named(crowded, number // 4), named(usual, number - number // 4 - 1))
    mixed = jax.random.permutation(jax.random.fold_in(own, 3), amount)
    donor, taker = mixed[0:amount // 2 * 2:2], mixed[1:amount // 2 * 2:2]
    slack = jnp.minimum(lengths[donor] - 1, reach - lengths[taker]) // 2
    slack = jnp.where((donor == sequence[0]) | (taker == sequence[0]) | (lengths[taker] == 0), 0, jnp.maximum(slack, 0))
    shifted = jax.random.randint(jax.random.fold_in(own, 4), (amount // 2,), 0, 1 << 20) % (slack + 1)
    lengths = lengths.at[donor].add(-shifted).at[taker].add(shifted)
    members = jnp.searchsorted(jnp.cumsum(lengths), jnp.arange(rows * top), side="right").astype(jnp.int32)
    table = members.reshape(top, rows).T
    table = table[jax.random.permutation(jax.random.fold_in(own, 1), rows)]
    offset_by = jax.random.randint(jax.random.fold_in(own, 2), (rows, 1), 0, top)
    return jnp.take_along_axis(table, (jnp.arange(top)[None, :] + offset_by) % top, axis=1)


def portions_of(count, total, limit, lean, full):
    loads = [(1 << 20) // math.isqrt(standing ** lean) + 1 for standing in range(1, count + 1)]
    largest = limit if full else min(limit, max(-(-total // count), total * loads[0] // sum(loads)))
    least = 1 if total - largest >= count - 1 else 0
    holding, surplus = [largest] + [least] * (count - 1), total - largest - least * (count - 1)
    while surplus > 0:
        movable = [i for i in range(1, count) if holding[i] < largest] or [i for i in range(1, count) if holding[i] < limit]
        whole, remaining = sum([loads[i] for i in movable]), surplus
        for i in movable:
            extra = min(limit - holding[i], max(1, remaining * loads[i] // whole), surplus)
            holding[i] = holding[i] + extra
            surplus = surplus - extra
    return np.array(holding)


def gaussian(stream_key, shape, deviation, limit, shards=(), kind=jnp.bfloat16):
    result = jax.random.normal(stream_key, shape, jnp.float32) * deviation
    if len(shards) > 0:
        result = block_scale(stream_key, shape, shards, -0.22, 0.18) * result
    return jnp.clip(result, min=-limit, max=limit).astype(kind)


def heavy_noise(key, extent, width, limit, shards, heavy, held_as=jnp.bfloat16):
    result = width * jax.random.normal(key, extent, jnp.float32)
    if shards:
        result = result * block_scale(key, extent, shards, -0.22, 0.18)
    return jnp.clip(spiked(result, jax.random.fold_in(key, 3), *heavy), -limit, limit).astype(held_as)


def setup_inputs(seed: int = 0) -> dict:
    arg_keys = jax.random.split(jax.random.key(seed), 13)
    cotangent = heavy_noise(arg_keys[0], (TOKENS, D), 1.0, 6.0, ((0, 8),), (0, 1, 8, 2.0))
    mixer_out = gaussian(arg_keys[1], (TOKENS, D), 1.0, 6.0, ((0, 8),))
    expert_ids_keys = jax.random.split(jax.random.fold_in(arg_keys[2], 1), TOKENS // TOK_DEV)
    expert_ids_turns = jax.random.permutation(jax.random.fold_in(arg_keys[2], 3), TOKENS // TOK_DEV)
    expert_ids = jax.vmap(lambda own, number: deal_out(jax.random.fold_in(arg_keys[2], 2), own, number, TOK_DEV, EXPERTS, TOPK, CAP, 1))(expert_ids_keys, expert_ids_turns).reshape((TOKENS, TOPK))
    route_weight = jnp.clip(0.3 + 1.2 * jax.random.uniform(arg_keys[3], (TOKENS, TOPK), jnp.float32) ** block_scale(arg_keys[3], (TOKENS, TOPK), ((0, 8),), -0.2, 0.2), 0.3, 1.5)
    saved_normalized = gaussian(arg_keys[4], (TOKENS, CHANNELS), 1.0, 6.0, ((0, 8), (1, 4)))
    inverse_deviation = jnp.clip(jnp.exp(math.log(3.0) - 2.3025851 * jax.random.uniform(arg_keys[5], (TOKENS,), jnp.float32) ** block_scale(arg_keys[5], (TOKENS,), ((0, 8),), -0.2, 0.2)), 0.3, 3.0)
    channel_norm_gain = jnp.clip(1.0 + 0.18 * jax.random.normal(arg_keys[6], (CHANNELS,), jnp.float32), 0.1, 1.9)
    taps = gaussian(arg_keys[7], (WIDTH, CHANNELS), 0.18, 1.0, ((1, 4),), jnp.float32)
    proj_weight = gaussian(arg_keys[8], (CHANNELS, D), CHANNELS ** -0.5, 0.125, ((0, 4),))
    gate_weight = gaussian(arg_keys[9], (EXPERTS, D, EXPERT_FF), D ** -0.5, 0.125, ((0, 8), (2, 4)))
    up_weight = gaussian(arg_keys[10], (EXPERTS, D, EXPERT_FF), D ** -0.5, 0.125, ((0, 8), (2, 4)))
    down_weight = gaussian(arg_keys[11], (EXPERTS, EXPERT_FF, D), EXPERT_FF ** -0.5, 0.125, ((0, 8), (1, 4)))
    return dict(cotangent=cotangent, mixer_out=mixer_out, expert_ids=expert_ids, route_weight=route_weight, saved_normalized=saved_normalized, inverse_deviation=inverse_deviation, channel_norm_gain=channel_norm_gain, taps=taps, proj_weight=proj_weight, gate_weight=gate_weight, up_weight=up_weight, down_weight=down_weight)


def expert_pass(operands):
    routed_rows, routed_grad, w_first, w_third, w_second = operands
    hidden_gate = jnp.dot(routed_rows, w_first, preferred_element_type=jnp.float32)
    hidden_up = jnp.dot(routed_rows, w_third, preferred_element_type=jnp.float32)
    sigma = jax.nn.sigmoid(hidden_gate)
    swish = hidden_gate * sigma
    activ = (swish * hidden_up).astype(jnp.bfloat16)
    grad_second = jnp.dot(activ.T, routed_grad, preferred_element_type=jnp.float32).astype(jnp.bfloat16)
    grad_activ = jnp.dot(routed_grad, w_second.T, preferred_element_type=jnp.float32)
    grad_gpre = (grad_activ * hidden_up * sigma * (1.0 + hidden_gate * (1.0 - sigma))).astype(jnp.bfloat16)
    grad_upre = (grad_activ * swish).astype(jnp.bfloat16)
    grad_first = jnp.dot(routed_rows.T, grad_gpre, preferred_element_type=jnp.float32).astype(jnp.bfloat16)
    grad_third = jnp.dot(routed_rows.T, grad_upre, preferred_element_type=jnp.float32).astype(jnp.bfloat16)
    slot_count = routed_rows.shape[0]
    model_width = routed_rows.shape[1]
    split_gate = grad_gpre.astype(jnp.float32).reshape(slot_count, N_TP, FFD)
    split_upre = grad_upre.astype(jnp.float32).reshape(slot_count, N_TP, FFD)
    first_split = w_first.astype(jnp.float32).reshape(model_width, N_TP, FFD)
    third_split = w_third.astype(jnp.float32).reshape(model_width, N_TP, FFD)
    partial_value = jnp.einsum('rgf,dgf->grd', split_gate, first_split) + jnp.einsum('rgf,dgf->grd', split_upre, third_split)
    rounded = lax.optimization_barrier(partial_value.astype(jnp.bfloat16))
    slot_grad = jnp.sum(rounded.astype(jnp.float32), axis=0).astype(jnp.bfloat16)
    return grad_first, grad_third, grad_second, slot_grad


def reference(cotangent, mixer_out, expert_ids, route_weight, saved_normalized, inverse_deviation, channel_norm_gain, taps,
              proj_weight, gate_weight, up_weight, down_weight):
    onehot = (expert_ids[:, :, None] == jnp.arange(EXPERTS, dtype=jnp.int32)[None, None, :]).astype(jnp.int32)
    flat_hot = onehot.reshape(N_SP, TOK_DEV * TOPK, EXPERTS)
    ranks = jnp.cumsum(flat_hot, axis=1) - flat_hot
    rank_pair = jnp.sum(ranks * flat_hot, axis=2).reshape(TOKENS, TOPK)
    block_index = (jnp.arange(TOKENS, dtype=jnp.int32) // TOK_DEV)[:, None]
    position = (expert_ids * (N_SP * CAP) + block_index * CAP + rank_pair).reshape(-1).astype(jnp.int32)
    rows_pair = jnp.broadcast_to(mixer_out[:, None, :], (TOKENS, TOPK, D)).reshape(-1, D)
    grad_pair = (route_weight[:, :, None] * cotangent.astype(jnp.float32)[:, None, :]).astype(jnp.bfloat16).reshape(-1, D)
    row_buffer = jnp.zeros((EXPERTS * N_SP * CAP, D), jnp.bfloat16).at[position].set(rows_pair)
    grad_buffer = jnp.zeros((EXPERTS * N_SP * CAP, D), jnp.bfloat16).at[position].set(grad_pair)
    row_buffer = row_buffer.reshape(EXPERTS, N_SP * CAP, D)
    grad_buffer = grad_buffer.reshape(EXPERTS, N_SP * CAP, D)
    grad_gate, grad_up, grad_down, slot_grad = lax.map(
        expert_pass, (row_buffer, grad_buffer, gate_weight, up_weight, down_weight))
    returned = slot_grad.reshape(-1, D)[position].reshape(TOKENS, TOPK, D).astype(jnp.float32)
    mixer_grad = (cotangent.astype(jnp.float32) + jnp.sum(returned, axis=1)).astype(jnp.bfloat16)

    normalized_values = saved_normalized.astype(jnp.float32) * channel_norm_gain[None, :]
    sigma = jax.nn.sigmoid(normalized_values)
    act_conv = (normalized_values * sigma).astype(jnp.bfloat16)
    grad_proj = jnp.dot(mixer_grad.T, act_conv, preferred_element_type=jnp.float32)
    grad_act = jnp.dot(mixer_grad, proj_weight.T, preferred_element_type=jnp.float32)
    norm_output_gradient = grad_act * sigma * (1.0 + normalized_values * (1.0 - sigma)) * channel_norm_gain[None, :]
    normalized_input = saved_normalized.astype(jnp.float32)
    gradient_mean = jnp.mean(norm_output_gradient, axis=1, keepdims=True)
    projected_mean = jnp.mean(norm_output_gradient * normalized_input, axis=1, keepdims=True)
    conv_output_gradient = inverse_deviation[:, None] * (norm_output_gradient - gradient_mean - normalized_input * projected_mean)
    padded = jnp.concatenate([conv_output_gradient, jnp.zeros((WIDTH - 1, CHANNELS), jnp.float32)], axis=0)
    total = jnp.zeros((TOKENS, CHANNELS), jnp.float32)
    for tap_index in range(WIDTH):
        total = total + taps[tap_index][None, :] * padded[tap_index:tap_index + TOKENS]
    return total.astype(jnp.bfloat16), grad_proj, grad_gate, grad_up, grad_down
```

```python
import functools

import jax
import jax.numpy as jnp
from jax import lax
from jax.experimental import pallas as pl
from jax.experimental.pallas import tpu as pltpu
from jax.sharding import PartitionSpec as P


def route_table(expert_ids, route_weight, slot_start, slot_span, capacity, experts):
    onehot = (expert_ids[:, :, None] == jnp.arange(experts, dtype=jnp.int32)[None, None, :]).astype(
        jnp.int32
    )
    flat_hot = onehot.reshape(-1, experts)
    ranks = jnp.cumsum(flat_hot, axis=0) - flat_hot
    rank_pair = jnp.sum(ranks * flat_hot, axis=1).reshape(expert_ids.shape)
    slot_index = expert_ids * capacity + rank_pair
    targets = (
        jnp.arange(experts, dtype=jnp.int32)[:, None] * capacity
        + slot_start
        + jnp.arange(slot_span, dtype=jnp.int32)[None, :]
    ).reshape(-1)
    matched = slot_index[None, :, :] == targets[:, None, None]
    dispatch = jnp.any(matched, axis=2).astype(jnp.bfloat16)
    slot_weight = jnp.sum(jnp.where(matched, route_weight[None, :, :], 0.0), axis=(1, 2))
    return (dispatch, slot_weight)


def remote(source, target, send_sem, recv_sem, device):
    return pltpu.make_async_remote_copy(
        src_ref=source,
        dst_ref=target,
        send_sem=send_sem,
        recv_sem=recv_sem,
        device_id=device,
        device_id_type=pl.DeviceIdType.MESH,
    )


def dispatch_kernel(experts, groups, *refs):
    sent = refs[:2]
    held = refs[2:4]
    local_sem, far_send, far_recv, row_send, row_recv, pair_send, pair_recv = refs[4:]
    mine = lax.axis_index("sp")
    place = lax.axis_index("tp")
    chips = groups // 2
    chip, core = place // 2, place % 2
    sibling = chip * 2 + 1 - core

    def at_chip(step):
        return ((chip + step) % chips) * 2 + core

    barrier = pltpu.get_barrier_semaphore()

    def greet(step, carry):
        pl.semaphore_signal(barrier, inc=1, device_id=((mine + step) % experts, place),
                            device_id_type=pl.DeviceIdType.MESH)
        return carry

    lax.fori_loop(1, experts, greet, 0)
    for step in range(1, chips):
        pl.semaphore_signal(barrier, inc=1, device_id=(mine, at_chip(step)),
                            device_id_type=pl.DeviceIdType.MESH)
    pl.semaphore_signal(barrier, inc=1, device_id=(mine, sibling),
                        device_id_type=pl.DeviceIdType.MESH)
    pl.semaphore_wait(barrier, experts - 1 + chips)

    def far(a, step):
        peer = (mine + step) % experts
        return remote(sent[a].at[peer], held[a].at[mine, place],
                      far_send.at[a, step], far_recv.at[a, step], (peer, place))

    def row(a, step, hop):
        source = (mine + experts - step) % experts
        block = held[a].at[source, place]
        return remote(block, block, row_send.at[a, step, hop], row_recv.at[a, step, hop],
                      (mine, at_chip(hop)))

    def pair(a, step, hop):
        source = (mine + experts - step) % experts
        block = held[a].at[source, at_chip(chips - hop)]
        return remote(block, block, pair_send.at[a, step, hop], pair_recv.at[a, step, hop],
                      (mine, sibling))

    own = [
        pltpu.make_async_copy(sent[a].at[mine], held[a].at[mine, place], local_sem.at[a])
        for a in range(2)
    ]
    for a in range(2):
        own[a].start()
    for a in range(2):
        def start_far(step, carry, a=a):
            far(a, step).start()
            return carry

        lax.fori_loop(1, experts, start_far, 0)

    def pass_on(a, step):
        for hop in range(1, chips):
            row(a, step, hop).start()
        pair(a, step, 0).start()

    def pass_rows(a, step):
        for hop in range(1, chips):
            row(a, step, hop).wait_recv()
            pair(a, step, hop).start()

    for a in range(2):
        own[a].wait()
        pass_on(a, 0)
    for a in range(2):
        def arrive(step, carry, a=a):
            far(a, step).wait_recv()
            pass_on(a, step)
            pass_rows(a, step - 1)
            return carry

        lax.fori_loop(1, experts, arrive, 0)
        pass_rows(a, experts - 1)
    for a in range(2):
        def finish(step, carry, a=a):
            for hop in range(chips):
                pair(a, step, hop).wait()
                if hop:
                    row(a, step, hop).wait_send()
            return carry

        lax.fori_loop(0, experts, finish, 0)

        def finish_far(step, carry, a=a):
            far(a, step).wait_send()
            return carry

        lax.fori_loop(1, experts, finish_far, 0)


def dispatch_blocks(rows, grads, groups):
    experts, span, width = rows.shape
    chips = groups // 2
    full = jax.ShapeDtypeStruct((experts, groups, span, width), rows.dtype)
    dma = pltpu.SemaphoreType.DMA
    return pl.pallas_call(
        functools.partial(dispatch_kernel, experts, groups),
        out_shape=(full, full),
        in_specs=[pl.BlockSpec(memory_space=pltpu.VMEM)] * 2,
        out_specs=[pl.BlockSpec(memory_space=pltpu.VMEM)] * 2,
        scratch_shapes=[dma((2,))]
        + [dma((2, experts))] * 2
        + [dma((2, experts, chips))] * 4,
        compiler_params=pltpu.CompilerParams(
            collective_id=0, has_side_effects=True, vmem_limit_bytes=24 * 2**20
        ),
        cost_estimate=pl.CostEstimate(
            flops=0, bytes_accessed=40 * full.size, transcendentals=0
        ),
    )(rows, grads)


def home_kernel(experts, groups, partial, home, pair_in, row_out, row_in, total, *sems):
    pair_send, pair_recv, row_send, row_recv, far_send, far_recv = sems
    mine = lax.axis_index("sp")
    place = lax.axis_index("tp")
    chips = groups // 2
    chip, core = place // 2, place % 2
    sibling = chip * 2 + 1 - core

    def at_chip(step):
        return ((chip + step) % chips) * 2 + core

    barrier = pltpu.get_barrier_semaphore()

    def greet(step, carry):
        pl.semaphore_signal(barrier, inc=1, device_id=((mine + step) % experts, place),
                            device_id_type=pl.DeviceIdType.MESH)
        return carry

    lax.fori_loop(1, experts, greet, 0)
    for step in range(1, chips):
        pl.semaphore_signal(barrier, inc=1, device_id=(mine, at_chip(step)),
                            device_id_type=pl.DeviceIdType.MESH)
    pl.semaphore_signal(barrier, inc=1, device_id=(mine, sibling),
                        device_id_type=pl.DeviceIdType.MESH)
    pl.semaphore_wait(barrier, experts - 1 + chips)

    def pair(step, hop):
        owner = (mine + step + 1) % experts
        other = ((chip + hop) % chips) * 2 + 1 - core
        return remote(partial.at[other, owner], pair_in.at[hop, owner],
                      pair_send.at[step, hop], pair_recv.at[step, hop], (mine, sibling))

    def row(step, hop):
        owner = (mine + step + 1) % experts
        return remote(row_out.at[hop, owner], row_in.at[hop, owner],
                      row_send.at[step, hop], row_recv.at[step, hop], (mine, at_chip(hop)))

    def far(step):
        owner = (mine + step + 1) % experts
        return remote(total.at[owner], home.at[mine],
                      far_send.at[step], far_recv.at[step], (owner, place))

    def start_pair(step, carry):
        for hop in reversed(range(chips)):
            pair(step, hop).start()
        return carry

    lax.fori_loop(0, experts, start_pair, 0)

    def add_pair(step, hop):
        owner = (mine + step + 1) % experts
        pair(step, hop).wait_recv()
        return partial[at_chip(hop), owner].astype(jnp.float32) + pair_in[hop, owner].astype(
            jnp.float32
        )

    def send_rows(step):
        owner = (mine + step + 1) % experts
        for hop in range(1, chips):
            row_out[hop, owner] = add_pair(step, hop).astype(row_out.dtype)
            row(step, hop).start()

    def add_rows(step):
        owner = (mine + step + 1) % experts
        value = add_pair(step, 0)
        for hop in range(1, chips):
            row(step, hop).wait_recv()
            value = value + row_in[hop, owner].astype(jnp.float32)
        return value.astype(total.dtype)

    def advance(step, carry):
        send_rows(step)
        before = step - 1
        total[(mine + before + 1) % experts] = add_rows(before)
        far(before).start()
        return carry

    send_rows(0)
    lax.fori_loop(1, experts, advance, 0)
    home[mine] = add_rows(experts - 1)

    def finish(step, carry):
        for hop in range(chips):
            pair(step, hop).wait_send()
            if hop:
                row(step, hop).wait_send()
        return carry

    lax.fori_loop(0, experts, finish, 0)

    def finish_far(step, carry):
        far(step).wait()
        return carry

    lax.fori_loop(0, experts - 1, finish_far, 0)


def home_blocks(partial):
    groups, experts, capacity, share = partial.shape
    chips = groups // 2
    dma = pltpu.SemaphoreType.DMA
    blocks = pltpu.VMEM((chips, experts, capacity, share), partial.dtype)
    return pl.pallas_call(
        functools.partial(home_kernel, experts, groups),
        out_shape=jax.ShapeDtypeStruct((experts, capacity, share), partial.dtype),
        in_specs=[pl.BlockSpec(memory_space=pltpu.VMEM)],
        out_specs=pl.BlockSpec(memory_space=pltpu.VMEM),
        scratch_shapes=[blocks] * 3
        + [pltpu.VMEM((experts, capacity, share), partial.dtype)]
        + [dma((experts, chips))] * 4
        + [dma((experts,))] * 2,
        compiler_params=pltpu.CompilerParams(
            collective_id=1, has_side_effects=True, vmem_limit_bytes=24 * 2**20
        ),
        cost_estimate=pl.CostEstimate(
            flops=0, bytes_accessed=40 * partial.size, transcendentals=0
        ),
    )(partial)


def line_width(experts):
    width = 1
    while 4 * width * width <= experts and experts % (2 * width) == 0:
        width = 2 * width
    return width


def sigmoid(value):
    return 1.0 / (1.0 + jnp.exp(-value))


def tail_kernel(
    experts, groups, lead, table, home, cotangent, saved, inverse, gain, taps, weight, result,
    grad_proj, blocks, every, acts, sums, extended, *sems
):
    (row_send, row_recv, pair_send, pair_recv, far_send, far_recv, half_send, half_recv,
     line_send, line_recv, side_send, side_recv, sum_send, sum_recv, halo_send, halo_recv) = sems
    mine = lax.axis_index("sp")
    place = lax.axis_index("tp")
    chips = groups // 2
    chip, core = place // 2, place % 2
    sibling = chip * 2 + 1 - core
    across = experts // lead
    line, side = mine // lead, mine % lead
    tok = saved.shape[0]
    channels = saved.shape[1]
    width = blocks.shape[-1]
    per = experts // groups
    half = tok // 2

    def at_chip(step):
        return ((chip + step) % chips) * 2 + core

    barrier = pltpu.get_barrier_semaphore()

    def greet(step, carry):
        pl.semaphore_signal(barrier, inc=1, device_id=((mine + step) % experts, place),
                            device_id_type=pl.DeviceIdType.MESH)
        return carry

    def greet_group(step, carry):
        pl.semaphore_signal(barrier, inc=1, device_id=(mine, (place + step) % groups),
                            device_id_type=pl.DeviceIdType.MESH)
        return carry

    lax.fori_loop(1, experts, greet, 0)
    lax.fori_loop(1, groups, greet_group, 0)
    normalized = saved[...].astype(jnp.float32)
    scaled = normalized * gain[...]
    gate = sigmoid(scaled)
    acts[mine] = (scaled * gate).astype(jnp.bfloat16)
    pl.semaphore_wait(barrier, experts + groups - 2)

    def along(step):
        return remote(acts.at[mine], acts.at[mine], line_send.at[step], line_recv.at[step],
                      (((line + step) % across) * lead + side, place))

    def arrived(step):
        source = ((line + across - step) % across) * lead + side
        return remote(acts.at[source], acts.at[source], line_send.at[step], line_recv.at[step],
                      (((line + step) % across) * lead + side, place))

    def beside(step, hop):
        source = ((line + across - step) % across) * lead + side
        return remote(acts.at[source], acts.at[source], side_send.at[step, hop],
                      side_recv.at[step, hop], (line * lead + (side + hop) % lead, place))

    def share_at(owner):
        return blocks.at[pl.ds(owner * per, per)]

    def row(hop):
        return remote(share_at(place), share_at(place), row_send.at[hop], row_recv.at[hop],
                      (mine, at_chip(hop)))

    def pair(hop):
        owner = at_chip(chips - hop)
        return remote(share_at(owner), share_at(owner), pair_send.at[hop], pair_recv.at[hop],
                      (mine, sibling))

    share = jnp.dot(table[...], home[...], preferred_element_type=jnp.float32)
    share = (share + cotangent[...].astype(jnp.float32)).astype(jnp.bfloat16)
    for part in range(per):
        piece = share[:, part * width : (part + 1) * width]
        blocks[place * per + part] = piece.reshape(2, half, width)
    for hop in range(1, chips):
        row(hop).start()
    pair(0).start()
    for step in range(1, across):
        along(step).start()
    for hop in range(1, lead):
        beside(0, hop).start()
    for hop in range(1, chips):
        row(hop).wait_recv()
        pair(hop).start()
    for hop in range(chips):
        pair(hop).wait_recv()

    def far(step):
        peer = (mine + step) % experts
        return remote(blocks.at[peer, core], every.at[mine, core], far_send.at[step],
                      far_recv.at[step], (peer, place))

    def to_half(step):
        source = (mine + experts - step) % experts
        return remote(every.at[source, core], every.at[source, core], half_send.at[step],
                      half_recv.at[step], (mine, sibling))

    def start_far(step, carry):
        far(step).start()
        return carry

    lax.fori_loop(1, experts, start_far, 0)
    every[mine] = blocks[mine]

    grad = jnp.zeros((tok, channels), jnp.float32)
    for part in range(experts):
        grad = grad + lax.dot_general(
            blocks[part].reshape(tok, width),
            weight[:, part * width : (part + 1) * width],
            (((1,), (1,)), ((), ())),
            preferred_element_type=jnp.float32,
        )
    normalized = saved[...].astype(jnp.float32)
    scaled = normalized * gain[...]
    gate = sigmoid(scaled)
    grad = grad * gate * (1.0 + scaled * (1.0 - gate)) * gain[...]
    lanes = min(channels, 128)
    first = jnp.zeros((tok, lanes), jnp.float32)
    second = jnp.zeros((tok, lanes), jnp.float32)
    for at in range(0, channels, lanes):
        first = first + grad[:, at : at + lanes]
        second = second + grad[:, at : at + lanes] * normalized[:, at : at + lanes]
    sums[place, 0] = jnp.sum(jnp.transpose(first).reshape(lanes // 8, 8, tok), axis=0)
    sums[place, 1] = jnp.sum(jnp.transpose(second).reshape(lanes // 8, 8, tok), axis=0)

    def tell(step):
        return remote(sums.at[place], sums.at[place], sum_send.at[step], sum_recv.at[step],
                      (mine, (place + step) % groups))

    def start_tell(step, carry):
        tell(step).start()
        return carry

    def wait_tell(step, carry):
        tell(step).wait()
        return carry

    lax.fori_loop(1, groups, start_tell, 0)
    for step in range(1, across - 1):
        arrived(step).wait_recv()
        for hop in range(1, lead):
            beside(step, hop).start()
    lax.fori_loop(1, groups, wait_tell, 0)
    count = channels * groups
    total = jnp.sum(sums[...], axis=0)

    def column(kind):
        flat = jnp.sum(total[kind], axis=0, keepdims=True) / count
        return jnp.transpose(jnp.broadcast_to(flat, (lanes, tok)))

    mean, slope = column(0), column(1)
    for at in range(0, channels, lanes):
        extended[at // lanes, 0:tok] = inverse[...] * (
            grad[:, at : at + lanes] - mean - normalized[:, at : at + lanes] * slope
        )
    reach = extended.shape[1] - tok

    def halo():
        return remote(extended.at[:, pl.ds(0, reach)], extended.at[:, pl.ds(tok, reach)],
                      halo_send, halo_recv, ((mine + experts - 1) % experts, place))

    @pl.when(mine > 0)
    def _():
        halo().start()

    @pl.when(mine == experts - 1)
    def _():
        extended[:, tok : tok + reach] = jnp.zeros((channels // lanes, reach, lanes), jnp.float32)

    arrived(across - 1).wait_recv()
    for hop in range(1, lead):
        beside(across - 1, hop).start()

    def forward(step, carry):
        far(step).wait_recv()
        to_half(step).start()
        return carry

    lax.fori_loop(1, experts, forward, 0)

    @pl.when(mine < experts - 1)
    def _():
        halo().wait_recv()

    for at in range(0, channels, lanes):
        value = jnp.zeros((tok, lanes), jnp.float32)
        for tap in range(taps.shape[0]):
            value = value + taps[tap : tap + 1, at : at + lanes] * extended[at // lanes, tap : tap + tok]
        result[:, at : at + lanes] = value.astype(result.dtype)

    def arrive(step, carry):
        to_half(step).wait_recv()
        return carry

    lax.fori_loop(1, experts, arrive, 0)
    for step in range(across):
        for hop in range(1, lead):
            beside(step, hop).wait_recv()
    grad_proj[...] = lax.dot_general(
        every[...].reshape(experts * tok, width),
        acts[...].reshape(experts * tok, channels),
        (((0,), (0,)), ((), ())),
        preferred_element_type=jnp.float32,
    )

    @pl.when(mine > 0)
    def _():
        halo().wait_send()

    for hop in range(chips):
        pair(hop).wait_send()
        if hop:
            row(hop).wait_send()
    for step in range(across):
        if step:
            along(step).wait_send()
        for hop in range(1, lead):
            beside(step, hop).wait_send()

    def finish(step, carry):
        far(step).wait_send()
        to_half(step).wait_send()
        return carry

    lax.fori_loop(1, experts, finish, 0)


def tail_blocks(table, home, cotangent, saved, inverse, gain, taps, weight, experts, groups):
    tok, channels = saved.shape
    model_width = weight.shape[1]
    width = model_width // experts
    lead = line_width(experts)
    across = experts // lead
    lanes = min(channels, 128)
    reach = (taps.shape[0] + 6) // 8 * 8
    dma = pltpu.SemaphoreType.DMA
    vmem = pl.BlockSpec(memory_space=pltpu.VMEM)
    return pl.pallas_call(
        functools.partial(tail_kernel, experts, groups, lead),
        out_shape=(
            jax.ShapeDtypeStruct((tok, channels), jnp.bfloat16),
            jax.ShapeDtypeStruct((width, channels), jnp.float32),
        ),
        in_specs=[vmem] * 8,
        out_specs=[vmem] * 2,
        scratch_shapes=[
            pltpu.VMEM((experts, 2, tok // 2, width), jnp.bfloat16),
            pltpu.VMEM((experts, 2, tok // 2, width), jnp.bfloat16),
            pltpu.VMEM((experts, tok, channels), jnp.bfloat16),
            pltpu.VMEM((groups, 2, 8, tok), jnp.float32),
            pltpu.VMEM((channels // lanes, tok + reach, lanes), jnp.float32),
        ]
        + [dma((groups // 2,))] * 4
        + [dma((experts,))] * 4
        + [dma((across,))] * 2
        + [dma((across, lead))] * 2
        + [dma((groups,))] * 2
        + [dma] * 2,
        compiler_params=pltpu.CompilerParams(
            collective_id=2, has_side_effects=True, vmem_limit_bytes=32 * 2**20
        ),
        cost_estimate=pl.CostEstimate(
            flops=10**9, bytes_accessed=10**7, transcendentals=0
        ),
    )(table, home, cotangent, saved, inverse, gain, taps, weight)


def shards(
    cotangent,
    mixer_out,
    expert_ids,
    route_weight,
    saved_normalized,
    inverse_deviation,
    channel_norm_gain,
    taps,
    proj_weight,
    gate_weight,
    up_weight,
    down_weight,
):
    experts = lax.axis_size("sp")
    groups = lax.axis_size("tp")
    tok_rows, model_width = cotangent.shape
    capacity = groups * max(1, 4 * tok_rows // (experts * groups))
    slot_span = capacity // groups
    slot_start = lax.axis_index("tp") * slot_span
    dispatch, slot_weight = route_table(
        expert_ids, route_weight, slot_start, slot_span, capacity, experts
    )
    sent_rows = jnp.dot(dispatch, mixer_out, preferred_element_type=jnp.float32).astype(
        jnp.bfloat16
    )
    sent_grad = (
        slot_weight[:, None] * jnp.dot(dispatch, cotangent, preferred_element_type=jnp.float32)
    ).astype(jnp.bfloat16)
    sent_rows = sent_rows.reshape(experts, slot_span, model_width)
    sent_grad = sent_grad.reshape(experts, slot_span, model_width)
    routed_rows, routed_grad = dispatch_blocks(sent_rows, sent_grad, groups)
    full_table, unused_weight = route_table(
        expert_ids, route_weight, 0, capacity, capacity, experts
    )
    routed_rows = routed_rows.reshape(-1, model_width)
    routed_grad = routed_grad.reshape(-1, model_width)
    w_first = gate_weight[0]
    w_third = up_weight[0]
    w_second = down_weight[0]
    contract_last = (((1,), (1,)), ((), ()))
    contract_first = (((0,), (0,)), ((), ()))
    hidden_gate = jnp.dot(routed_rows, w_first, preferred_element_type=jnp.float32)
    hidden_up = jnp.dot(routed_rows, w_third, preferred_element_type=jnp.float32)
    sigma = jax.nn.sigmoid(hidden_gate)
    swish = hidden_gate * sigma
    activ = (swish * hidden_up).astype(jnp.bfloat16)
    grad_second = lax.dot_general(
        activ, routed_grad, contract_first, preferred_element_type=jnp.float32
    ).astype(jnp.bfloat16)
    grad_activ = lax.dot_general(
        routed_grad, w_second, contract_last, preferred_element_type=jnp.float32
    )
    grad_gpre = (grad_activ * hidden_up * sigma * (1.0 + hidden_gate * (1.0 - sigma))).astype(
        jnp.bfloat16
    )
    grad_upre = (grad_activ * swish).astype(jnp.bfloat16)
    grad_first = lax.dot_general(
        routed_rows, grad_gpre, contract_first, preferred_element_type=jnp.float32
    ).astype(jnp.bfloat16)
    grad_third = lax.dot_general(
        routed_rows, grad_upre, contract_first, preferred_element_type=jnp.float32
    ).astype(jnp.bfloat16)
    partial_value = lax.dot_general(
        grad_gpre, w_first, contract_last, preferred_element_type=jnp.float32
    ) + lax.dot_general(grad_upre, w_third, contract_last, preferred_element_type=jnp.float32)
    share = model_width // groups
    partial_groups = jnp.transpose(
        partial_value.astype(jnp.bfloat16).reshape(-1, groups, share), (1, 0, 2)
    )
    home_rows = home_blocks(partial_groups.reshape(groups, experts, capacity, share))
    own_cotangent = lax.dynamic_slice_in_dim(
        cotangent, lax.axis_index("tp") * share, share, axis=1
    )
    result, grad_proj = tail_blocks(
        jnp.transpose(full_table),
        home_rows.reshape(-1, share),
        own_cotangent,
        saved_normalized,
        inverse_deviation[:, None],
        channel_norm_gain[None, :],
        taps,
        proj_weight,
        experts,
        groups,
    )
    return (
        result,
        grad_proj,
        grad_first[None],
        grad_third[None],
        grad_second[None],
    )


def solution(mesh):
    return jax.shard_map(
        shards,
        mesh=mesh,
        in_specs=(
            P("sp", None),
            P("sp", None),
            P("sp", None),
            P("sp", None),
            P("sp", "tp"),
            P("sp"),
            P("tp"),
            P(None, "tp"),
            P("tp", None),
            P("sp", None, "tp"),
            P("sp", None, "tp"),
            P("sp", "tp", None),
        ),
        out_specs=(
            P("sp", "tp"),
            P("sp", "tp"),
            P("sp", None, "tp"),
            P("sp", None, "tp"),
            P("sp", "tp", None),
        ),
        check_vma=False,
    )
```

```python
import functools

import jax
import jax.numpy as jnp
from jax import lax
from jax.experimental import pallas as pl
from jax.experimental.pallas import tpu as pltpu
from jax.sharding import PartitionSpec as P


def remote(source, target, send_sem, recv_sem, device):
    return pltpu.make_async_remote_copy(
        src_ref=source,
        dst_ref=target,
        send_sem=send_sem,
        recv_sem=recv_sem,
        device_id=device,
        device_id_type=pl.DeviceIdType.MESH,
    )


CONTRACT_LAST = (((1,), (1,)), ((), ()))
CONTRACT_FIRST = (((0,), (0,)), ((), ()))


def expert_kernel(
    experts, groups, ids, route, mixer, cotangent, gate_far, up_far, down_far,
    home, grad_gate, grad_up, grad_down, table,
    rows, grads, sent_rows, sent_grads, gate, up, down, hidden_gate, hidden_up, active,
    grad_hg, grad_hu, partial, pair_in, row_out, row_in, total, slot_weight, *sems
):
    (load_sem, far_send, far_recv, row_send, row_recv, pair_send, pair_recv,
     home_send, home_recv, sum_send, sum_recv, back_send, back_recv) = sems
    mine = lax.axis_index("sp")
    place = lax.axis_index("tp")
    chips = groups // 2
    chip, core = place // 2, place % 2
    sibling = chip * 2 + 1 - core
    tok = mixer.shape[0]
    capacity, share = rows.shape[2:]
    slots = experts * capacity
    ff = gate.shape[1]
    middle = experts // 2
    sent = (sent_rows, sent_grads)
    held = (rows, grads)

    def at_chip(step):
        return ((chip + step) % chips) * 2 + core

    loads = [
        pltpu.make_async_copy(source, target, load_sem.at[at])
        for at, (source, target) in enumerate(((gate_far, gate), (up_far, up), (down_far, down)))
    ]
    for load in loads:
        load.start()
    barrier = pltpu.get_barrier_semaphore()

    def greet(step, carry):
        pl.semaphore_signal(barrier, inc=1, device_id=((mine + step) % experts, place),
                            device_id_type=pl.DeviceIdType.MESH)
        return carry

    lax.fori_loop(1, experts, greet, 0)
    for step in range(1, chips):
        pl.semaphore_signal(barrier, inc=1, device_id=(mine, at_chip(step)),
                            device_id_type=pl.DeviceIdType.MESH)
    pl.semaphore_signal(barrier, inc=1, device_id=(mine, sibling),
                        device_id_type=pl.DeviceIdType.MESH)

    expert = lax.broadcasted_iota(jnp.int32, (experts, tok), 0)
    hot = [(ids[k : k + 1] == expert).astype(jnp.float32) for k in range(ids.shape[0])]
    before = lax.broadcasted_iota(jnp.int32, (tok, tok), 0)
    after = lax.broadcasted_iota(jnp.int32, (tok, tok), 1)
    rank = jnp.dot(
        sum(hot).astype(jnp.bfloat16),
        (before < after).astype(jnp.float32).astype(jnp.bfloat16),
        preferred_element_type=jnp.float32,
    )
    slot = expert.astype(jnp.float32) * capacity + rank
    number = lax.broadcasted_iota(jnp.int32, (slots, tok), 0).astype(jnp.float32)
    chosen = jnp.zeros((slots, tok), jnp.float32)
    weighted = jnp.zeros((slots, tok), jnp.float32)
    for k in range(ids.shape[0]):
        match = number == jnp.sum(hot[k] * slot, axis=0, keepdims=True)
        chosen = jnp.where(match, 1.0, chosen)
        weighted = jnp.where(match, route[k : k + 1], weighted)
    table[...] = chosen.astype(jnp.bfloat16).reshape(experts, capacity, tok)
    slot_weight[...] = jnp.sum(weighted, axis=1, keepdims=True).reshape(experts, capacity, 1)
    columns = pl.ds(pl.multiple_of(place * share, share), share)
    every = table[...].reshape(slots, tok)
    scale = slot_weight[...].reshape(slots, 1)
    sent_rows[...] = (
        jnp.dot(every, mixer[:, columns], preferred_element_type=jnp.float32)
        .astype(jnp.bfloat16).reshape(experts, capacity, share)
    )
    sent_grads[...] = (
        (scale * jnp.dot(every, cotangent[:, columns], preferred_element_type=jnp.float32))
        .astype(jnp.bfloat16).reshape(experts, capacity, share)
    )
    pl.semaphore_wait(barrier, experts - 1 + chips)

    def far(a, step):
        peer = (mine + step) % experts
        return remote(sent[a].at[peer], held[a].at[step, place],
                      far_send.at[a, step], far_recv.at[a, step], (peer, place))

    def row(a, step, hop):
        block = held[a].at[step, place]
        return remote(block, block, row_send.at[a, step, hop], row_recv.at[a, step, hop],
                      (mine, at_chip(hop)))

    def pair(a, step, hop):
        block = held[a].at[step, at_chip(chips - hop)]
        return remote(block, block, pair_send.at[a, step, hop], pair_recv.at[a, step, hop],
                      (mine, sibling))

    for a in range(2):
        def start_far(step, carry, a=a):
            far(a, step).start()
            return carry

        lax.fori_loop(1, experts, start_far, 0)

    own = table[mine]
    own_scale = slot_weight[mine]
    for g in range(groups):
        span = slice(g * share, (g + 1) * share)
        rows[0, g] = jnp.dot(
            own, mixer[:, span], preferred_element_type=jnp.float32
        ).astype(jnp.bfloat16)
        grads[0, g] = (
            own_scale * jnp.dot(own, cotangent[:, span], preferred_element_type=jnp.float32)
        ).astype(jnp.bfloat16)

    def each(low, high, act):
        def body(step, carry):
            act(step)
            return carry

        lax.fori_loop(low, high, body, 0)

    def service(a, step):
        far(a, step).wait_recv()
        for hop in range(1, chips):
            row(a, step, hop).start()
        pair(a, step, 0).start()

    def settle(a, step):
        for hop in range(1, chips):
            row(a, step, hop).wait_recv()
            pair(a, step, hop).start()

    def complete(a, step):
        for hop in range(chips):
            pair(a, step, hop).wait_recv()

    def both(a):
        def act(step):
            service(a, step)
            settle(a, step - 2)
        return act

    def chunk(ref, at, g):
        return ref[at * middle : (at + 1) * middle, g].reshape(middle * capacity, share)

    def lines(at):
        return slice(at * middle * capacity, (at + 1) * middle * capacity)

    def ahead(at):
        for weight, result in ((gate, hidden_gate), (up, hidden_up)):
            value = None
            for g in range(groups):
                term = jnp.dot(
                    chunk(rows, at, g), weight[g * share : (g + 1) * share, :],
                    preferred_element_type=jnp.float32,
                )
                value = term if value is None else value + term
            result[lines(at), :] = value

    def back(at):
        value = None
        for g in range(groups):
            term = lax.dot_general(
                chunk(grads, at, g), down[:, g * share : (g + 1) * share], CONTRACT_LAST,
                preferred_element_type=jnp.float32,
            )
            value = term if value is None else value + term
        hg = hidden_gate[lines(at), :]
        hu = hidden_up[lines(at), :]
        sigma = sigmoid(hg)
        swish = hg * sigma
        active[lines(at), :] = (swish * hu).astype(jnp.bfloat16)
        grad_hg[lines(at), :] = (value * hu * sigma * (1.0 + hg * (1.0 - sigma))).astype(jnp.bfloat16)
        grad_hu[lines(at), :] = (value * swish).astype(jnp.bfloat16)
        for g in range(groups):
            term = lax.dot_general(
                grad_hg[lines(at), :], gate[g * share : (g + 1) * share, :], CONTRACT_LAST,
                preferred_element_type=jnp.float32,
            ) + lax.dot_general(
                grad_hu[lines(at), :], up[g * share : (g + 1) * share, :], CONTRACT_LAST,
                preferred_element_type=jnp.float32,
            )
            partial[g, at * middle : (at + 1) * middle] = term.astype(jnp.bfloat16).reshape(
                middle, capacity, share
            )

    def weight_grads(g):
        span = pl.ds(pl.multiple_of(g * share, share), share)
        left = rows[:, g].reshape(slots, share)
        grad_gate[span, :] = lax.dot_general(
            left, grad_hg[...], CONTRACT_FIRST, preferred_element_type=jnp.float32
        ).astype(jnp.bfloat16)
        grad_up[span, :] = lax.dot_general(
            left, grad_hu[...], CONTRACT_FIRST, preferred_element_type=jnp.float32
        ).astype(jnp.bfloat16)
        grad_down[:, span] = lax.dot_general(
            active[...], grads[:, g].reshape(slots, share), CONTRACT_FIRST,
            preferred_element_type=jnp.float32,
        ).astype(jnp.bfloat16)

    def home_pair(step, hop):
        other = ((chip + hop) % chips) * 2 + 1 - core
        return remote(partial.at[other, step], pair_in.at[hop, step],
                      home_send.at[step, hop], home_recv.at[step, hop], (mine, sibling))

    def home_row(step, hop):
        return remote(row_out.at[hop, step], row_in.at[hop, step],
                      sum_send.at[step, hop], sum_recv.at[step, hop], (mine, at_chip(hop)))

    def home_far(step):
        owner = (mine + experts - step) % experts
        return remote(total.at[step], home.at[mine],
                      back_send.at[step], back_recv.at[step], (owner, place))

    def start_pair(step):
        for hop in reversed(range(chips)):
            home_pair(step, hop).start()

    def add_pair(step, hop):
        home_pair(step, hop).wait_recv()
        return partial[at_chip(hop), step].astype(jnp.float32) + pair_in[hop, step].astype(
            jnp.float32
        )

    def send_rows(step):
        for hop in range(1, chips):
            row_out[hop, step] = add_pair(step, hop).astype(row_out.dtype)
            home_row(step, hop).start()

    def add_rows(step):
        value = add_pair(step, 0)
        for hop in range(1, chips):
            home_row(step, hop).wait_recv()
            value = value + row_in[hop, step].astype(jnp.float32)
        return value.astype(total.dtype)

    def send_home(step):
        total[step] = add_rows(step)
        home_far(step).start()

    each(1, 3, functools.partial(service, 0))
    each(3, experts, both(0))
    service(1, 1)
    settle(0, experts - 2)
    service(1, 2)
    settle(0, experts - 1)
    loads[0].wait()
    loads[1].wait()
    each(1, middle, functools.partial(complete, 0))
    ahead(0)
    each(3, middle + 1, both(1))
    each(middle, experts, functools.partial(complete, 0))
    ahead(1)
    each(middle + 1, middle + 2, both(1))
    loads[2].wait()
    each(1, middle, functools.partial(complete, 1))
    back(0)
    each(0, middle, start_pair)
    each(middle + 2, experts, both(1))
    settle(1, experts - 2)
    settle(1, experts - 1)
    each(0, middle, send_rows)
    each(middle, experts, functools.partial(complete, 1))
    back(1)
    each(middle, experts, start_pair)
    weight_grads(0)
    home[mine] = add_rows(0)
    each(1, middle, send_home)
    each(middle, experts, send_rows)
    each(1, groups - 1, weight_grads)
    each(middle, experts, send_home)
    weight_grads(groups - 1)

    def finish(step):
        for hop in range(chips):
            home_pair(step, hop).wait_send()
            if hop:
                home_row(step, hop).wait_send()

    def finish_far(step):
        home_far(step).wait()
        for a in range(2):
            far(a, step).wait_send()
            for hop in range(chips):
                pair(a, step, hop).wait_send()
                if hop:
                    row(a, step, hop).wait_send()

    each(0, experts, finish)
    each(1, experts, finish_far)


def expert_blocks(ids, route, mixer, cotangent, gate, up, down, experts, groups):
    tok, width = mixer.shape
    ff = gate.shape[1]
    share = width // groups
    capacity = groups * max(1, 4 * tok // (experts * groups))
    chips = groups // 2
    slots = experts * capacity
    half = jnp.bfloat16
    dma = pltpu.SemaphoreType.DMA
    vmem = pl.BlockSpec(memory_space=pltpu.VMEM)
    held = pltpu.VMEM((experts, groups, capacity, share), half)
    sent = pltpu.VMEM((experts, capacity, share), half)
    blocks = pltpu.VMEM((chips, experts, capacity, share), half)
    return pl.pallas_call(
        functools.partial(expert_kernel, experts, groups),
        out_shape=(
            jax.ShapeDtypeStruct((experts, capacity, share), half),
            jax.ShapeDtypeStruct(gate.shape, half),
            jax.ShapeDtypeStruct(up.shape, half),
            jax.ShapeDtypeStruct(down.shape, half),
            jax.ShapeDtypeStruct((experts, capacity, tok), half),
        ),
        in_specs=[vmem] * 4 + [pl.BlockSpec(memory_space=pl.ANY)] * 3,
        out_specs=[vmem] * 5,
        scratch_shapes=[held] * 2
        + [sent] * 2
        + [pltpu.VMEM(array.shape, half) for array in (gate, up, down)]
        + [pltpu.VMEM((slots, ff), jnp.float32)] * 2
        + [pltpu.VMEM((slots, ff), half)] * 3
        + [pltpu.VMEM((groups, experts, capacity, share), half)]
        + [blocks] * 3
        + [sent, pltpu.VMEM((experts, capacity, 1), jnp.float32)]
        + [dma((3,))]
        + [dma((2, experts))] * 2
        + [dma((2, experts, chips))] * 4
        + [dma((experts, chips))] * 4
        + [dma((experts,))] * 2,
        compiler_params=pltpu.CompilerParams(
            collective_id=0, has_side_effects=True, vmem_limit_bytes=48 * 2**20
        ),
        cost_estimate=pl.CostEstimate(flops=10**10, bytes_accessed=10**7, transcendentals=0),
    )(ids, route, mixer, cotangent, gate, up, down)


def line_width(experts):
    width = 1
    while 4 * width * width <= experts and experts % (2 * width) == 0:
        width = 2 * width
    return width


def sigmoid(value):
    return 1.0 / (1.0 + jnp.exp(-value))


def tail_kernel(
    experts, groups, lead, table, home, cotangent, saved, inverse, gain, taps, weight, result,
    grad_proj, blocks, every, acts, sums, extended, *sems
):
    (row_send, row_recv, pair_send, pair_recv, far_send, far_recv, half_send, half_recv,
     line_send, line_recv, side_send, side_recv, sum_send, sum_recv, halo_send, halo_recv) = sems
    mine = lax.axis_index("sp")
    place = lax.axis_index("tp")
    chips = groups // 2
    chip, core = place // 2, place % 2
    sibling = chip * 2 + 1 - core
    across = experts // lead
    line, side = mine // lead, mine % lead
    tok = saved.shape[0]
    channels = saved.shape[1]
    width = blocks.shape[-1]
    per = experts // groups
    half = tok // 2

    def at_chip(step):
        return ((chip + step) % chips) * 2 + core

    barrier = pltpu.get_barrier_semaphore()

    def greet(step, carry):
        pl.semaphore_signal(barrier, inc=1, device_id=((mine + step) % experts, place),
                            device_id_type=pl.DeviceIdType.MESH)
        return carry

    def greet_group(step, carry):
        pl.semaphore_signal(barrier, inc=1, device_id=(mine, (place + step) % groups),
                            device_id_type=pl.DeviceIdType.MESH)
        return carry

    lax.fori_loop(1, experts, greet, 0)
    lax.fori_loop(1, groups, greet_group, 0)
    normalized = saved[...].astype(jnp.float32)
    scaled = normalized * gain[...]
    gate = sigmoid(scaled)
    acts[mine] = (scaled * gate).astype(jnp.bfloat16)
    pl.semaphore_wait(barrier, experts + groups - 2)

    def along(step):
        return remote(acts.at[mine], acts.at[mine], line_send.at[step], line_recv.at[step],
                      (((line + step) % across) * lead + side, place))

    def arrived(step):
        source = ((line + across - step) % across) * lead + side
        return remote(acts.at[source], acts.at[source], line_send.at[step], line_recv.at[step],
                      (((line + step) % across) * lead + side, place))

    def beside(step, hop):
        source = ((line + across - step) % across) * lead + side
        return remote(acts.at[source], acts.at[source], side_send.at[step, hop],
                      side_recv.at[step, hop], (line * lead + (side + hop) % lead, place))

    def share_at(owner):
        return blocks.at[pl.ds(owner * per, per)]

    def row(hop):
        return remote(share_at(place), share_at(place), row_send.at[hop], row_recv.at[hop],
                      (mine, at_chip(hop)))

    def pair(hop):
        owner = at_chip(chips - hop)
        return remote(share_at(owner), share_at(owner), pair_send.at[hop], pair_recv.at[hop],
                      (mine, sibling))

    share = lax.dot_general(
        table[...], home[...], CONTRACT_FIRST, preferred_element_type=jnp.float32
    )
    share = (share + cotangent[...].astype(jnp.float32)).astype(jnp.bfloat16)
    for part in range(per):
        piece = share[:, part * width : (part + 1) * width]
        blocks[place * per + part] = piece.reshape(2, half, width)
    for hop in range(1, chips):
        row(hop).start()
    pair(0).start()
    for step in range(1, across):
        along(step).start()
    for hop in range(1, lead):
        beside(0, hop).start()
    for hop in range(1, chips):
        row(hop).wait_recv()
        pair(hop).start()
    for hop in range(chips):
        pair(hop).wait_recv()

    def far(step):
        peer = (mine + step) % experts
        return remote(blocks.at[peer, core], every.at[mine, core], far_send.at[step],
                      far_recv.at[step], (peer, place))

    def to_half(step):
        source = (mine + experts - step) % experts
        return remote(every.at[source, core], every.at[source, core], half_send.at[step],
                      half_recv.at[step], (mine, sibling))

    def start_far(step, carry):
        far(step).start()
        return carry

    lax.fori_loop(1, experts, start_far, 0)
    every[mine] = blocks[mine]

    grad = jnp.zeros((tok, channels), jnp.float32)
    for part in range(experts):
        grad = grad + lax.dot_general(
            blocks[part].reshape(tok, width),
            weight[:, part * width : (part + 1) * width],
            (((1,), (1,)), ((), ())),
            preferred_element_type=jnp.float32,
        )
    normalized = saved[...].astype(jnp.float32)
    scaled = normalized * gain[...]
    gate = sigmoid(scaled)
    grad = grad * gate * (1.0 + scaled * (1.0 - gate)) * gain[...]
    lanes = min(channels, 128)
    first = jnp.zeros((tok, lanes), jnp.float32)
    second = jnp.zeros((tok, lanes), jnp.float32)
    for at in range(0, channels, lanes):
        first = first + grad[:, at : at + lanes]
        second = second + grad[:, at : at + lanes] * normalized[:, at : at + lanes]
    sums[place, 0] = jnp.sum(jnp.transpose(first).reshape(lanes // 8, 8, tok), axis=0)
    sums[place, 1] = jnp.sum(jnp.transpose(second).reshape(lanes // 8, 8, tok), axis=0)

    def tell(step):
        return remote(sums.at[place], sums.at[place], sum_send.at[step], sum_recv.at[step],
                      (mine, (place + step) % groups))

    def start_tell(step, carry):
        tell(step).start()
        return carry

    def wait_tell(step, carry):
        tell(step).wait()
        return carry

    lax.fori_loop(1, groups, start_tell, 0)
    for step in range(1, across - 1):
        arrived(step).wait_recv()
        for hop in range(1, lead):
            beside(step, hop).start()
    lax.fori_loop(1, groups, wait_tell, 0)
    count = channels * groups
    total = jnp.sum(sums[...], axis=0)

    def column(kind):
        flat = jnp.sum(total[kind], axis=0, keepdims=True) / count
        return jnp.transpose(jnp.broadcast_to(flat, (lanes, tok)))

    mean, slope = column(0), column(1)
    for at in range(0, channels, lanes):
        extended[at // lanes, 0:tok] = inverse[...] * (
            grad[:, at : at + lanes] - mean - normalized[:, at : at + lanes] * slope
        )
    reach = extended.shape[1] - tok

    def halo():
        return remote(extended.at[:, pl.ds(0, reach)], extended.at[:, pl.ds(tok, reach)],
                      halo_send, halo_recv, ((mine + experts - 1) % experts, place))

    @pl.when(mine > 0)
    def _():
        halo().start()

    @pl.when(mine == experts - 1)
    def _():
        extended[:, tok : tok + reach] = jnp.zeros((channels // lanes, reach, lanes), jnp.float32)

    arrived(across - 1).wait_recv()
    for hop in range(1, lead):
        beside(across - 1, hop).start()

    def forward(step, carry):
        far(step).wait_recv()
        to_half(step).start()
        return carry

    lax.fori_loop(1, experts, forward, 0)

    @pl.when(mine < experts - 1)
    def _():
        halo().wait_recv()

    for at in range(0, channels, lanes):
        value = jnp.zeros((tok, lanes), jnp.float32)
        for tap in range(taps.shape[0]):
            value = value + taps[tap : tap + 1, at : at + lanes] * extended[at // lanes, tap : tap + tok]
        result[:, at : at + lanes] = value.astype(result.dtype)

    def arrive(step, carry):
        to_half(step).wait_recv()
        return carry

    lax.fori_loop(1, experts, arrive, 0)
    for step in range(across):
        for hop in range(1, lead):
            beside(step, hop).wait_recv()
    grad_proj[...] = lax.dot_general(
        every[...].reshape(experts * tok, width),
        acts[...].reshape(experts * tok, channels),
        (((0,), (0,)), ((), ())),
        preferred_element_type=jnp.float32,
    )

    @pl.when(mine > 0)
    def _():
        halo().wait_send()

    for hop in range(chips):
        pair(hop).wait_send()
        if hop:
            row(hop).wait_send()
    for step in range(across):
        if step:
            along(step).wait_send()
        for hop in range(1, lead):
            beside(step, hop).wait_send()

    def finish(step, carry):
        far(step).wait_send()
        to_half(step).wait_send()
        return carry

    lax.fori_loop(1, experts, finish, 0)


def tail_blocks(table, home, cotangent, saved, inverse, gain, taps, weight, experts, groups):
    tok, channels = saved.shape
    model_width = weight.shape[1]
    width = model_width // experts
    lead = line_width(experts)
    across = experts // lead
    lanes = min(channels, 128)
    reach = (taps.shape[0] + 6) // 8 * 8
    dma = pltpu.SemaphoreType.DMA
    vmem = pl.BlockSpec(memory_space=pltpu.VMEM)
    return pl.pallas_call(
        functools.partial(tail_kernel, experts, groups, lead),
        out_shape=(
            jax.ShapeDtypeStruct((tok, channels), jnp.bfloat16),
            jax.ShapeDtypeStruct((width, channels), jnp.float32),
        ),
        in_specs=[vmem] * 8,
        out_specs=[vmem] * 2,
        scratch_shapes=[
            pltpu.VMEM((experts, 2, tok // 2, width), jnp.bfloat16),
            pltpu.VMEM((experts, 2, tok // 2, width), jnp.bfloat16),
            pltpu.VMEM((experts, tok, channels), jnp.bfloat16),
            pltpu.VMEM((groups, 2, 8, tok), jnp.float32),
            pltpu.VMEM((channels // lanes, tok + reach, lanes), jnp.float32),
        ]
        + [dma((groups // 2,))] * 4
        + [dma((experts,))] * 4
        + [dma((across,))] * 2
        + [dma((across, lead))] * 2
        + [dma((groups,))] * 2
        + [dma] * 2,
        compiler_params=pltpu.CompilerParams(
            collective_id=2, has_side_effects=True, vmem_limit_bytes=32 * 2**20
        ),
        cost_estimate=pl.CostEstimate(
            flops=10**9, bytes_accessed=10**7, transcendentals=0
        ),
    )(table, home, cotangent, saved, inverse, gain, taps, weight)


def shards(
    cotangent,
    mixer_out,
    expert_ids,
    route_weight,
    saved_normalized,
    inverse_deviation,
    channel_norm_gain,
    taps,
    proj_weight,
    gate_weight,
    up_weight,
    down_weight,
):
    experts = lax.axis_size("sp")
    groups = lax.axis_size("tp")
    share = cotangent.shape[1] // groups
    home_rows, grad_first, grad_third, grad_second, table = expert_blocks(
        jnp.transpose(expert_ids),
        jnp.transpose(route_weight),
        mixer_out,
        cotangent,
        gate_weight[0],
        up_weight[0],
        down_weight[0],
        experts,
        groups,
    )
    own_cotangent = lax.dynamic_slice_in_dim(
        cotangent, lax.axis_index("tp") * share, share, axis=1
    )
    result, grad_proj = tail_blocks(
        table.reshape(-1, table.shape[-1]),
        home_rows.reshape(-1, share),
        own_cotangent,
        saved_normalized,
        inverse_deviation[:, None],
        channel_norm_gain[None, :],
        taps,
        proj_weight,
        experts,
        groups,
    )
    return (
        result,
        grad_proj,
        grad_first[None],
        grad_third[None],
        grad_second[None],
    )


def solution(mesh):
    return jax.shard_map(
        shards,
        mesh=mesh,
        in_specs=(
            P("sp", None),
            P("sp", None),
            P("sp", None),
            P("sp", None),
            P("sp", "tp"),
            P("sp"),
            P("tp"),
            P(None, "tp"),
            P("tp", None),
            P("sp", None, "tp"),
            P("sp", None, "tp"),
            P("sp", "tp", None),
        ),
        out_specs=(
            P("sp", "tp"),
            P("sp", "tp"),
            P("sp", None, "tp"),
            P("sp", None, "tp"),
            P("sp", "tp", None),
        ),
        check_vma=False,
    )
```

```python
import functools

import jax
import jax.numpy as jnp
from jax import lax
from jax.experimental import pallas as pl
from jax.experimental.pallas import tpu as pltpu
from jax.sharding import PartitionSpec as P


def remote(source, target, send_sem, recv_sem, device):
    return pltpu.make_async_remote_copy(
        src_ref=source,
        dst_ref=target,
        send_sem=send_sem,
        recv_sem=recv_sem,
        device_id=device,
        device_id_type=pl.DeviceIdType.MESH,
    )


CONTRACT_LAST = (((1,), (1,)), ((), ()))
CONTRACT_FIRST = (((0,), (0,)), ((), ()))


def expert_kernel(
    experts, groups, ids_far, route_far, mixer_far, cotangent_far, gate_far, up_far, down_far,
    home, grad_gate, grad_up, grad_down, table,
    ids, route, mixer, cotangent, rows, grads, sent_rows, sent_grads, gate, up, down, hidden_gate, hidden_up, active,
    grad_hg, grad_hu, partial, pair_in, row_out, row_in, total, slot_weight, *sems
):
    (load_sem, far_send, far_recv, row_send, row_recv, pair_send, pair_recv,
     home_send, home_recv, sum_send, sum_recv, back_send, back_recv) = sems
    mine = lax.axis_index("sp")
    place = lax.axis_index("tp")
    chips = groups // 2
    chip, core = place // 2, place % 2
    sibling = chip * 2 + 1 - core
    tok = mixer.shape[0]
    capacity, share = rows.shape[2:]
    slots = experts * capacity
    ff = gate.shape[1]
    middle = experts // 2
    sent = (sent_rows, sent_grads)
    held = (rows, grads)

    def at_chip(step):
        return ((chip + step) % chips) * 2 + core

    loads = [
        pltpu.make_async_copy(source, target, load_sem.at[at])
        for at, (source, target) in enumerate(
            (
                (ids_far, ids), (route_far, route), (mixer_far, mixer), (cotangent_far, cotangent),
                (gate_far, gate), (up_far, up), (down_far, down),
            )
        )
    ]
    for load in loads:
        load.start()
    barrier = pltpu.get_barrier_semaphore()

    def greet(step, carry):
        pl.semaphore_signal(barrier, inc=1, device_id=((mine + step) % experts, place),
                            device_id_type=pl.DeviceIdType.MESH)
        return carry

    lax.fori_loop(1, experts, greet, 0)
    for step in range(1, chips):
        pl.semaphore_signal(barrier, inc=1, device_id=(mine, at_chip(step)),
                            device_id_type=pl.DeviceIdType.MESH)
    pl.semaphore_signal(barrier, inc=1, device_id=(mine, sibling),
                        device_id_type=pl.DeviceIdType.MESH)

    loads[0].wait()
    loads[1].wait()
    expert = lax.broadcasted_iota(jnp.int32, (experts, tok), 0)
    hot = [(ids[k : k + 1] == expert).astype(jnp.float32) for k in range(ids.shape[0])]
    before = lax.broadcasted_iota(jnp.int32, (tok, tok), 0)
    after = lax.broadcasted_iota(jnp.int32, (tok, tok), 1)
    rank = jnp.dot(
        sum(hot).astype(jnp.bfloat16),
        (before < after).astype(jnp.float32).astype(jnp.bfloat16),
        preferred_element_type=jnp.float32,
    )
    slot = expert.astype(jnp.float32) * capacity + rank
    number = lax.broadcasted_iota(jnp.int32, (slots, tok), 0).astype(jnp.float32)
    chosen = jnp.zeros((slots, tok), jnp.float32)
    weighted = jnp.zeros((slots, tok), jnp.float32)
    for k in range(ids.shape[0]):
        match = number == jnp.sum(hot[k] * slot, axis=0, keepdims=True)
        chosen = jnp.where(match, 1.0, chosen)
        weighted = jnp.where(match, route[k : k + 1], weighted)
    table[...] = chosen.astype(jnp.bfloat16).reshape(experts, capacity, tok)
    slot_weight[...] = jnp.sum(weighted, axis=1, keepdims=True).reshape(experts, capacity, 1)
    columns = pl.ds(pl.multiple_of(place * share, share), share)
    every = table[...].reshape(slots, tok)
    scale = slot_weight[...].reshape(slots, 1)
    loads[2].wait()
    sent_rows[...] = (
        jnp.dot(every, mixer[:, columns], preferred_element_type=jnp.float32)
        .astype(jnp.bfloat16).reshape(experts, capacity, share)
    )
    loads[3].wait()
    sent_grads[...] = (
        (scale * jnp.dot(every, cotangent[:, columns], preferred_element_type=jnp.float32))
        .astype(jnp.bfloat16).reshape(experts, capacity, share)
    )
    pl.semaphore_wait(barrier, experts - 1 + chips)

    def far(a, step):
        peer = (mine + step) % experts
        return remote(sent[a].at[peer], held[a].at[step, place],
                      far_send.at[a, step], far_recv.at[a, step], (peer, place))

    def row(a, step, hop):
        block = held[a].at[step, place]
        return remote(block, block, row_send.at[a, step, hop], row_recv.at[a, step, hop],
                      (mine, at_chip(hop)))

    def pair(a, step, hop):
        block = held[a].at[step, at_chip(chips - hop)]
        return remote(block, block, pair_send.at[a, step, hop], pair_recv.at[a, step, hop],
                      (mine, sibling))

    for a in range(2):
        def start_far(step, carry, a=a):
            far(a, step).start()
            return carry

        lax.fori_loop(1, experts, start_far, 0)

    own = table[mine]
    own_scale = slot_weight[mine]
    for g in range(groups):
        span = slice(g * share, (g + 1) * share)
        rows[0, g] = jnp.dot(
            own, mixer[:, span], preferred_element_type=jnp.float32
        ).astype(jnp.bfloat16)
        grads[0, g] = (
            own_scale * jnp.dot(own, cotangent[:, span], preferred_element_type=jnp.float32)
        ).astype(jnp.bfloat16)

    def each(low, high, act):
        def body(step, carry):
            act(step)
            return carry

        lax.fori_loop(low, high, body, 0)

    def service(a, step):
        far(a, step).wait_recv()
        for hop in range(1, chips):
            row(a, step, hop).start()
        pair(a, step, 0).start()

    def settle(a, step):
        for hop in range(1, chips):
            row(a, step, hop).wait_recv()
            pair(a, step, hop).start()

    def complete(a, step):
        for hop in range(chips):
            pair(a, step, hop).wait_recv()

    def both(a):
        def act(step):
            service(a, step)
            settle(a, step - 2)
        return act

    def chunk(ref, at, g):
        return ref[at * middle : (at + 1) * middle, g].reshape(middle * capacity, share)

    def lines(at):
        return slice(at * middle * capacity, (at + 1) * middle * capacity)

    def ahead(at):
        for weight, result in ((gate, hidden_gate), (up, hidden_up)):
            value = None
            for g in range(groups):
                term = jnp.dot(
                    chunk(rows, at, g), weight[g * share : (g + 1) * share, :],
                    preferred_element_type=jnp.float32,
                )
                value = term if value is None else value + term
            result[lines(at), :] = value

    def back(at):
        value = None
        for g in range(groups):
            term = lax.dot_general(
                chunk(grads, at, g), down[:, g * share : (g + 1) * share], CONTRACT_LAST,
                preferred_element_type=jnp.float32,
            )
            value = term if value is None else value + term
        hg = hidden_gate[lines(at), :]
        hu = hidden_up[lines(at), :]
        sigma = sigmoid(hg)
        swish = hg * sigma
        active[lines(at), :] = (swish * hu).astype(jnp.bfloat16)
        grad_hg[lines(at), :] = (value * hu * sigma * (1.0 + hg * (1.0 - sigma))).astype(jnp.bfloat16)
        grad_hu[lines(at), :] = (value * swish).astype(jnp.bfloat16)
        for g in range(groups):
            term = lax.dot_general(
                grad_hg[lines(at), :], gate[g * share : (g + 1) * share, :], CONTRACT_LAST,
                preferred_element_type=jnp.float32,
            ) + lax.dot_general(
                grad_hu[lines(at), :], up[g * share : (g + 1) * share, :], CONTRACT_LAST,
                preferred_element_type=jnp.float32,
            )
            partial[g, at * middle : (at + 1) * middle] = term.astype(jnp.bfloat16).reshape(
                middle, capacity, share
            )

    def weight_grads(g):
        span = pl.ds(pl.multiple_of(g * share, share), share)
        left = rows[:, g].reshape(slots, share)
        grad_gate[span, :] = lax.dot_general(
            left, grad_hg[...], CONTRACT_FIRST, preferred_element_type=jnp.float32
        ).astype(jnp.bfloat16)
        grad_up[span, :] = lax.dot_general(
            left, grad_hu[...], CONTRACT_FIRST, preferred_element_type=jnp.float32
        ).astype(jnp.bfloat16)
        grad_down[:, span] = lax.dot_general(
            active[...], grads[:, g].reshape(slots, share), CONTRACT_FIRST,
            preferred_element_type=jnp.float32,
        ).astype(jnp.bfloat16)

    def home_pair(step, hop):
        other = ((chip + hop) % chips) * 2 + 1 - core
        return remote(partial.at[other, step], pair_in.at[hop, step],
                      home_send.at[step, hop], home_recv.at[step, hop], (mine, sibling))

    def home_row(step, hop):
        return remote(row_out.at[hop, step], row_in.at[hop, step],
                      sum_send.at[step, hop], sum_recv.at[step, hop], (mine, at_chip(hop)))

    def home_far(step):
        owner = (mine + experts - step) % experts
        return remote(total.at[step], home.at[mine],
                      back_send.at[step], back_recv.at[step], (owner, place))

    def start_pair(step):
        for hop in reversed(range(chips)):
            home_pair(step, hop).start()

    def add_pair(step, hop):
        home_pair(step, hop).wait_recv()
        return partial[at_chip(hop), step].astype(jnp.float32) + pair_in[hop, step].astype(
            jnp.float32
        )

    def send_rows(step):
        for hop in range(1, chips):
            row_out[hop, step] = add_pair(step, hop).astype(row_out.dtype)
            home_row(step, hop).start()

    def add_rows(step):
        value = add_pair(step, 0)
        for hop in range(1, chips):
            home_row(step, hop).wait_recv()
            value = value + row_in[hop, step].astype(jnp.float32)
        return value.astype(total.dtype)

    def send_home(step):
        total[step] = add_rows(step)
        home_far(step).start()

    each(1, 3, functools.partial(service, 0))
    each(3, experts, both(0))
    service(1, 1)
    settle(0, experts - 2)
    service(1, 2)
    settle(0, experts - 1)
    loads[4].wait()
    loads[5].wait()
    each(1, middle, functools.partial(complete, 0))
    ahead(0)
    each(3, middle + 1, both(1))
    each(middle, experts, functools.partial(complete, 0))
    ahead(1)
    each(middle + 1, middle + 2, both(1))
    loads[6].wait()
    each(1, middle, functools.partial(complete, 1))
    back(0)
    each(0, middle, start_pair)
    each(middle + 2, experts, both(1))
    settle(1, experts - 2)
    settle(1, experts - 1)
    each(0, middle, send_rows)
    each(middle, experts, functools.partial(complete, 1))
    back(1)
    each(middle, experts, start_pair)
    weight_grads(0)
    home[mine] = add_rows(0)
    each(1, middle, send_home)
    each(middle, experts, send_rows)
    each(1, groups - 1, weight_grads)
    each(middle, experts, send_home)
    weight_grads(groups - 1)

    def finish(step):
        for hop in range(chips):
            home_pair(step, hop).wait_send()
            if hop:
                home_row(step, hop).wait_send()

    def finish_far(step):
        home_far(step).wait()
        for a in range(2):
            far(a, step).wait_send()
            for hop in range(chips):
                pair(a, step, hop).wait_send()
                if hop:
                    row(a, step, hop).wait_send()

    each(0, experts, finish)
    each(1, experts, finish_far)


def expert_blocks(ids, route, mixer, cotangent, gate, up, down, experts, groups):
    tok, width = mixer.shape
    ff = gate.shape[1]
    share = width // groups
    capacity = groups * max(1, 4 * tok // (experts * groups))
    chips = groups // 2
    slots = experts * capacity
    half = jnp.bfloat16
    dma = pltpu.SemaphoreType.DMA
    vmem = pl.BlockSpec(memory_space=pltpu.VMEM)
    held = pltpu.VMEM((experts, groups, capacity, share), half)
    sent = pltpu.VMEM((experts, capacity, share), half)
    blocks = pltpu.VMEM((chips, experts, capacity, share), half)
    return pl.pallas_call(
        functools.partial(expert_kernel, experts, groups),
        out_shape=(
            jax.ShapeDtypeStruct((experts, capacity, share), half),
            jax.ShapeDtypeStruct(gate.shape, half),
            jax.ShapeDtypeStruct(up.shape, half),
            jax.ShapeDtypeStruct(down.shape, half),
            jax.ShapeDtypeStruct((experts, capacity, tok), half),
        ),
        in_specs=[pl.BlockSpec(memory_space=pltpu.HBM)] * 7,
        out_specs=[vmem] * 5,
        scratch_shapes=[pltpu.VMEM(array.shape, array.dtype) for array in (ids, route, mixer, cotangent)]
        + [held] * 2
        + [sent] * 2
        + [pltpu.VMEM(array.shape, half) for array in (gate, up, down)]
        + [pltpu.VMEM((slots, ff), jnp.float32)] * 2
        + [pltpu.VMEM((slots, ff), half)] * 3
        + [pltpu.VMEM((groups, experts, capacity, share), half)]
        + [blocks] * 3
        + [sent, pltpu.VMEM((experts, capacity, 1), jnp.float32)]
        + [dma((7,))]
        + [dma((2, experts))] * 2
        + [dma((2, experts, chips))] * 4
        + [dma((experts, chips))] * 4
        + [dma((experts,))] * 2,
        compiler_params=pltpu.CompilerParams(
            collective_id=0, has_side_effects=True, vmem_limit_bytes=36 * 2**20
        ),
        cost_estimate=pl.CostEstimate(flops=10**10, bytes_accessed=10**7, transcendentals=0),
    )(
        *(
            pltpu.with_memory_space_constraint(array, pltpu.HBM)
            for array in (ids, route, mixer, cotangent, gate, up, down)
        )
    )


def line_width(experts):
    width = 1
    while 4 * width * width <= experts and experts % (2 * width) == 0:
        width = 2 * width
    return width


def sigmoid(value):
    return 1.0 / (1.0 + jnp.exp(-value))


def tail_kernel(
    experts, groups, lead, table, home, cotangent_far, saved, inverse, gain, weight,
    every, acts, extended, cotangent, blocks, sums, load_sem, *sems
):
    (row_send, row_recv, pair_send, pair_recv, far_send, far_recv, half_send, half_recv,
     line_send, line_recv, side_send, side_recv, sum_send, sum_recv, halo_send, halo_recv) = sems
    mine = lax.axis_index("sp")
    place = lax.axis_index("tp")
    chips = groups // 2
    chip, core = place // 2, place % 2
    sibling = chip * 2 + 1 - core
    across = experts // lead
    line, side = mine // lead, mine % lead
    tok = saved.shape[0]
    channels = saved.shape[1]
    width = blocks.shape[-1]
    per = experts // groups
    half = tok // 2

    def at_chip(step):
        return ((chip + step) % chips) * 2 + core

    part_width = cotangent.shape[1]
    load = pltpu.make_async_copy(
        cotangent_far.at[:, pl.ds(pl.multiple_of(place * part_width, part_width), part_width)],
        cotangent, load_sem,
    )
    load.start()
    barrier = pltpu.get_barrier_semaphore()

    def greet(step, carry):
        pl.semaphore_signal(barrier, inc=1, device_id=((mine + step) % experts, place),
                            device_id_type=pl.DeviceIdType.MESH)
        return carry

    def greet_group(step, carry):
        pl.semaphore_signal(barrier, inc=1, device_id=(mine, (place + step) % groups),
                            device_id_type=pl.DeviceIdType.MESH)
        return carry

    lax.fori_loop(1, experts, greet, 0)
    lax.fori_loop(1, groups, greet_group, 0)
    normalized = saved[...].astype(jnp.float32)
    scaled = normalized * gain[...]
    gate = sigmoid(scaled)
    acts[mine] = (scaled * gate).astype(jnp.bfloat16)
    pl.semaphore_wait(barrier, experts + groups - 2)

    def along(step):
        return remote(acts.at[mine], acts.at[mine], line_send.at[step], line_recv.at[step],
                      (((line + step) % across) * lead + side, place))

    def arrived(step):
        source = ((line + across - step) % across) * lead + side
        return remote(acts.at[source], acts.at[source], line_send.at[step], line_recv.at[step],
                      (((line + step) % across) * lead + side, place))

    def beside(step, hop):
        source = ((line + across - step) % across) * lead + side
        return remote(acts.at[source], acts.at[source], side_send.at[step, hop],
                      side_recv.at[step, hop], (line * lead + (side + hop) % lead, place))

    def share_at(owner):
        return blocks.at[pl.ds(owner * per, per)]

    def row(hop):
        return remote(share_at(place), share_at(place), row_send.at[hop], row_recv.at[hop],
                      (mine, at_chip(hop)))

    def pair(hop):
        owner = at_chip(chips - hop)
        return remote(share_at(owner), share_at(owner), pair_send.at[hop], pair_recv.at[hop],
                      (mine, sibling))

    share = lax.dot_general(
        table[...], home[...], CONTRACT_FIRST, preferred_element_type=jnp.float32
    )
    load.wait()
    share = (share + cotangent[...].astype(jnp.float32)).astype(jnp.bfloat16)
    for part in range(per):
        piece = share[:, part * width : (part + 1) * width]
        blocks[place * per + part] = piece.reshape(2, half, width)
    for hop in range(1, chips):
        row(hop).start()
    pair(0).start()
    for step in range(1, across):
        along(step).start()
    for hop in range(1, lead):
        beside(0, hop).start()
    for hop in range(1, chips):
        row(hop).wait_recv()
        pair(hop).start()
    for hop in range(chips):
        pair(hop).wait_recv()

    def far(step):
        peer = (mine + step) % experts
        return remote(blocks.at[peer, core], every.at[mine, core], far_send.at[step],
                      far_recv.at[step], (peer, place))

    def to_half(step):
        source = (mine + experts - step) % experts
        return remote(every.at[source, core], every.at[source, core], half_send.at[step],
                      half_recv.at[step], (mine, sibling))

    def start_far(step, carry):
        far(step).start()
        return carry

    lax.fori_loop(1, experts, start_far, 0)
    every[mine] = blocks[mine]

    grad = jnp.zeros((tok, channels), jnp.float32)
    for part in range(experts):
        grad = grad + lax.dot_general(
            blocks[part].reshape(tok, width),
            weight[:, part * width : (part + 1) * width],
            (((1,), (1,)), ((), ())),
            preferred_element_type=jnp.float32,
        )
    normalized = saved[...].astype(jnp.float32)
    scaled = normalized * gain[...]
    gate = sigmoid(scaled)
    grad = grad * gate * (1.0 + scaled * (1.0 - gate)) * gain[...]
    lanes = min(channels, 128)
    first = jnp.zeros((tok, lanes), jnp.float32)
    second = jnp.zeros((tok, lanes), jnp.float32)
    for at in range(0, channels, lanes):
        first = first + grad[:, at : at + lanes]
        second = second + grad[:, at : at + lanes] * normalized[:, at : at + lanes]
    sums[place, 0] = jnp.sum(jnp.transpose(first).reshape(lanes // 8, 8, tok), axis=0)
    sums[place, 1] = jnp.sum(jnp.transpose(second).reshape(lanes // 8, 8, tok), axis=0)

    def tell(step):
        return remote(sums.at[place], sums.at[place], sum_send.at[step], sum_recv.at[step],
                      (mine, (place + step) % groups))

    def start_tell(step, carry):
        tell(step).start()
        return carry

    def wait_tell(step, carry):
        tell(step).wait()
        return carry

    lax.fori_loop(1, groups, start_tell, 0)
    for step in range(1, across - 1):
        arrived(step).wait_recv()
        for hop in range(1, lead):
            beside(step, hop).start()
    lax.fori_loop(1, groups, wait_tell, 0)
    count = channels * groups
    total = jnp.sum(sums[...], axis=0)

    def column(kind):
        flat = jnp.sum(total[kind], axis=0, keepdims=True) / count
        return jnp.transpose(jnp.broadcast_to(flat, (lanes, tok)))

    mean, slope = column(0), column(1)
    deviation = jnp.transpose(jnp.broadcast_to(inverse[...], (lanes, tok)))
    for at in range(0, channels, lanes):
        extended[at // lanes, 0:tok] = deviation * (
            grad[:, at : at + lanes] - mean - normalized[:, at : at + lanes] * slope
        )
    reach = extended.shape[1] - tok

    def halo():
        return remote(extended.at[:, pl.ds(0, reach)], extended.at[:, pl.ds(tok, reach)],
                      halo_send, halo_recv, ((mine + experts - 1) % experts, place))

    @pl.when(mine > 0)
    def _():
        halo().start()

    @pl.when(mine == experts - 1)
    def _():
        extended[:, tok : tok + reach] = jnp.zeros((channels // lanes, reach, lanes), jnp.float32)

    arrived(across - 1).wait_recv()
    for hop in range(1, lead):
        beside(across - 1, hop).start()

    def forward(step, carry):
        far(step).wait_recv()
        to_half(step).start()
        return carry

    lax.fori_loop(1, experts, forward, 0)

    @pl.when(mine < experts - 1)
    def _():
        halo().wait_recv()

    def arrive(step, carry):
        to_half(step).wait_recv()
        return carry

    lax.fori_loop(1, experts, arrive, 0)
    for step in range(across):
        for hop in range(1, lead):
            beside(step, hop).wait_recv()
    @pl.when(mine > 0)
    def _():
        halo().wait_send()

    for hop in range(chips):
        pair(hop).wait_send()
        if hop:
            row(hop).wait_send()
    for step in range(across):
        if step:
            along(step).wait_send()
        for hop in range(1, lead):
            beside(step, hop).wait_send()

    def finish(step, carry):
        far(step).wait_send()
        to_half(step).wait_send()
        return carry

    lax.fori_loop(1, experts, finish, 0)


def tail_blocks(table, home, cotangent, saved, inverse, gain, weight, reach, experts, groups):
    tok, channels = saved.shape
    model_width = weight.shape[1]
    width = model_width // experts
    lead = line_width(experts)
    across = experts // lead
    lanes = min(channels, 128)
    dma = pltpu.SemaphoreType.DMA
    vmem = pl.BlockSpec(memory_space=pltpu.VMEM)
    return pl.pallas_call(
        functools.partial(tail_kernel, experts, groups, lead),
        out_shape=(
            jax.ShapeDtypeStruct((experts, 2, tok // 2, width), jnp.bfloat16),
            jax.ShapeDtypeStruct((experts, tok, channels), jnp.bfloat16),
            jax.ShapeDtypeStruct((channels // lanes, tok + reach, lanes), jnp.float32),
        ),
        in_specs=[vmem] * 2 + [pl.BlockSpec(memory_space=pltpu.HBM)] + [vmem] * 4,
        out_specs=[vmem] * 3,
        scratch_shapes=[
            pltpu.VMEM((tok, model_width // groups), jnp.bfloat16),
            pltpu.VMEM((experts, 2, tok // 2, width), jnp.bfloat16),
            pltpu.VMEM((groups, 2, 8, tok), jnp.float32),
            dma,
        ]
        + [dma((groups // 2,))] * 4
        + [dma((experts,))] * 4
        + [dma((across,))] * 2
        + [dma((across, lead))] * 2
        + [dma((groups,))] * 2
        + [dma] * 2,
        compiler_params=pltpu.CompilerParams(
            collective_id=2, has_side_effects=True, vmem_limit_bytes=16 * 2**20
        ),
        cost_estimate=pl.CostEstimate(
            flops=10**9, bytes_accessed=10**7, transcendentals=0
        ),
    )(
        table, home, pltpu.with_memory_space_constraint(cotangent, pltpu.HBM), saved, inverse,
        gain, weight,
    )


def last_kernel(
    every, acts, extended, taps, gate, up, down, result_far, proj_far, gate_far, up_far, down_far,
    result, proj, sems
):
    stores = [
        pltpu.make_async_copy(source, target, sems.at[at])
        for at, (source, target) in enumerate(
            (
                (gate, gate_far), (up, up_far), (down, down_far), (result, result_far),
                (proj, proj_far),
            )
        )
    ]
    for store in stores[:3]:
        store.start()
    tok, channels = result.shape
    lanes = extended.shape[-1]
    for at in range(0, channels, lanes):
        value = jnp.zeros((tok, lanes), jnp.float32)
        for tap in range(taps.shape[0]):
            value = value + taps[tap : tap + 1, at : at + lanes] * extended[at // lanes, tap : tap + tok]
        result[:, at : at + lanes] = value.astype(result.dtype)
    stores[3].start()
    proj[...] = lax.dot_general(
        every[...].reshape(-1, every.shape[-1]),
        acts[...].reshape(-1, channels),
        CONTRACT_FIRST,
        preferred_element_type=jnp.float32,
    )
    stores[4].start()
    for store in stores:
        store.wait()


def last_blocks(every, acts, extended, taps, gate, up, down):
    tok, channels = acts.shape[1:]
    vmem = pl.BlockSpec(memory_space=pltpu.VMEM)
    shapes = (
        jax.ShapeDtypeStruct((tok, channels), jnp.bfloat16),
        jax.ShapeDtypeStruct((every.shape[-1], channels), jnp.float32),
    )
    return pl.pallas_call(
        last_kernel,
        out_shape=shapes
        + tuple(jax.ShapeDtypeStruct(array.shape, array.dtype) for array in (gate, up, down)),
        in_specs=[vmem] * 7,
        out_specs=[pl.BlockSpec(memory_space=pltpu.HBM)] * 5,
        scratch_shapes=[pltpu.VMEM(shape.shape, shape.dtype) for shape in shapes]
        + [pltpu.SemaphoreType.DMA((5,))],
        compiler_params=pltpu.CompilerParams(vmem_limit_bytes=16 * 2**20),
        cost_estimate=pl.CostEstimate(flops=10**9, bytes_accessed=10**7, transcendentals=0),
    )(every, acts, extended, taps, gate, up, down)


def shards(
    cotangent,
    mixer_out,
    expert_ids,
    route_weight,
    saved_normalized,
    inverse_deviation,
    channel_norm_gain,
    taps,
    proj_weight,
    gate_weight,
    up_weight,
    down_weight,
):
    experts = lax.axis_size("sp")
    groups = lax.axis_size("tp")
    share = cotangent.shape[1] // groups
    home_rows, grad_first, grad_third, grad_second, table = expert_blocks(
        jnp.transpose(expert_ids),
        jnp.transpose(route_weight),
        mixer_out,
        cotangent,
        gate_weight[0],
        up_weight[0],
        down_weight[0],
        experts,
        groups,
    )
    every, acts, extended = tail_blocks(
        table.reshape(-1, table.shape[-1]),
        home_rows.reshape(-1, share),
        cotangent,
        saved_normalized,
        inverse_deviation[None, :],
        channel_norm_gain[None, :],
        proj_weight,
        (taps.shape[0] + 6) // 8 * 8,
        experts,
        groups,
    )
    result, grad_proj, grad_first, grad_third, grad_second = last_blocks(
        every, acts, extended, taps, grad_first, grad_third, grad_second
    )
    return (
        result,
        grad_proj,
        grad_first[None],
        grad_third[None],
        grad_second[None],
    )


def solution(mesh):
    return jax.shard_map(
        shards,
        mesh=mesh,
        in_specs=(
            P("sp", None),
            P("sp", None),
            P("sp", None),
            P("sp", None),
            P("sp", "tp"),
            P("sp"),
            P("tp"),
            P(None, "tp"),
            P("tp", None),
            P("sp", None, "tp"),
            P("sp", None, "tp"),
            P("sp", "tp", None),
        ),
        out_specs=(
            P("sp", "tp"),
            P("sp", "tp"),
            P("sp", None, "tp"),
            P("sp", None, "tp"),
            P("sp", "tp", None),
        ),
        check_vma=False,
    )
```

```python
import functools

import jax
import jax.numpy as jnp
from jax import lax
from jax.experimental import pallas as pl
from jax.experimental.pallas import tpu as pltpu
from jax.sharding import PartitionSpec as P


def line_width(experts):
    width = 1
    while 4 * width * width <= experts and experts % (2 * width) == 0:
        width = 2 * width
    return width


def sigmoid(value):
    return 1.0 / (1.0 + jnp.exp(-value))


def mate(index, step, count):
    if count & (count - 1):
        raise ValueError("count")
    value, bit = 0, 1
    while bit < count:
        value = value + bit * ((index // bit + step // bit) % 2)
        bit = 2 * bit
    return value


def remote(source, target, send_sem, recv_sem, device):
    return pltpu.make_async_remote_copy(
        src_ref=source,
        dst_ref=target,
        send_sem=send_sem,
        recv_sem=recv_sem,
        device_id=device,
        device_id_type=pl.DeviceIdType.MESH,
    )


CONTRACT_LAST = (((1,), (1,)), ((), ()))
CONTRACT_FIRST = (((0,), (0,)), ((), ()))


def expert_kernel(
    experts, groups, lead, ids_far, route_far, mixer_far, cotangent_far, gate_far, up_far, down_far,
    saved_far, gain_far, weight_far, inverse_far, grad_gate, grad_up, grad_down, acts, crossed,
    every, extended, ids, route, mixer, cotangent, saved, gain, weight, inverse, home, table,
    blocks, sums, held, sent, gate, up, down, hidden_gate, hidden_up, active,
    grad_hg, grad_hu, partial, pair_in, row_out, row_in, total, slot_weight, *sems
):
    (load_sem, far_send, far_recv, row_send, row_recv, pair_send, pair_recv,
     home_send, home_recv, sum_send, sum_recv, back_send, back_recv,
     line_send, line_recv, side_send, side_recv) = sems[:17]
    mine = lax.axis_index("sp")
    place = lax.axis_index("tp")
    chips = groups // 2
    chip, core = place // 2, place % 2
    sibling = chip * 2 + 1 - core
    tok = mixer.shape[0]
    capacity, share = held.shape[3:]
    slots = experts * capacity

    def at_chip(step):
        return ((chip + step) % chips) * 2 + core

    loads = [
        pltpu.make_async_copy(source, target, load_sem.at[at])
        for at, (source, target) in enumerate(
            (
                (ids_far, ids), (route_far, route), (mixer_far, mixer), (cotangent_far, cotangent),
                (gate_far, gate), (up_far, up), (down_far, down), (saved_far, saved),
                (gain_far, gain), (weight_far, weight), (inverse_far, inverse),
            )
        )
    ]
    for load in loads:
        load.start()
    barrier = pltpu.get_barrier_semaphore()

    def greet(step, carry):
        pl.semaphore_signal(barrier, inc=1, device_id=((mine + step) % experts, place),
                            device_id_type=pl.DeviceIdType.MESH)
        return carry

    lax.fori_loop(1, experts, greet, 0)

    def greet_group(step, carry):
        pl.semaphore_signal(barrier, inc=1, device_id=(mine, (place + step) % groups),
                            device_id_type=pl.DeviceIdType.MESH)
        return carry

    lax.fori_loop(1, groups, greet_group, 0)
    loads[0].wait()
    loads[1].wait()
    expert = lax.broadcasted_iota(jnp.int32, (experts, tok), 0)
    hot = [(ids[k : k + 1] == expert).astype(jnp.float32) for k in range(ids.shape[0])]
    before = lax.broadcasted_iota(jnp.int32, (tok, tok), 0)
    after = lax.broadcasted_iota(jnp.int32, (tok, tok), 1)
    rank = jnp.dot(
        sum(hot).astype(jnp.bfloat16),
        (before < after).astype(jnp.float32).astype(jnp.bfloat16),
        preferred_element_type=jnp.float32,
    )
    slot = expert.astype(jnp.float32) * capacity + rank
    number = lax.broadcasted_iota(jnp.int32, (slots, tok), 0).astype(jnp.float32)
    chosen = jnp.zeros((slots, tok), jnp.float32)
    weighted = jnp.zeros((slots, tok), jnp.float32)
    for k in range(ids.shape[0]):
        match = number == jnp.sum(hot[k] * slot, axis=0, keepdims=True)
        chosen = jnp.where(match, 1.0, chosen)
        weighted = jnp.where(match, route[k : k + 1], weighted)
    table[...] = chosen.astype(jnp.bfloat16).reshape(experts, capacity, tok)
    slot_weight[...] = jnp.sum(weighted, axis=1, keepdims=True).reshape(experts, capacity, 1)
    columns = pl.ds(pl.multiple_of(place * share, share), share)
    whole = table[...].reshape(slots, tok)
    scale = slot_weight[...].reshape(slots, 1)
    loads[2].wait()
    sent[:, 0] = (
        jnp.dot(whole, mixer[:, columns], preferred_element_type=jnp.float32)
        .astype(jnp.bfloat16).reshape(experts, capacity, share)
    )
    loads[3].wait()
    sent[:, 1] = (
        (scale * jnp.dot(whole, cotangent[:, columns], preferred_element_type=jnp.float32))
        .astype(jnp.bfloat16).reshape(experts, capacity, share)
    )
    pl.semaphore_wait(barrier, experts + groups - 2)

    def far(step):
        peer = mate(mine, step, experts)
        return remote(sent.at[peer], held.at[step, place],
                      far_send.at[step], far_recv.at[step], (peer, place))

    def row(step, hop):
        block = held.at[step, place]
        return remote(block, block, row_send.at[step, hop], row_recv.at[step, hop],
                      (mine, at_chip(hop)))

    def pair(step, hop):
        block = held.at[step, at_chip(chips - hop)]
        return remote(block, block, pair_send.at[step, hop], pair_recv.at[step, hop],
                      (mine, sibling))

    def each(low, high, act):
        def body(step, carry):
            act(step)
            return carry

        lax.fori_loop(low, high, body, 0)

    each(1, experts, lambda step: far(step).start())
    own = table[mine]
    own_scale = slot_weight[mine]
    for g in range(groups):
        span = slice(g * share, (g + 1) * share)
        held[0, g, 0] = jnp.dot(
            own, mixer[:, span], preferred_element_type=jnp.float32
        ).astype(jnp.bfloat16)
        held[0, g, 1] = (
            own_scale * jnp.dot(own, cotangent[:, span], preferred_element_type=jnp.float32)
        ).astype(jnp.bfloat16)

    across = experts // lead
    line, side = mine // lead, mine % lead

    def along(step, bit):
        peer = mate(line, bit, across) * lead + side
        return remote(acts.at[step], acts.at[step + bit], line_send.at[step + bit],
                      line_recv.at[step + bit], (peer, place))

    acts_order = sorted(range(1, across), key=lambda step: -(step & -step))

    def spread(step):
        bit = 1
        while bit < across:
            if step % (2 * bit) == 0:
                along(step, bit).start()
            bit = 2 * bit

    def reached(step):
        bit = 1
        while step % (2 * bit) == 0:
            bit = 2 * bit
        return along(step - bit, bit)

    def beside(step, hop):
        return remote(acts.at[step], crossed.at[hop - 1, step], side_send.at[step, hop],
                      side_recv.at[step, hop], (line * lead + mate(side, hop, lead), place))

    def cross(step):
        for hop in range(1, lead):
            beside(step, hop).start()

    def extend(step):
        reached(step).wait_recv()
        spread(step)

    def early_acts():
        spread(0)
        cross(0)

    def relay_acts():
        for step in acts_order:
            if step & (step - 1) == 0 and step > 1:
                extend(step)

    def later_acts():
        for step in acts_order:
            if step & (step - 1) or step == 1:
                extend(step)
            cross(step)

    def finish_acts():
        for step in range(1, across):
            reached(step).wait_send()
        for step in range(across):
            for hop in range(1, lead):
                beside(step, hop).wait()

    loads[7].wait()
    loads[8].wait()
    scaled = saved[...].astype(jnp.float32) * gain[...]
    acts[0] = (scaled * sigmoid(scaled)).astype(jnp.bfloat16)

    def service(step):
        far(step).wait_recv()
        for hop in range(1, chips):
            row(step, hop).start()
        pair(step, 0).start()

    def settle(step):
        for hop in range(1, chips):
            row(step, hop).wait_recv()
            pair(step, hop).start()

    def complete(step):
        for hop in range(chips):
            pair(step, hop).wait_recv()

    def chunk(kind, low, high, g):
        return held[low:high, g, kind].reshape((high - low) * capacity, share)

    def ahead(low, high):
        lines = slice(low * capacity, high * capacity)
        for matrix, result in ((gate, hidden_gate), (up, hidden_up)):
            value = None
            for g in range(groups):
                term = jnp.dot(
                    chunk(0, low, high, g), matrix[g * share : (g + 1) * share, :],
                    preferred_element_type=jnp.float32,
                )
                value = term if value is None else value + term
            result[lines, :] = value

    def back(low, high):
        lines = slice(low * capacity, high * capacity)
        value = None
        for g in range(groups):
            term = lax.dot_general(
                chunk(1, low, high, g), down[:, g * share : (g + 1) * share], CONTRACT_LAST,
                preferred_element_type=jnp.float32,
            )
            value = term if value is None else value + term
        hg = hidden_gate[lines, :]
        hu = hidden_up[lines, :]
        sigma = sigmoid(hg)
        swish = hg * sigma
        active[lines, :] = (swish * hu).astype(jnp.bfloat16)
        grad_hg[lines, :] = (value * hu * sigma * (1.0 + hg * (1.0 - sigma))).astype(jnp.bfloat16)
        grad_hu[lines, :] = (value * swish).astype(jnp.bfloat16)
        for g in range(groups):
            term = lax.dot_general(
                grad_hg[lines, :], gate[g * share : (g + 1) * share, :], CONTRACT_LAST,
                preferred_element_type=jnp.float32,
            ) + lax.dot_general(
                grad_hu[lines, :], up[g * share : (g + 1) * share, :], CONTRACT_LAST,
                preferred_element_type=jnp.float32,
            )
            partial[g, low:high] = term.astype(jnp.bfloat16).reshape(high - low, capacity, share)

    def weight_grads(g):
        span = pl.ds(pl.multiple_of(g * share, share), share)
        left = held[:, g, 0].reshape(slots, share)
        grad_gate[span, :] = lax.dot_general(
            left, grad_hg[...], CONTRACT_FIRST, preferred_element_type=jnp.float32
        ).astype(jnp.bfloat16)
        grad_up[span, :] = lax.dot_general(
            left, grad_hu[...], CONTRACT_FIRST, preferred_element_type=jnp.float32
        ).astype(jnp.bfloat16)
        grad_down[:, span] = lax.dot_general(
            active[...], held[:, g, 1].reshape(slots, share), CONTRACT_FIRST,
            preferred_element_type=jnp.float32,
        ).astype(jnp.bfloat16)

    def home_pair(step, hop):
        other = ((chip + hop) % chips) * 2 + 1 - core
        return remote(partial.at[other, step], pair_in.at[hop, step],
                      home_send.at[step, hop], home_recv.at[step, hop], (mine, sibling))

    def home_row(step, hop):
        return remote(row_out.at[hop, step], row_in.at[hop, step],
                      sum_send.at[step, hop], sum_recv.at[step, hop], (mine, at_chip(hop)))

    def home_far(step):
        owner = mate(mine, step, experts)
        return remote(total.at[step], home.at[mine],
                      back_send.at[step], back_recv.at[step], (owner, place))

    def start_pair(step):
        for hop in reversed(range(chips)):
            home_pair(step, hop).start()

    def add_pair(step, hop):
        home_pair(step, hop).wait_recv()
        return partial[at_chip(hop), step].astype(jnp.float32) + pair_in[hop, step].astype(
            jnp.float32
        )

    def send_rows(step):
        for hop in range(1, chips):
            row_out[hop, step] = add_pair(step, hop).astype(row_out.dtype)
            home_row(step, hop).start()

    def add_rows(step):
        value = add_pair(step, 0)
        for hop in range(1, chips):
            home_row(step, hop).wait_recv()
            value = value + row_in[hop, step].astype(jnp.float32)
        return value.astype(total.dtype)

    def send_home(step):
        total[step] = add_rows(step)
        home_far(step).start()

    first, second = experts // 2, 3 * experts // 4
    each(1, first, service)
    each(1, first, settle)
    for load in loads[4:7]:
        load.wait()
    each(1, first, complete)
    ahead(0, first)
    each(first, first + 1, service)
    back(0, first)
    each(0, first, start_pair)
    each(first + 1, second, service)
    each(first, first + 1, settle)
    each(second, second + 1, service)
    each(first + 1, second, settle)
    early_acts()
    each(second + 1, experts, service)
    each(0, first, send_rows)
    each(first, second, complete)
    ahead(first, second)
    back(first, second)
    each(first, second, start_pair)
    each(second, experts, settle)
    each(first, second, send_rows)
    each(second, experts, complete)
    ahead(second, experts)
    back(second, experts)
    each(second, experts, start_pair)
    home[mine] = add_rows(0)
    each(first, second, send_home)
    each(second, experts, send_rows)
    each(1, first, send_home)
    weight_grads(0)
    relay_acts()
    each(1, groups - 1, weight_grads)
    each(second, experts, send_home)
    weight_grads(groups - 1)
    later_acts()

    def return_done(step):
        home_far(step).wait_recv()

    each(1, experts, return_done)
    loads[9].wait()
    loads[10].wait()
    tail_part(
        experts, groups, mine, place, table, home, cotangent[:, columns], saved, inverse, gain,
        weight, every, extended, blocks, sums, *sems[17:],
    )

    def finish(step):
        for hop in range(chips):
            home_pair(step, hop).wait_send()
            if hop:
                home_row(step, hop).wait_send()

    def finish_far(step):
        home_far(step).wait_send()
        far(step).wait_send()
        for hop in range(chips):
            pair(step, hop).wait_send()
            if hop:
                row(step, hop).wait_send()

    finish_acts()
    each(0, experts, finish)
    each(1, experts, finish_far)


def expert_blocks(
    ids, route, mixer, cotangent, gate, up, down, saved, gain, weight, inverse, reach, experts,
    groups,
):
    tok, width = mixer.shape
    ff = gate.shape[1]
    share = width // groups
    capacity = groups * max(1, 4 * tok // (experts * groups))
    chips = groups // 2
    slots = experts * capacity
    lead = line_width(experts)
    across = experts // lead
    half = jnp.bfloat16
    dma = pltpu.SemaphoreType.DMA
    vmem = pl.BlockSpec(memory_space=pltpu.VMEM)
    held = pltpu.VMEM((experts, groups, 2, capacity, share), half)
    sent = pltpu.VMEM((experts, 2, capacity, share), half)
    kept = pltpu.VMEM((experts, capacity, share), half)
    blocks = pltpu.VMEM((chips, experts, capacity, share), half)
    channels = saved.shape[1]
    lanes = min(channels, 128)
    columns = width // experts
    outs = tuple(jax.ShapeDtypeStruct(array.shape, half) for array in (gate, up, down)) + (
        jax.ShapeDtypeStruct((across,) + saved.shape, half),
        jax.ShapeDtypeStruct((lead - 1, across) + saved.shape, half),
        jax.ShapeDtypeStruct((experts, 2, tok // 2, columns), half),
        jax.ShapeDtypeStruct((channels // lanes, tok + reach, lanes), jnp.float32),
    )
    inputs = (ids, route, mixer, cotangent, gate, up, down, saved, gain, weight, inverse)
    return pl.pallas_call(
        functools.partial(expert_kernel, experts, groups, lead),
        out_shape=outs,
        in_specs=[pl.BlockSpec(memory_space=pltpu.HBM)] * len(inputs),
        out_specs=[vmem] * len(outs),
        scratch_shapes=[
            pltpu.VMEM(array.shape, array.dtype)
            for array in (ids, route, mixer, cotangent, saved, gain, weight, inverse)
        ]
        + [
            kept,
            pltpu.VMEM((experts, capacity, tok), half),
            pltpu.VMEM((experts, 2, tok // 2, columns), half),
            pltpu.VMEM((groups, 2, 8, tok), jnp.float32),
        ]
        + [held, sent]
        + [pltpu.VMEM(array.shape, half) for array in (gate, up, down)]
        + [pltpu.VMEM((slots, ff), jnp.float32)] * 2
        + [pltpu.VMEM((slots, ff), half)] * 3
        + [pltpu.VMEM((groups, experts, capacity, share), half)]
        + [blocks] * 3
        + [kept, pltpu.VMEM((experts, capacity, 1), jnp.float32)]
        + [dma((11,))]
        + [dma((experts,))] * 2
        + [dma((experts, chips))] * 8
        + [dma((experts,))] * 2
        + [dma((across,))] * 2
        + [dma((across, lead))] * 2
        + [dma((chips,))] * 4
        + [dma((experts,))] * 4
        + [dma((groups,))] * 2
        + [dma] * 2,
        compiler_params=pltpu.CompilerParams(
            collective_id=0, has_side_effects=True, vmem_limit_bytes=42 * 2**20
        ),
        cost_estimate=pl.CostEstimate(flops=10**10, bytes_accessed=10**7, transcendentals=0),
    )(
        *(
            pltpu.with_memory_space_constraint(array, pltpu.HBM)
            for array in inputs
        )
    )


def tail_part(
    experts, groups, mine, place, table, home, cotangent, saved, inverse, gain, weight,
    every, extended, blocks, sums, *sems
):
    (row_send, row_recv, pair_send, pair_recv, far_send, far_recv, half_send, half_recv,
     sum_send, sum_recv, halo_send, halo_recv) = sems
    chips = groups // 2
    chip, core = place // 2, place % 2
    sibling = chip * 2 + 1 - core
    tok = saved.shape[0]
    channels = saved.shape[1]
    width = blocks.shape[-1]
    per = experts // groups
    half = tok // 2

    def at_chip(step):
        return ((chip + step) % chips) * 2 + core

    def share_at(owner):
        return blocks.at[pl.ds(owner * per, per)]

    def row(hop):
        return remote(share_at(place), share_at(place), row_send.at[hop], row_recv.at[hop],
                      (mine, at_chip(hop)))

    def pair(hop):
        owner = at_chip(chips - hop)
        return remote(share_at(owner), share_at(owner), pair_send.at[hop], pair_recv.at[hop],
                      (mine, sibling))

    share = lax.dot_general(
        table[...].reshape(-1, tok), home[...].reshape(-1, home.shape[-1]), CONTRACT_FIRST, preferred_element_type=jnp.float32
    )
    share = (share + cotangent.astype(jnp.float32)).astype(jnp.bfloat16)
    for part in range(per):
        piece = share[:, part * width : (part + 1) * width]
        blocks[place * per + part] = piece.reshape(2, half, width)
    for hop in range(1, chips):
        row(hop).start()
    pair(0).start()
    for hop in range(1, chips):
        row(hop).wait_recv()
        pair(hop).start()
    for hop in range(chips):
        pair(hop).wait_recv()

    def far(step):
        peer = mate(mine, step, experts)
        return remote(blocks.at[peer, core], every.at[step, core], far_send.at[step],
                      far_recv.at[step], (peer, place))

    def to_half(step):
        return remote(every.at[step, core], every.at[step, core], half_send.at[step],
                      half_recv.at[step], (mine, sibling))

    def start_far(step, carry):
        far(step).start()
        return carry

    lax.fori_loop(1, experts, start_far, 0)
    every[0] = blocks[mine]

    grad = jnp.zeros((tok, channels), jnp.float32)
    for part in range(experts):
        grad = grad + lax.dot_general(
            blocks[part].reshape(tok, width),
            weight[:, part * width : (part + 1) * width],
            (((1,), (1,)), ((), ())),
            preferred_element_type=jnp.float32,
        )
    normalized = saved[...].astype(jnp.float32)
    scaled = normalized * gain[...]
    gate = sigmoid(scaled)
    grad = grad * gate * (1.0 + scaled * (1.0 - gate)) * gain[...]
    lanes = min(channels, 128)
    first = jnp.zeros((tok, lanes), jnp.float32)
    second = jnp.zeros((tok, lanes), jnp.float32)
    for at in range(0, channels, lanes):
        first = first + grad[:, at : at + lanes]
        second = second + grad[:, at : at + lanes] * normalized[:, at : at + lanes]
    sums[place, 0] = jnp.sum(jnp.transpose(first).reshape(lanes // 8, 8, tok), axis=0)
    sums[place, 1] = jnp.sum(jnp.transpose(second).reshape(lanes // 8, 8, tok), axis=0)

    def tell(step):
        return remote(sums.at[place], sums.at[place], sum_send.at[step], sum_recv.at[step],
                      (mine, (place + step) % groups))

    def start_tell(step, carry):
        tell(step).start()
        return carry

    def wait_tell(step, carry):
        tell(step).wait()
        return carry

    lax.fori_loop(1, groups, start_tell, 0)
    lax.fori_loop(1, groups, wait_tell, 0)
    count = channels * groups
    total = jnp.sum(sums[...], axis=0)

    def column(kind):
        flat = jnp.sum(total[kind], axis=0, keepdims=True) / count
        return jnp.transpose(jnp.broadcast_to(flat, (lanes, tok)))

    mean, slope = column(0), column(1)
    deviation = jnp.transpose(jnp.broadcast_to(inverse[...], (lanes, tok)))
    for at in range(0, channels, lanes):
        extended[at // lanes, 0:tok] = deviation * (
            grad[:, at : at + lanes] - mean - normalized[:, at : at + lanes] * slope
        )
    reach = extended.shape[1] - tok

    def halo():
        return remote(extended.at[:, pl.ds(0, reach)], extended.at[:, pl.ds(tok, reach)],
                      halo_send, halo_recv, ((mine + experts - 1) % experts, place))

    @pl.when(mine > 0)
    def _():
        halo().start()

    @pl.when(mine == experts - 1)
    def _():
        extended[:, tok : tok + reach] = jnp.zeros((channels // lanes, reach, lanes), jnp.float32)

    def forward(step, carry):
        far(step).wait_recv()
        to_half(step).start()
        return carry

    lax.fori_loop(1, experts, forward, 0)

    @pl.when(mine < experts - 1)
    def _():
        halo().wait_recv()

    def arrive(step, carry):
        to_half(step).wait_recv()
        return carry

    lax.fori_loop(1, experts, arrive, 0)
    @pl.when(mine > 0)
    def _():
        halo().wait_send()

    for hop in range(chips):
        pair(hop).wait_send()
        if hop:
            row(hop).wait_send()

    def finish(step, carry):
        far(step).wait_send()
        to_half(step).wait_send()
        return carry

    lax.fori_loop(1, experts, finish, 0)


def last_kernel(
    lead, every, acts, crossed, extended, taps, gate, up, down, result_far, proj_far, gate_far, up_far, down_far,
    result, proj, sems
):
    stores = [
        pltpu.make_async_copy(source, target, sems.at[at])
        for at, (source, target) in enumerate(
            (
                (gate, gate_far), (up, up_far), (down, down_far), (result, result_far),
                (proj, proj_far),
            )
        )
    ]
    for store in stores[:3]:
        store.start()
    tok, channels = result.shape
    lanes = extended.shape[-1]
    for at in range(0, channels, lanes):
        value = jnp.zeros((tok, lanes), jnp.float32)
        for tap in range(taps.shape[0]):
            value = value + taps[tap : tap + 1, at : at + lanes] * extended[at // lanes, tap : tap + tok]
        result[:, at : at + lanes] = value.astype(result.dtype)
    stores[3].start()
    def product(hop, right):
        return lax.dot_general(
            every[:, hop].reshape(-1, every.shape[-1]),
            right.reshape(-1, channels),
            CONTRACT_FIRST,
            preferred_element_type=jnp.float32,
        )

    value = product(0, acts[...])
    for hop in range(1, lead):
        value = value + product(hop, crossed[hop - 1])
    proj[...] = value
    stores[4].start()
    for store in stores:
        store.wait()


def last_blocks(every, acts, crossed, extended, taps, gate, up, down):
    across, tok, channels = acts.shape
    lead = every.shape[0] // across
    every = every.reshape((across, lead) + every.shape[1:])
    vmem = pl.BlockSpec(memory_space=pltpu.VMEM)
    shapes = (
        jax.ShapeDtypeStruct((tok, channels), jnp.bfloat16),
        jax.ShapeDtypeStruct((every.shape[-1], channels), jnp.float32),
    )
    return pl.pallas_call(
        functools.partial(last_kernel, lead),
        out_shape=shapes
        + tuple(jax.ShapeDtypeStruct(array.shape, array.dtype) for array in (gate, up, down)),
        in_specs=[vmem] * 8,
        out_specs=[pl.BlockSpec(memory_space=pltpu.HBM)] * 5,
        scratch_shapes=[pltpu.VMEM(shape.shape, shape.dtype) for shape in shapes]
        + [pltpu.SemaphoreType.DMA((5,))],
        compiler_params=pltpu.CompilerParams(vmem_limit_bytes=16 * 2**20),
        cost_estimate=pl.CostEstimate(flops=10**9, bytes_accessed=10**7, transcendentals=0),
    )(every, acts, crossed, extended, taps, gate, up, down)


def shards(
    cotangent,
    mixer_out,
    expert_ids,
    route_weight,
    saved_normalized,
    inverse_deviation,
    channel_norm_gain,
    taps,
    proj_weight,
    gate_weight,
    up_weight,
    down_weight,
):
    experts = lax.axis_size("sp")
    groups = lax.axis_size("tp")
    grad_first, grad_third, grad_second, acts, crossed, every, extended = expert_blocks(
        jnp.transpose(expert_ids),
        jnp.transpose(route_weight),
        mixer_out,
        cotangent,
        gate_weight[0],
        up_weight[0],
        down_weight[0],
        saved_normalized,
        channel_norm_gain[None, :],
        proj_weight,
        inverse_deviation[None, :],
        (taps.shape[0] + 6) // 8 * 8,
        experts,
        groups,
    )
    result, grad_proj, grad_first, grad_third, grad_second = last_blocks(
        every, acts, crossed, extended, taps, grad_first, grad_third, grad_second
    )
    return (
        result,
        grad_proj,
        grad_first[None],
        grad_third[None],
        grad_second[None],
    )


def solution(mesh):
    return jax.shard_map(
        shards,
        mesh=mesh,
        in_specs=(
            P("sp", None),
            P("sp", None),
            P("sp", None),
            P("sp", None),
            P("sp", "tp"),
            P("sp"),
            P("tp"),
            P(None, "tp"),
            P("tp", None),
            P("sp", None, "tp"),
            P("sp", None, "tp"),
            P("sp", "tp", None),
        ),
        out_specs=(
            P("sp", "tp"),
            P("sp", "tp"),
            P("sp", None, "tp"),
            P("sp", None, "tp"),
            P("sp", "tp", None),
        ),
        check_vma=False,
    )
```

```python
import functools

import jax
import jax.numpy as jnp
from jax import lax
from jax.experimental import pallas as pl
from jax.experimental.pallas import tpu as pltpu
from jax.sharding import PartitionSpec as P


def line_width(experts):
    width = 1
    while 4 * width * width <= experts and experts % (2 * width) == 0:
        width = 2 * width
    return width


def sigmoid(value):
    return 1.0 / (1.0 + jnp.exp(-value))


def mate(index, step, count):
    if count & (count - 1):
        raise ValueError("count")
    value, bit = 0, 1
    while bit < count:
        value = value + bit * ((index // bit + step // bit) % 2)
        bit = 2 * bit
    return value


def remote(source, target, send_sem, recv_sem, device):
    return pltpu.make_async_remote_copy(
        src_ref=source,
        dst_ref=target,
        send_sem=send_sem,
        recv_sem=recv_sem,
        device_id=device,
        device_id_type=pl.DeviceIdType.MESH,
    )


CONTRACT_LAST = (((1,), (1,)), ((), ()))
CONTRACT_FIRST = (((0,), (0,)), ((), ()))


def expert_kernel(
    experts, groups, lead, ids_far, route_far, mixer_far, cotangent_far, gate_far, up_far, down_far,
    saved_far, gain_far, weight_far, inverse_far, grad_gate, grad_up, grad_down, acts, crossed,
    every, extended, ids, route, mixer, cotangent, saved, gain, weight, inverse, home, table,
    blocks, sums, held, sent, gate, up, down, hidden_gate, hidden_up, active,
    grad_hg, grad_hu, partial, pair_in, row_out, row_in, total, slot_weight, *sems
):
    (load_sem, far_send, far_recv, row_send, row_recv, pair_send, pair_recv,
     home_send, home_recv, sum_send, sum_recv, back_send, back_recv,
     line_send, line_recv, side_send, side_recv) = sems[:17]
    mine = lax.axis_index("sp")
    place = lax.axis_index("tp")
    chips = groups // 2
    chip, core = place // 2, place % 2
    sibling = chip * 2 + 1 - core
    tok = mixer.shape[0]
    capacity, share = held.shape[3:]
    slots = experts * capacity

    def at_chip(step):
        return ((chip + step) % chips) * 2 + core

    loads = [
        pltpu.make_async_copy(source, target, load_sem.at[at])
        for at, (source, target) in enumerate(
            (
                (ids_far, ids), (route_far, route), (mixer_far, mixer), (cotangent_far, cotangent),
                (gate_far, gate), (up_far, up), (down_far, down), (saved_far, saved),
                (gain_far, gain), (weight_far, weight), (inverse_far, inverse),
            )
        )
    ]
    for load in loads:
        load.start()
    barrier = pltpu.get_barrier_semaphore()

    def greet(step, carry):
        pl.semaphore_signal(barrier, inc=1, device_id=((mine + step) % experts, place),
                            device_id_type=pl.DeviceIdType.MESH)
        return carry

    lax.fori_loop(1, experts, greet, 0)

    def greet_group(step, carry):
        pl.semaphore_signal(barrier, inc=1, device_id=(mine, (place + step) % groups),
                            device_id_type=pl.DeviceIdType.MESH)
        return carry

    lax.fori_loop(1, groups, greet_group, 0)
    loads[0].wait()
    loads[1].wait()
    expert = lax.broadcasted_iota(jnp.int32, (experts, tok), 0)
    hot = [(ids[k : k + 1] == expert).astype(jnp.float32) for k in range(ids.shape[0])]
    before = lax.broadcasted_iota(jnp.int32, (tok, tok), 0)
    after = lax.broadcasted_iota(jnp.int32, (tok, tok), 1)
    rank = jnp.dot(
        sum(hot).astype(jnp.bfloat16),
        (before < after).astype(jnp.float32).astype(jnp.bfloat16),
        preferred_element_type=jnp.float32,
    )
    slot = expert.astype(jnp.float32) * capacity + rank
    number = lax.broadcasted_iota(jnp.int32, (slots, tok), 0).astype(jnp.float32)
    chosen = jnp.zeros((slots, tok), jnp.float32)
    weighted = jnp.zeros((slots, tok), jnp.float32)
    for k in range(ids.shape[0]):
        match = number == jnp.sum(hot[k] * slot, axis=0, keepdims=True)
        chosen = jnp.where(match, 1.0, chosen)
        weighted = jnp.where(match, route[k : k + 1], weighted)
    table[...] = chosen.astype(jnp.bfloat16).reshape(experts, capacity, tok)
    slot_weight[...] = jnp.sum(weighted, axis=1, keepdims=True).reshape(experts, capacity, 1)
    columns = pl.ds(pl.multiple_of(place * share, share), share)
    whole = table[...].reshape(slots, tok)
    scale = slot_weight[...].reshape(slots, 1)
    loads[2].wait()
    sent[:, 0] = (
        jnp.dot(whole, mixer[:, columns], preferred_element_type=jnp.float32)
        .astype(jnp.bfloat16).reshape(experts, capacity, share)
    )
    loads[3].wait()
    sent[:, 1] = (
        (scale * jnp.dot(whole, cotangent[:, columns], preferred_element_type=jnp.float32))
        .astype(jnp.bfloat16).reshape(experts, capacity, share)
    )
    pl.semaphore_wait(barrier, experts + groups - 2)

    def far(step):
        peer = mate(mine, step, experts)
        return remote(sent.at[peer], held.at[step, place],
                      far_send.at[step], far_recv.at[step], (peer, place))

    def row(step, hop):
        block = held.at[step, place]
        return remote(block, block, row_send.at[step, hop], row_recv.at[step, hop],
                      (mine, at_chip(hop)))

    def pair(step, hop):
        block = held.at[step, at_chip(chips - hop)]
        return remote(block, block, pair_send.at[step, hop], pair_recv.at[step, hop],
                      (mine, sibling))

    def each(low, high, act):
        def body(step, carry):
            act(step)
            return carry

        lax.fori_loop(low, high, body, 0)

    each(1, experts, lambda step: far(step).start())
    own = table[mine]
    own_scale = slot_weight[mine]
    for g in range(groups):
        span = slice(g * share, (g + 1) * share)
        held[0, g, 0] = jnp.dot(
            own, mixer[:, span], preferred_element_type=jnp.float32
        ).astype(jnp.bfloat16)
        held[0, g, 1] = (
            own_scale * jnp.dot(own, cotangent[:, span], preferred_element_type=jnp.float32)
        ).astype(jnp.bfloat16)

    across = experts // lead
    line, side = mine // lead, mine % lead

    def along(step, bit):
        peer = mate(line, bit, across) * lead + side
        return remote(acts.at[step], acts.at[step + bit], line_send.at[step + bit],
                      line_recv.at[step + bit], (peer, place))

    acts_order = sorted(range(1, across), key=lambda step: -(step & -step))

    def spread(step):
        bit = 1
        while bit < across:
            if step % (2 * bit) == 0:
                along(step, bit).start()
            bit = 2 * bit

    def reached(step):
        bit = 1
        while step % (2 * bit) == 0:
            bit = 2 * bit
        return along(step - bit, bit)

    def beside(step, hop):
        return remote(acts.at[step], crossed.at[hop - 1, step], side_send.at[step, hop],
                      side_recv.at[step, hop], (line * lead + mate(side, hop, lead), place))

    def cross(step):
        for hop in range(1, lead):
            beside(step, hop).start()

    def extend(step):
        reached(step).wait_recv()
        spread(step)

    def early_acts():
        spread(0)
        cross(0)

    def relay_acts():
        for step in acts_order:
            if step & (step - 1) == 0 and step > 1:
                extend(step)

    def later_acts():
        for step in acts_order:
            if step & (step - 1) or step == 1:
                extend(step)
            cross(step)

    def finish_acts():
        for step in range(1, across):
            reached(step).wait_send()
        for step in range(across):
            for hop in range(1, lead):
                beside(step, hop).wait()

    loads[7].wait()
    loads[8].wait()
    scaled = saved[...].astype(jnp.float32) * gain[...]
    acts[0] = (scaled * sigmoid(scaled)).astype(jnp.bfloat16)

    def service(step):
        far(step).wait_recv()
        for hop in range(1, chips):
            row(step, hop).start()
        pair(step, 0).start()

    def settle(step):
        for hop in range(1, chips):
            row(step, hop).wait_recv()
            pair(step, hop).start()

    def complete(step):
        for hop in range(chips):
            pair(step, hop).wait_recv()

    def chunk(kind, low, high, g):
        return held[low:high, g, kind].reshape((high - low) * capacity, share)

    def ahead(low, high):
        lines = slice(low * capacity, high * capacity)
        for matrix, result in ((gate, hidden_gate), (up, hidden_up)):
            value = None
            for g in range(groups):
                term = jnp.dot(
                    chunk(0, low, high, g), matrix[g * share : (g + 1) * share, :],
                    preferred_element_type=jnp.float32,
                )
                value = term if value is None else value + term
            result[lines, :] = value

    def back(low, high):
        lines = slice(low * capacity, high * capacity)
        value = None
        for g in range(groups):
            term = lax.dot_general(
                chunk(1, low, high, g), down[:, g * share : (g + 1) * share], CONTRACT_LAST,
                preferred_element_type=jnp.float32,
            )
            value = term if value is None else value + term
        hg = hidden_gate[lines, :]
        hu = hidden_up[lines, :]
        sigma = sigmoid(hg)
        swish = hg * sigma
        active[lines, :] = (swish * hu).astype(jnp.bfloat16)
        grad_hg[lines, :] = (value * hu * sigma * (1.0 + hg * (1.0 - sigma))).astype(jnp.bfloat16)
        grad_hu[lines, :] = (value * swish).astype(jnp.bfloat16)
        for g in range(groups):
            term = lax.dot_general(
                grad_hg[lines, :], gate[g * share : (g + 1) * share, :], CONTRACT_LAST,
                preferred_element_type=jnp.float32,
            ) + lax.dot_general(
                grad_hu[lines, :], up[g * share : (g + 1) * share, :], CONTRACT_LAST,
                preferred_element_type=jnp.float32,
            )
            partial[g, low:high] = term.astype(jnp.bfloat16).reshape(high - low, capacity, share)

    def weight_grads(g):
        span = pl.ds(pl.multiple_of(g * share, share), share)
        left = held[:, g, 0].reshape(slots, share)
        grad_gate[span, :] = lax.dot_general(
            left, grad_hg[...], CONTRACT_FIRST, preferred_element_type=jnp.float32
        ).astype(jnp.bfloat16)
        grad_up[span, :] = lax.dot_general(
            left, grad_hu[...], CONTRACT_FIRST, preferred_element_type=jnp.float32
        ).astype(jnp.bfloat16)
        grad_down[:, span] = lax.dot_general(
            active[...], held[:, g, 1].reshape(slots, share), CONTRACT_FIRST,
            preferred_element_type=jnp.float32,
        ).astype(jnp.bfloat16)

    def home_pair(step, hop):
        other = ((chip + hop) % chips) * 2 + 1 - core
        return remote(partial.at[other, step], pair_in.at[hop, step],
                      home_send.at[step, hop], home_recv.at[step, hop], (mine, sibling))

    def home_row(step, hop):
        return remote(row_out.at[hop, step], row_in.at[hop, step],
                      sum_send.at[step, hop], sum_recv.at[step, hop], (mine, at_chip(hop)))

    def home_far(step):
        owner = mate(mine, step, experts)
        return remote(total.at[step], home.at[mine],
                      back_send.at[step], back_recv.at[step], (owner, place))

    def start_pair(step):
        for hop in reversed(range(chips)):
            home_pair(step, hop).start()

    def add_pair(step, hop):
        home_pair(step, hop).wait_recv()
        return partial[at_chip(hop), step].astype(jnp.float32) + pair_in[hop, step].astype(
            jnp.float32
        )

    def send_rows(step):
        for hop in range(1, chips):
            row_out[hop, step] = add_pair(step, hop).astype(row_out.dtype)
            home_row(step, hop).start()

    def add_rows(step):
        value = add_pair(step, 0)
        for hop in range(1, chips):
            home_row(step, hop).wait_recv()
            value = value + row_in[hop, step].astype(jnp.float32)
        return value.astype(total.dtype)

    def send_home(step):
        total[step] = add_rows(step)
        home_far(step).start()

    first, second = experts // 2, 3 * experts // 4
    each(1, first, service)
    each(1, 2, settle)
    each(first, second, service)
    each(2, second, settle)
    for load in loads[4:7]:
        load.wait()
    each(first, second, complete)
    ahead(first, second)
    back(first, second)
    each(first, second, start_pair)
    each(second, second + 1, service)
    each(1, first, complete)
    ahead(0, first)
    each(second + 1, experts, service)
    each(first, second, send_rows)
    early_acts()
    back(0, first)
    each(0, first, start_pair)
    each(second, experts, settle)
    each(0, first // 2, send_rows)
    each(second, experts, complete)
    ahead(second, experts)
    back(second, experts)
    each(second, experts, start_pair)
    each(first, second, send_home)
    weight_grads(0)
    each(second, experts, send_rows)
    each(first // 2, first, send_rows)
    home[mine] = add_rows(0)
    each(1, first // 2, send_home)
    relay_acts()
    each(1, groups - 1, weight_grads)
    each(second, experts, send_home)
    weight_grads(groups - 1)
    each(first // 2, first, send_home)
    later_acts()

    def return_done(step):
        home_far(step).wait_recv()

    each(1, experts, return_done)
    loads[9].wait()
    loads[10].wait()
    tail_part(
        experts, groups, mine, place, table, home, cotangent[:, columns], saved, inverse, gain,
        weight, every, extended, blocks, sums, *sems[17:],
    )

    def finish(step):
        for hop in range(chips):
            home_pair(step, hop).wait_send()
            if hop:
                home_row(step, hop).wait_send()

    def finish_far(step):
        home_far(step).wait_send()
        far(step).wait_send()
        for hop in range(chips):
            pair(step, hop).wait_send()
            if hop:
                row(step, hop).wait_send()

    finish_acts()
    each(0, experts, finish)
    each(1, experts, finish_far)


def expert_blocks(
    ids, route, mixer, cotangent, gate, up, down, saved, gain, weight, inverse, reach, experts,
    groups,
):
    tok, width = mixer.shape
    ff = gate.shape[1]
    share = width // groups
    capacity = groups * max(1, 4 * tok // (experts * groups))
    chips = groups // 2
    slots = experts * capacity
    lead = line_width(experts)
    across = experts // lead
    half = jnp.bfloat16
    dma = pltpu.SemaphoreType.DMA
    vmem = pl.BlockSpec(memory_space=pltpu.VMEM)
    held = pltpu.VMEM((experts, groups, 2, capacity, share), half)
    sent = pltpu.VMEM((experts, 2, capacity, share), half)
    kept = pltpu.VMEM((experts, capacity, share), half)
    blocks = pltpu.VMEM((chips, experts, capacity, share), half)
    channels = saved.shape[1]
    lanes = min(channels, 128)
    columns = width // experts
    outs = tuple(jax.ShapeDtypeStruct(array.shape, half) for array in (gate, up, down)) + (
        jax.ShapeDtypeStruct((across,) + saved.shape, half),
        jax.ShapeDtypeStruct((lead - 1, across) + saved.shape, half),
        jax.ShapeDtypeStruct((experts, 2, tok // 2, columns), half),
        jax.ShapeDtypeStruct((channels // lanes, tok + reach, lanes), jnp.float32),
    )
    inputs = (ids, route, mixer, cotangent, gate, up, down, saved, gain, weight, inverse)
    return pl.pallas_call(
        functools.partial(expert_kernel, experts, groups, lead),
        out_shape=outs,
        in_specs=[pl.BlockSpec(memory_space=pltpu.HBM)] * len(inputs),
        out_specs=[vmem] * len(outs),
        scratch_shapes=[
            pltpu.VMEM(array.shape, array.dtype)
            for array in (ids, route, mixer, cotangent, saved, gain, weight, inverse)
        ]
        + [
            kept,
            pltpu.VMEM((experts, capacity, tok), half),
            pltpu.VMEM((experts, 2, tok // 2, columns), half),
            pltpu.VMEM((groups, 2, 8, tok), jnp.float32),
        ]
        + [held, sent]
        + [pltpu.VMEM(array.shape, half) for array in (gate, up, down)]
        + [pltpu.VMEM((slots, ff), jnp.float32)] * 2
        + [pltpu.VMEM((slots, ff), half)] * 3
        + [pltpu.VMEM((groups, experts, capacity, share), half)]
        + [blocks] * 3
        + [kept, pltpu.VMEM((experts, capacity, 1), jnp.float32)]
        + [dma((11,))]
        + [dma((experts,))] * 2
        + [dma((experts, chips))] * 8
        + [dma((experts,))] * 2
        + [dma((across,))] * 2
        + [dma((across, lead))] * 2
        + [dma((chips,))] * 4
        + [dma((experts,))] * 4
        + [dma((groups,))] * 2
        + [dma] * 2,
        compiler_params=pltpu.CompilerParams(
            collective_id=0, has_side_effects=True, vmem_limit_bytes=42 * 2**20
        ),
        cost_estimate=pl.CostEstimate(flops=10**10, bytes_accessed=10**7, transcendentals=0),
    )(
        *(
            pltpu.with_memory_space_constraint(array, pltpu.HBM)
            for array in inputs
        )
    )


def tail_part(
    experts, groups, mine, place, table, home, cotangent, saved, inverse, gain, weight,
    every, extended, blocks, sums, *sems
):
    (row_send, row_recv, pair_send, pair_recv, far_send, far_recv, half_send, half_recv,
     sum_send, sum_recv, halo_send, halo_recv) = sems
    chips = groups // 2
    chip, core = place // 2, place % 2
    sibling = chip * 2 + 1 - core
    tok = saved.shape[0]
    channels = saved.shape[1]
    width = blocks.shape[-1]
    per = experts // groups
    half = tok // 2

    def at_chip(step):
        return ((chip + step) % chips) * 2 + core

    def share_at(owner):
        return blocks.at[pl.ds(owner * per, per)]

    def row(hop):
        return remote(share_at(place), share_at(place), row_send.at[hop], row_recv.at[hop],
                      (mine, at_chip(hop)))

    def pair(hop):
        owner = at_chip(chips - hop)
        return remote(share_at(owner), share_at(owner), pair_send.at[hop], pair_recv.at[hop],
                      (mine, sibling))

    share = lax.dot_general(
        table[...].reshape(-1, tok), home[...].reshape(-1, home.shape[-1]), CONTRACT_FIRST, preferred_element_type=jnp.float32
    )
    share = (share + cotangent.astype(jnp.float32)).astype(jnp.bfloat16)
    for part in range(per):
        piece = share[:, part * width : (part + 1) * width]
        blocks[place * per + part] = piece.reshape(2, half, width)
    def far(step):
        peer = mate(mine, step, experts)
        return remote(blocks.at[peer, core], every.at[step, core], far_send.at[step],
                      far_recv.at[step], (peer, place))

    def to_half(step):
        return remote(every.at[step, core], every.at[step, core],
                      half_send.at[step], half_recv.at[step], (mine, sibling))

    def send_share(owner):
        for part in range(per):
            peer = owner * per + part

            @pl.when(peer != mine)
            def _(peer=peer):
                far(mate(mine, peer, experts)).start()

    def product(owner):
        side = weight[:, pl.ds(pl.multiple_of(owner * per * width, per * width), per * width)]
        value = None
        for part in range(per):
            term = lax.dot_general(
                blocks[owner * per + part].reshape(tok, width),
                side[:, part * width : (part + 1) * width],
                CONTRACT_LAST,
                preferred_element_type=jnp.float32,
            )
            value = term if value is None else value + term
        return value

    for hop in range(1, chips):
        row(hop).start()
    pair(0).start()
    send_share(place)
    grad = product(place)
    pair(0).wait_recv()
    send_share(sibling)
    grad = grad + product(sibling)
    for hop in range(1, chips):
        row(hop).wait_recv()
        pair(hop).start()
        send_share(at_chip(chips - hop))
        grad = grad + product(at_chip(chips - hop))
    for hop in range(1, chips):
        pair(hop).wait_recv()
        other = ((chip + chips - hop) % chips) * 2 + 1 - core
        send_share(other)
        grad = grad + product(other)
    every[0] = blocks[mine]
    normalized = saved[...].astype(jnp.float32)
    scaled = normalized * gain[...]
    gate = sigmoid(scaled)
    grad = grad * gate * (1.0 + scaled * (1.0 - gate)) * gain[...]
    lanes = min(channels, 128)
    first = jnp.zeros((tok, lanes), jnp.float32)
    second = jnp.zeros((tok, lanes), jnp.float32)
    for at in range(0, channels, lanes):
        first = first + grad[:, at : at + lanes]
        second = second + grad[:, at : at + lanes] * normalized[:, at : at + lanes]
    sums[place, 0] = jnp.sum(jnp.transpose(first).reshape(lanes // 8, 8, tok), axis=0)
    sums[place, 1] = jnp.sum(jnp.transpose(second).reshape(lanes // 8, 8, tok), axis=0)

    def tell(step):
        return remote(sums.at[place], sums.at[place], sum_send.at[step], sum_recv.at[step],
                      (mine, (place + step) % groups))

    def start_tell(step, carry):
        tell(step).start()
        return carry

    def wait_tell(step, carry):
        tell(step).wait()
        return carry

    lax.fori_loop(1, groups, start_tell, 0)
    lax.fori_loop(1, groups, wait_tell, 0)
    count = channels * groups
    total = jnp.sum(sums[...], axis=0)

    def column(kind):
        flat = jnp.sum(total[kind], axis=0, keepdims=True) / count
        return jnp.transpose(jnp.broadcast_to(flat, (lanes, tok)))

    mean, slope = column(0), column(1)
    deviation = jnp.transpose(jnp.broadcast_to(inverse[...], (lanes, tok)))
    for at in range(0, channels, lanes):
        extended[at // lanes, 0:tok] = deviation * (
            grad[:, at : at + lanes] - mean - normalized[:, at : at + lanes] * slope
        )
    reach = extended.shape[1] - tok

    def halo():
        return remote(extended.at[:, pl.ds(0, reach)], extended.at[:, pl.ds(tok, reach)],
                      halo_send, halo_recv, ((mine + experts - 1) % experts, place))

    @pl.when(mine > 0)
    def _():
        halo().start()

    @pl.when(mine == experts - 1)
    def _():
        extended[:, tok : tok + reach] = jnp.zeros((channels // lanes, reach, lanes), jnp.float32)

    def forward(step, carry):
        far(step).wait_recv()
        to_half(step).start()
        return carry

    lax.fori_loop(1, experts, forward, 0)

    @pl.when(mine < experts - 1)
    def _():
        halo().wait_recv()

    def arrive(step, carry):
        to_half(step).wait_recv()
        return carry

    lax.fori_loop(1, experts, arrive, 0)
    @pl.when(mine > 0)
    def _():
        halo().wait_send()

    for hop in range(chips):
        pair(hop).wait_send()
        if hop:
            row(hop).wait_send()

    def finish(step, carry):
        far(step).wait_send()
        to_half(step).wait_send()
        return carry

    lax.fori_loop(1, experts, finish, 0)


def last_kernel(
    lead, every, acts, crossed, extended, taps, gate, up, down, result_far, proj_far, gate_far, up_far, down_far,
    result, proj, sems
):
    stores = [
        pltpu.make_async_copy(source, target, sems.at[at])
        for at, (source, target) in enumerate(
            (
                (gate, gate_far), (up, up_far), (down, down_far), (result, result_far),
                (proj, proj_far),
            )
        )
    ]
    for store in stores[:3]:
        store.start()
    tok, channels = result.shape
    lanes = extended.shape[-1]
    for at in range(0, channels, lanes):
        value = jnp.zeros((tok, lanes), jnp.float32)
        for tap in range(taps.shape[0]):
            value = value + taps[tap : tap + 1, at : at + lanes] * extended[at // lanes, tap : tap + tok]
        result[:, at : at + lanes] = value.astype(result.dtype)
    stores[3].start()
    def product(hop, right):
        return lax.dot_general(
            every[:, hop].reshape(-1, every.shape[-1]),
            right.reshape(-1, channels),
            CONTRACT_FIRST,
            preferred_element_type=jnp.float32,
        )

    value = product(0, acts[...])
    for hop in range(1, lead):
        value = value + product(hop, crossed[hop - 1])
    proj[...] = value
    stores[4].start()
    for store in stores:
        store.wait()


def last_blocks(every, acts, crossed, extended, taps, gate, up, down):
    across, tok, channels = acts.shape
    lead = every.shape[0] // across
    every = every.reshape((across, lead) + every.shape[1:])
    vmem = pl.BlockSpec(memory_space=pltpu.VMEM)
    shapes = (
        jax.ShapeDtypeStruct((tok, channels), jnp.bfloat16),
        jax.ShapeDtypeStruct((every.shape[-1], channels), jnp.float32),
    )
    return pl.pallas_call(
        functools.partial(last_kernel, lead),
        out_shape=shapes
        + tuple(jax.ShapeDtypeStruct(array.shape, array.dtype) for array in (gate, up, down)),
        in_specs=[vmem] * 8,
        out_specs=[pl.BlockSpec(memory_space=pltpu.HBM)] * 5,
        scratch_shapes=[pltpu.VMEM(shape.shape, shape.dtype) for shape in shapes]
        + [pltpu.SemaphoreType.DMA((5,))],
        compiler_params=pltpu.CompilerParams(vmem_limit_bytes=16 * 2**20),
        cost_estimate=pl.CostEstimate(flops=10**9, bytes_accessed=10**7, transcendentals=0),
    )(every, acts, crossed, extended, taps, gate, up, down)


def shards(
    cotangent,
    mixer_out,
    expert_ids,
    route_weight,
    saved_normalized,
    inverse_deviation,
    channel_norm_gain,
    taps,
    proj_weight,
    gate_weight,
    up_weight,
    down_weight,
):
    experts = lax.axis_size("sp")
    groups = lax.axis_size("tp")
    grad_first, grad_third, grad_second, acts, crossed, every, extended = expert_blocks(
        jnp.transpose(expert_ids),
        jnp.transpose(route_weight),
        mixer_out,
        cotangent,
        gate_weight[0],
        up_weight[0],
        down_weight[0],
        saved_normalized,
        channel_norm_gain[None, :],
        proj_weight,
        inverse_deviation[None, :],
        (taps.shape[0] + 6) // 8 * 8,
        experts,
        groups,
    )
    result, grad_proj, grad_first, grad_third, grad_second = last_blocks(
        every, acts, crossed, extended, taps, grad_first, grad_third, grad_second
    )
    return (
        result,
        grad_proj,
        grad_first[None],
        grad_third[None],
        grad_second[None],
    )


def solution(mesh):
    return jax.shard_map(
        shards,
        mesh=mesh,
        in_specs=(
            P("sp", None),
            P("sp", None),
            P("sp", None),
            P("sp", None),
            P("sp", "tp"),
            P("sp"),
            P("tp"),
            P(None, "tp"),
            P("tp", None),
            P("sp", None, "tp"),
            P("sp", None, "tp"),
            P("sp", "tp", None),
        ),
        out_specs=(
            P("sp", "tp"),
            P("sp", "tp"),
            P("sp", None, "tp"),
            P("sp", None, "tp"),
            P("sp", "tp", None),
        ),
        check_vma=False,
    )
```

```python
import functools

import jax
import jax.numpy as jnp
from jax import lax
from jax.experimental import pallas as pl
from jax.experimental.pallas import tpu as pltpu
from jax.sharding import PartitionSpec as P


def line_width(experts):
    width = 1
    while 4 * width * width <= experts and experts % (2 * width) == 0:
        width = 2 * width
    return width


def sigmoid(value):
    return 1.0 / (1.0 + jnp.exp(-value))


def mate(index, step, count):
    if count & (count - 1):
        raise ValueError("count")
    value, bit = 0, 1
    while bit < count:
        value = value + bit * ((index // bit + step // bit) % 2)
        bit = 2 * bit
    return value


def remote(source, target, send_sem, recv_sem, device):
    return pltpu.make_async_remote_copy(
        src_ref=source,
        dst_ref=target,
        send_sem=send_sem,
        recv_sem=recv_sem,
        device_id=device,
        device_id_type=pl.DeviceIdType.MESH,
    )


CONTRACT_LAST = (((1,), (1,)), ((), ()))
CONTRACT_FIRST = (((0,), (0,)), ((), ()))


def expert_kernel(
    experts, groups, lead, ids_far, route_far, mixer_far, cotangent_far, gate_far, up_far, down_far,
    saved_far, gain_far, weight_far, inverse_far, grad_gate, grad_up, grad_down, acts, crossed,
    every, extended, ids, route, mixer, cotangent, saved, gain, weight, inverse, home, table,
    blocks, sums, tokens, ids_in, route_in, relayed, more, held, sent, gate, up, down, hidden_gate, hidden_up, active,
    grad_hg, grad_hu, partial, pair_in, row_out, row_in, total, slot_weight, *sems
):
    (load_sem, far_send, far_recv, row_send, row_recv, pair_send, pair_recv,
     home_send, home_recv, sum_send, sum_recv, back_send, back_recv,
     line_send, line_recv, side_send, side_recv, token_send, token_recv, relay_send,
     relay_recv) = sems[:21]
    mine = lax.axis_index("sp")
    place = lax.axis_index("tp")
    chips = groups // 2
    chip, core = place // 2, place % 2
    sibling = chip * 2 + 1 - core
    tok = mixer.shape[0]
    capacity, share = held.shape[3:]
    slots = experts * capacity

    def at_chip(step):
        return ((chip + step) % chips) * 2 + core

    loads = [
        pltpu.make_async_copy(source, target, load_sem.at[at])
        for at, (source, target) in enumerate(
            (
                (ids_far, ids), (route_far, route), (mixer_far, mixer), (cotangent_far, cotangent),
                (gate_far, gate), (up_far, up), (down_far, down), (saved_far, saved),
                (gain_far, gain), (weight_far, weight), (inverse_far, inverse),
            )
        )
    ]
    for load in loads:
        load.start()
    barrier = pltpu.get_barrier_semaphore()

    def greet(step, carry):
        pl.semaphore_signal(barrier, inc=1, device_id=((mine + step) % experts, place),
                            device_id_type=pl.DeviceIdType.MESH)
        return carry

    lax.fori_loop(1, experts, greet, 0)

    def greet_group(step, carry):
        pl.semaphore_signal(barrier, inc=1, device_id=(mine, (place + step) % groups),
                            device_id_type=pl.DeviceIdType.MESH)
        return carry

    lax.fori_loop(1, groups, greet_group, 0)
    first = experts // 2
    base = mine // first * first
    columns = pl.ds(pl.multiple_of(place * share, share), share)
    for load in loads[:4]:
        load.wait()
    pl.semaphore_wait(barrier, experts + groups - 2)
    opposite = mate(mine, first, experts)
    crossing = [
        remote(source, target, token_send.at[at], token_recv.at[at], (opposite, place))
        for at, (source, target) in enumerate(
            (
                (ids, ids_in), (route, route_in), (mixer.at[:, columns], tokens.at[0]),
                (cotangent.at[:, columns], tokens.at[1]),
            )
        )
    ]
    crossing[0].start()
    crossing[1].start()

    def slot_table(chosen_ids, weights, low, count):
        expert = lax.broadcasted_iota(jnp.int32, (experts, tok), 0)
        hot = [(chosen_ids[k : k + 1] == expert).astype(jnp.float32) for k in range(ids.shape[0])]
        before = lax.broadcasted_iota(jnp.int32, (tok, tok), 0)
        after = lax.broadcasted_iota(jnp.int32, (tok, tok), 1)
        rank = jnp.dot(
            sum(hot).astype(jnp.bfloat16),
            (before < after).astype(jnp.float32).astype(jnp.bfloat16),
            preferred_element_type=jnp.float32,
        )
        slot = expert.astype(jnp.float32) * capacity + rank
        number = (lax.broadcasted_iota(jnp.int32, (count, tok), 0) + low).astype(jnp.float32)
        chosen = jnp.zeros((count, tok), jnp.float32)
        weighted = jnp.zeros((count, tok), jnp.float32)
        for k in range(ids.shape[0]):
            match = number == jnp.sum(hot[k] * slot, axis=0, keepdims=True)
            chosen = jnp.where(match, 1.0, chosen)
            weighted = jnp.where(match, weights[k : k + 1], weighted)
        return chosen.astype(jnp.bfloat16), jnp.sum(weighted, axis=1, keepdims=True)

    def pick(picks, values):
        return jnp.dot(picks, values, preferred_element_type=jnp.float32)

    every_slot, scale = slot_table(ids[...], route[...], 0, slots)
    table[...] = every_slot.reshape(experts, capacity, tok)
    slot_weight[...] = scale.reshape(experts, capacity, 1)
    near = table[pl.ds(base, first)].reshape(first * capacity, tok)
    near_scale = slot_weight[pl.ds(base, first)].reshape(first * capacity, 1)
    sent[:, 0] = pick(near, mixer[:, columns]).astype(jnp.bfloat16).reshape(first, capacity, share)
    sent[:, 1] = (
        (near_scale * pick(near, cotangent[:, columns]))
        .astype(jnp.bfloat16).reshape(first, capacity, share)
    )

    def far(step):
        peer = mate(mine, step, experts)
        return remote(sent.at[peer - base], held.at[step, place],
                      far_send.at[step], far_recv.at[step], (peer, place))

    def row(step, hop):
        block = held.at[step, place]
        return remote(block, block, row_send.at[step, hop], row_recv.at[step, hop],
                      (mine, at_chip(hop)))

    def pair(step, hop):
        block = held.at[step, at_chip(chips - hop)]
        return remote(block, block, pair_send.at[step, hop], pair_recv.at[step, hop],
                      (mine, sibling))

    def each(low, high, act):
        def body(step, carry):
            act(step)
            return carry

        lax.fori_loop(low, high, body, 0)

    def extra(step, hop):
        return remote(more.at[hop - 1, step - 1], held.at[step, at_chip(chips - hop)],
                      row_send.at[step, hop], row_recv.at[step, hop],
                      (mate(mine, step, experts), place))

    each(1, first, lambda step: far(step).start())
    for hop in range(1, chips):
        other = pl.ds(pl.multiple_of(at_chip(chips - hop) * share, share), share)
        for step in range(1, lead):
            peer = mate(mine, step, experts)
            picks = table[peer]
            more[hop - 1, step - 1, 0] = pick(picks, mixer[:, other]).astype(jnp.bfloat16)
            more[hop - 1, step - 1, 1] = (
                slot_weight[peer] * pick(picks, cotangent[:, other])
            ).astype(jnp.bfloat16)
            extra(step, hop).start()
    crossing[2].start()
    crossing[3].start()

    def relay(kind, step):
        peer = mate(mine, step, experts)
        return remote(relayed.at[peer - base, kind], held.at[step + first, place, kind],
                      relay_send.at[kind, step], relay_recv.at[kind, step], (peer, place))

    own = table[mine]
    own_scale = slot_weight[mine]
    for g in range(groups):
        span = slice(g * share, (g + 1) * share)
        held[0, g, 0] = jnp.dot(
            own, mixer[:, span], preferred_element_type=jnp.float32
        ).astype(jnp.bfloat16)
        held[0, g, 1] = (
            own_scale * jnp.dot(own, cotangent[:, span], preferred_element_type=jnp.float32)
        ).astype(jnp.bfloat16)

    across = experts // lead
    line, side = mine // lead, mine % lead

    def along(step, bit):
        peer = mate(line, bit, across) * lead + side
        return remote(acts.at[step], acts.at[step + bit], line_send.at[step + bit],
                      line_recv.at[step + bit], (peer, place))

    acts_order = sorted(range(1, across), key=lambda step: -(step & -step))

    def spread(step):
        bit = 1
        while bit < across:
            if step % (2 * bit) == 0:
                along(step, bit).start()
            bit = 2 * bit

    def reached(step):
        bit = 1
        while step % (2 * bit) == 0:
            bit = 2 * bit
        return along(step - bit, bit)

    def beside(step, hop):
        return remote(acts.at[step], crossed.at[hop - 1, step], side_send.at[step, hop],
                      side_recv.at[step, hop], (line * lead + mate(side, hop, lead), place))

    def cross(step):
        for hop in range(1, lead):
            beside(step, hop).start()

    def extend(step):
        reached(step).wait_recv()
        spread(step)

    def early_acts():
        spread(0)
        cross(0)

    def relay_acts():
        for step in acts_order:
            if step & (step - 1) == 0 and step > 1:
                extend(step)

    def later_acts():
        for step in acts_order:
            if step & (step - 1) or step == 1:
                extend(step)
            cross(step)

    def finish_acts():
        for step in range(1, across):
            reached(step).wait_send()
        for step in range(across):
            for hop in range(1, lead):
                beside(step, hop).wait()

    loads[7].wait()
    loads[8].wait()
    scaled = saved[...].astype(jnp.float32) * gain[...]
    acts[0] = (scaled * sigmoid(scaled)).astype(jnp.bfloat16)

    def greeted(step):
        far(step).wait_recv()
        pair(step, 0).start()

    def service(step):
        far(step).wait_recv()
        hand_on(step)

    def serve(step):
        relay(0, step - first).wait_recv()
        relay(1, step - first).wait_recv()
        hand_on(step)

    def hand_on(step):
        for hop in range(1, chips):
            row(step, hop).start()
        pair(step, 0).start()

    def settle(step):
        for hop in range(1, chips):
            row(step, hop).wait_recv()
            pair(step, hop).start()

    def complete(step):
        for hop in range(chips):
            pair(step, hop).wait_recv()

    def chunk(kind, low, high, g):
        return held[low:high, g, kind].reshape((high - low) * capacity, share)

    crossing[0].wait_recv()
    crossing[1].wait_recv()
    far_table, far_scale = slot_table(ids_in[...], route_in[...], base * capacity, first * capacity)

    def relay_kind(kind):
        crossing[kind + 2].wait_recv()
        value = pick(far_table, tokens[kind])
        if kind:
            value = far_scale * value
        relayed[:, kind] = value.astype(jnp.bfloat16).reshape(first, capacity, share)
        each(1, first, lambda step: relay(kind, step).start())
        held[first, place, kind] = relayed[mine - base, kind]

    def ahead(low, high):
        lines = slice(low * capacity, high * capacity)
        for matrix, result in ((gate, hidden_gate), (up, hidden_up)):
            value = None
            for g in range(groups):
                term = jnp.dot(
                    chunk(0, low, high, g), matrix[g * share : (g + 1) * share, :],
                    preferred_element_type=jnp.float32,
                )
                value = term if value is None else value + term
            result[lines, :] = value

    def back(low, high):
        lines = slice(low * capacity, high * capacity)
        value = None
        for g in range(groups):
            term = lax.dot_general(
                chunk(1, low, high, g), down[:, g * share : (g + 1) * share], CONTRACT_LAST,
                preferred_element_type=jnp.float32,
            )
            value = term if value is None else value + term
        hg = hidden_gate[lines, :]
        hu = hidden_up[lines, :]
        sigma = sigmoid(hg)
        swish = hg * sigma
        active[lines, :] = (swish * hu).astype(jnp.bfloat16)
        grad_hg[lines, :] = (value * hu * sigma * (1.0 + hg * (1.0 - sigma))).astype(jnp.bfloat16)
        grad_hu[lines, :] = (value * swish).astype(jnp.bfloat16)
        for g in range(groups):
            term = lax.dot_general(
                grad_hg[lines, :], gate[g * share : (g + 1) * share, :], CONTRACT_LAST,
                preferred_element_type=jnp.float32,
            ) + lax.dot_general(
                grad_hu[lines, :], up[g * share : (g + 1) * share, :], CONTRACT_LAST,
                preferred_element_type=jnp.float32,
            )
            partial[g, low:high] = term.astype(jnp.bfloat16).reshape(high - low, capacity, share)

    def weight_grads(g):
        span = pl.ds(pl.multiple_of(g * share, share), share)
        left = held[:, g, 0].reshape(slots, share)
        grad_gate[span, :] = lax.dot_general(
            left, grad_hg[...], CONTRACT_FIRST, preferred_element_type=jnp.float32
        ).astype(jnp.bfloat16)
        grad_up[span, :] = lax.dot_general(
            left, grad_hu[...], CONTRACT_FIRST, preferred_element_type=jnp.float32
        ).astype(jnp.bfloat16)
        grad_down[:, span] = lax.dot_general(
            active[...], held[:, g, 1].reshape(slots, share), CONTRACT_FIRST,
            preferred_element_type=jnp.float32,
        ).astype(jnp.bfloat16)

    def home_pair(step, hop):
        other = ((chip + hop) % chips) * 2 + 1 - core
        return remote(partial.at[other, step], pair_in.at[hop, step],
                      home_send.at[step, hop], home_recv.at[step, hop], (mine, sibling))

    def home_row(step, hop):
        return remote(row_out.at[hop, step], row_in.at[hop, step],
                      sum_send.at[step, hop], sum_recv.at[step, hop], (mine, at_chip(hop)))

    def home_far(step):
        owner = mate(mine, step, experts)
        return remote(total.at[step], home.at[mine],
                      back_send.at[step], back_recv.at[step], (owner, place))

    def start_pair(step):
        for hop in reversed(range(chips)):
            home_pair(step, hop).start()

    def add_pair(step, hop):
        home_pair(step, hop).wait_recv()
        return partial[at_chip(hop), step].astype(jnp.float32) + pair_in[hop, step].astype(
            jnp.float32
        )

    def send_rows(step):
        for hop in range(1, chips):
            row_out[hop, step] = add_pair(step, hop).astype(row_out.dtype)
            home_row(step, hop).start()

    def add_rows(step):
        value = add_pair(step, 0)
        for hop in range(1, chips):
            home_row(step, hop).wait_recv()
            value = value + row_in[hop, step].astype(jnp.float32)
        return value.astype(total.dtype)

    def send_home(step):
        total[step] = add_rows(step)
        home_far(step).start()

    second = 3 * experts // 4
    each(1, lead, greeted)
    each(lead, first, service)
    relay_kind(0)
    relay_kind(1)
    hand_on(first)
    each(1, first, settle)
    each(first + 1, second, serve)
    for load in loads[4:7]:
        load.wait()
    each(1, first, complete)
    ahead(0, first)
    each(second, experts, serve)
    back(0, first)
    each(0, first, start_pair)
    early_acts()
    each(first, second, settle)
    each(first, second, complete)
    ahead(first, second)
    back(first, second)
    each(first, second, start_pair)
    each(second, experts, settle)
    each(first, second, send_rows)
    each(0, first // 2, send_rows)
    each(second, experts, complete)
    ahead(second, experts)
    back(second, experts)
    each(second, experts, start_pair)
    each(first, second, send_home)
    weight_grads(0)
    each(second, experts, send_rows)
    each(first // 2, first, send_rows)
    home[mine] = add_rows(0)
    each(1, first // 2, send_home)
    relay_acts()
    each(1, groups - 1, weight_grads)
    each(second, experts, send_home)
    weight_grads(groups - 1)
    each(first // 2, first, send_home)
    later_acts()

    def return_done(step):
        home_far(step).wait_recv()

    each(1, experts, return_done)
    loads[9].wait()
    loads[10].wait()
    tail_part(
        experts, groups, mine, place, table, home, cotangent[:, columns], saved, inverse, gain,
        weight, every, extended, blocks, sums, *sems[21:],
    )

    def finish(step):
        for hop in range(chips):
            home_pair(step, hop).wait_send()
            if hop:
                home_row(step, hop).wait_send()

    def finish_far(step):
        home_far(step).wait_send()
        for hop in range(chips):
            pair(step, hop).wait_send()
            if hop:
                row(step, hop).wait_send()

    finish_acts()
    each(0, experts, finish)
    each(1, experts, finish_far)

    def finish_near(step):
        far(step).wait_send()
        relay(0, step).wait_send()
        relay(1, step).wait_send()

    each(1, first, finish_near)
    for copy in crossing:
        copy.wait_send()


def expert_blocks(
    ids, route, mixer, cotangent, gate, up, down, saved, gain, weight, inverse, reach, experts,
    groups,
):
    tok, width = mixer.shape
    ff = gate.shape[1]
    share = width // groups
    capacity = groups * max(1, 4 * tok // (experts * groups))
    chips = groups // 2
    slots = experts * capacity
    lead = line_width(experts)
    across = experts // lead
    half = jnp.bfloat16
    dma = pltpu.SemaphoreType.DMA
    vmem = pl.BlockSpec(memory_space=pltpu.VMEM)
    held = pltpu.VMEM((experts, groups, 2, capacity, share), half)
    sent = pltpu.VMEM((experts // 2, 2, capacity, share), half)
    kept = pltpu.VMEM((experts, capacity, share), half)
    blocks = pltpu.VMEM((chips, experts, capacity, share), half)
    channels = saved.shape[1]
    lanes = min(channels, 128)
    columns = width // experts
    outs = tuple(jax.ShapeDtypeStruct(array.shape, half) for array in (gate, up, down)) + (
        jax.ShapeDtypeStruct((across,) + saved.shape, half),
        jax.ShapeDtypeStruct((lead - 1, across) + saved.shape, half),
        jax.ShapeDtypeStruct((experts, 2, tok // 2, columns), half),
        jax.ShapeDtypeStruct((channels // lanes, tok + reach, lanes), jnp.float32),
    )
    inputs = (ids, route, mixer, cotangent, gate, up, down, saved, gain, weight, inverse)
    return pl.pallas_call(
        functools.partial(expert_kernel, experts, groups, lead),
        out_shape=outs,
        in_specs=[pl.BlockSpec(memory_space=pltpu.HBM)] * len(inputs),
        out_specs=[vmem] * len(outs),
        scratch_shapes=[
            pltpu.VMEM(array.shape, array.dtype)
            for array in (ids, route, mixer, cotangent, saved, gain, weight, inverse)
        ]
        + [
            kept,
            pltpu.VMEM((experts, capacity, tok), half),
            pltpu.VMEM((experts, 2, tok // 2, columns), half),
            pltpu.VMEM((groups, 2, 8, tok), jnp.float32),
            pltpu.VMEM((2, tok, share), half),
            pltpu.VMEM(ids.shape, ids.dtype),
            pltpu.VMEM(route.shape, route.dtype),
            sent,
            pltpu.VMEM((chips - 1, lead - 1, 2, capacity, share), half),
        ]
        + [held, sent]
        + [pltpu.VMEM(array.shape, half) for array in (gate, up, down)]
        + [pltpu.VMEM((slots, ff), jnp.float32)] * 2
        + [pltpu.VMEM((slots, ff), half)] * 3
        + [pltpu.VMEM((groups, experts, capacity, share), half)]
        + [blocks] * 3
        + [kept, pltpu.VMEM((experts, capacity, 1), jnp.float32)]
        + [dma((11,))]
        + [dma((experts,))] * 2
        + [dma((experts, chips))] * 8
        + [dma((experts,))] * 2
        + [dma((across,))] * 2
        + [dma((across, lead))] * 2
        + [dma((4,))] * 2
        + [dma((2, experts // 2))] * 2
        + [dma((chips,))] * 4
        + [dma((experts,))] * 4
        + [dma((groups,))] * 2
        + [dma] * 2,
        compiler_params=pltpu.CompilerParams(
            collective_id=0, has_side_effects=True, vmem_limit_bytes=42 * 2**20
        ),
        cost_estimate=pl.CostEstimate(flops=10**10, bytes_accessed=10**7, transcendentals=0),
    )(
        *(
            pltpu.with_memory_space_constraint(array, pltpu.HBM)
            for array in inputs
        )
    )


def tail_part(
    experts, groups, mine, place, table, home, cotangent, saved, inverse, gain, weight,
    every, extended, blocks, sums, *sems
):
    (row_send, row_recv, pair_send, pair_recv, far_send, far_recv, half_send, half_recv,
     sum_send, sum_recv, halo_send, halo_recv) = sems
    chips = groups // 2
    chip, core = place // 2, place % 2
    sibling = chip * 2 + 1 - core
    tok = saved.shape[0]
    channels = saved.shape[1]
    width = blocks.shape[-1]
    per = experts // groups
    half = tok // 2

    def at_chip(step):
        return ((chip + step) % chips) * 2 + core

    def share_at(owner):
        return blocks.at[pl.ds(owner * per, per)]

    def row(hop):
        return remote(share_at(place), share_at(place), row_send.at[hop], row_recv.at[hop],
                      (mine, at_chip(hop)))

    def pair(hop):
        owner = at_chip(chips - hop)
        return remote(share_at(owner), share_at(owner), pair_send.at[hop], pair_recv.at[hop],
                      (mine, sibling))

    share = lax.dot_general(
        table[...].reshape(-1, tok), home[...].reshape(-1, home.shape[-1]), CONTRACT_FIRST, preferred_element_type=jnp.float32
    )
    share = (share + cotangent.astype(jnp.float32)).astype(jnp.bfloat16)
    for part in range(per):
        piece = share[:, part * width : (part + 1) * width]
        blocks[place * per + part] = piece.reshape(2, half, width)
    def far(step):
        peer = mate(mine, step, experts)
        return remote(blocks.at[peer, core], every.at[step, core], far_send.at[step],
                      far_recv.at[step], (peer, place))

    def to_half(step):
        return remote(every.at[step, core], every.at[step, core],
                      half_send.at[step], half_recv.at[step], (mine, sibling))

    def send_share(owner):
        for part in range(per):
            peer = owner * per + part

            @pl.when(peer != mine)
            def _(peer=peer):
                far(mate(mine, peer, experts)).start()

    def product(owner):
        side = weight[:, pl.ds(pl.multiple_of(owner * per * width, per * width), per * width)]
        value = None
        for part in range(per):
            term = lax.dot_general(
                blocks[owner * per + part].reshape(tok, width),
                side[:, part * width : (part + 1) * width],
                CONTRACT_LAST,
                preferred_element_type=jnp.float32,
            )
            value = term if value is None else value + term
        return value

    for hop in range(1, chips):
        row(hop).start()
    pair(0).start()
    send_share(place)
    grad = product(place)
    pair(0).wait_recv()
    send_share(sibling)
    grad = grad + product(sibling)
    for hop in range(1, chips):
        row(hop).wait_recv()
        pair(hop).start()
        send_share(at_chip(chips - hop))
        grad = grad + product(at_chip(chips - hop))
    for hop in range(1, chips):
        pair(hop).wait_recv()
        other = ((chip + chips - hop) % chips) * 2 + 1 - core
        send_share(other)
        grad = grad + product(other)
    every[0] = blocks[mine]
    normalized = saved[...].astype(jnp.float32)
    scaled = normalized * gain[...]
    gate = sigmoid(scaled)
    grad = grad * gate * (1.0 + scaled * (1.0 - gate)) * gain[...]
    lanes = min(channels, 128)
    first = jnp.zeros((tok, lanes), jnp.float32)
    second = jnp.zeros((tok, lanes), jnp.float32)
    for at in range(0, channels, lanes):
        first = first + grad[:, at : at + lanes]
        second = second + grad[:, at : at + lanes] * normalized[:, at : at + lanes]
    sums[place, 0] = jnp.sum(jnp.transpose(first).reshape(lanes // 8, 8, tok), axis=0)
    sums[place, 1] = jnp.sum(jnp.transpose(second).reshape(lanes // 8, 8, tok), axis=0)

    def tell(step):
        return remote(sums.at[place], sums.at[place], sum_send.at[step], sum_recv.at[step],
                      (mine, (place + step) % groups))

    def start_tell(step, carry):
        tell(step).start()
        return carry

    def wait_tell(step, carry):
        tell(step).wait()
        return carry

    lax.fori_loop(1, groups, start_tell, 0)
    lax.fori_loop(1, groups, wait_tell, 0)
    count = channels * groups
    total = jnp.sum(sums[...], axis=0)

    def column(kind):
        flat = jnp.sum(total[kind], axis=0, keepdims=True) / count
        return jnp.transpose(jnp.broadcast_to(flat, (lanes, tok)))

    mean, slope = column(0), column(1)
    deviation = jnp.transpose(jnp.broadcast_to(inverse[...], (lanes, tok)))
    for at in range(0, channels, lanes):
        extended[at // lanes, 0:tok] = deviation * (
            grad[:, at : at + lanes] - mean - normalized[:, at : at + lanes] * slope
        )
    reach = extended.shape[1] - tok

    def halo():
        return remote(extended.at[:, pl.ds(0, reach)], extended.at[:, pl.ds(tok, reach)],
                      halo_send, halo_recv, ((mine + experts - 1) % experts, place))

    @pl.when(mine > 0)
    def _():
        halo().start()

    @pl.when(mine == experts - 1)
    def _():
        extended[:, tok : tok + reach] = jnp.zeros((channels // lanes, reach, lanes), jnp.float32)

    def forward(step, carry):
        far(step).wait_recv()
        to_half(step).start()
        return carry

    lax.fori_loop(1, experts, forward, 0)

    @pl.when(mine < experts - 1)
    def _():
        halo().wait_recv()

    def arrive(step, carry):
        to_half(step).wait_recv()
        return carry

    lax.fori_loop(1, experts, arrive, 0)
    @pl.when(mine > 0)
    def _():
        halo().wait_send()

    for hop in range(chips):
        pair(hop).wait_send()
        if hop:
            row(hop).wait_send()

    def finish(step, carry):
        far(step).wait_send()
        to_half(step).wait_send()
        return carry

    lax.fori_loop(1, experts, finish, 0)


def last_kernel(
    lead, every, acts, crossed, extended, taps, gate, up, down, result_far, proj_far, gate_far, up_far, down_far,
    result, proj, sems
):
    stores = [
        pltpu.make_async_copy(source, target, sems.at[at])
        for at, (source, target) in enumerate(
            (
                (gate, gate_far), (up, up_far), (down, down_far), (result, result_far),
                (proj, proj_far),
            )
        )
    ]
    for store in stores[:3]:
        store.start()
    tok, channels = result.shape
    lanes = extended.shape[-1]
    for at in range(0, channels, lanes):
        value = jnp.zeros((tok, lanes), jnp.float32)
        for tap in range(taps.shape[0]):
            value = value + taps[tap : tap + 1, at : at + lanes] * extended[at // lanes, tap : tap + tok]
        result[:, at : at + lanes] = value.astype(result.dtype)
    stores[3].start()
    def product(hop, right):
        return lax.dot_general(
            every[:, hop].reshape(-1, every.shape[-1]),
            right.reshape(-1, channels),
            CONTRACT_FIRST,
            preferred_element_type=jnp.float32,
        )

    value = product(0, acts[...])
    for hop in range(1, lead):
        value = value + product(hop, crossed[hop - 1])
    proj[...] = value
    stores[4].start()
    for store in stores:
        store.wait()


def last_blocks(every, acts, crossed, extended, taps, gate, up, down):
    across, tok, channels = acts.shape
    lead = every.shape[0] // across
    every = every.reshape((across, lead) + every.shape[1:])
    vmem = pl.BlockSpec(memory_space=pltpu.VMEM)
    shapes = (
        jax.ShapeDtypeStruct((tok, channels), jnp.bfloat16),
        jax.ShapeDtypeStruct((every.shape[-1], channels), jnp.float32),
    )
    return pl.pallas_call(
        functools.partial(last_kernel, lead),
        out_shape=shapes
        + tuple(jax.ShapeDtypeStruct(array.shape, array.dtype) for array in (gate, up, down)),
        in_specs=[vmem] * 8,
        out_specs=[pl.BlockSpec(memory_space=pltpu.HBM)] * 5,
        scratch_shapes=[pltpu.VMEM(shape.shape, shape.dtype) for shape in shapes]
        + [pltpu.SemaphoreType.DMA((5,))],
        compiler_params=pltpu.CompilerParams(vmem_limit_bytes=16 * 2**20),
        cost_estimate=pl.CostEstimate(flops=10**9, bytes_accessed=10**7, transcendentals=0),
    )(every, acts, crossed, extended, taps, gate, up, down)


def shards(
    cotangent,
    mixer_out,
    expert_ids,
    route_weight,
    saved_normalized,
    inverse_deviation,
    channel_norm_gain,
    taps,
    proj_weight,
    gate_weight,
    up_weight,
    down_weight,
):
    experts = lax.axis_size("sp")
    groups = lax.axis_size("tp")
    grad_first, grad_third, grad_second, acts, crossed, every, extended = expert_blocks(
        jnp.transpose(expert_ids),
        jnp.transpose(route_weight),
        mixer_out,
        cotangent,
        gate_weight[0],
        up_weight[0],
        down_weight[0],
        saved_normalized,
        channel_norm_gain[None, :],
        proj_weight,
        inverse_deviation[None, :],
        (taps.shape[0] + 6) // 8 * 8,
        experts,
        groups,
    )
    result, grad_proj, grad_first, grad_third, grad_second = last_blocks(
        every, acts, crossed, extended, taps, grad_first, grad_third, grad_second
    )
    return (
        result,
        grad_proj,
        grad_first[None],
        grad_third[None],
        grad_second[None],
    )


def solution(mesh):
    return jax.shard_map(
        shards,
        mesh=mesh,
        in_specs=(
            P("sp", None),
            P("sp", None),
            P("sp", None),
            P("sp", None),
            P("sp", "tp"),
            P("sp"),
            P("tp"),
            P(None, "tp"),
            P("tp", None),
            P("sp", None, "tp"),
            P("sp", None, "tp"),
            P("sp", "tp", None),
        ),
        out_specs=(
            P("sp", "tp"),
            P("sp", "tp"),
            P("sp", None, "tp"),
            P("sp", None, "tp"),
            P("sp", "tp", None),
        ),
        check_vma=False,
    )
```

```python
import functools

import jax
import jax.numpy as jnp
from jax import lax
from jax.experimental import pallas as pl
from jax.experimental.pallas import tpu as pltpu
from jax.sharding import PartitionSpec as P


def line_width(experts):
    width = 1
    while 4 * width * width <= experts and experts % (2 * width) == 0:
        width = 2 * width
    return width


def sigmoid(value):
    return 1.0 / (1.0 + jnp.exp(-value))


def mate(index, step, count):
    if count & (count - 1):
        raise ValueError("count")
    value, bit = 0, 1
    while bit < count:
        value = value + bit * ((index // bit + step // bit) % 2)
        bit = 2 * bit
    return value


def remote(source, target, send_sem, recv_sem, device):
    return pltpu.make_async_remote_copy(
        src_ref=source,
        dst_ref=target,
        send_sem=send_sem,
        recv_sem=recv_sem,
        device_id=device,
        device_id_type=pl.DeviceIdType.MESH,
    )


CONTRACT_LAST = (((1,), (1,)), ((), ()))
CONTRACT_FIRST = (((0,), (0,)), ((), ()))


def expert_kernel(
    experts, groups, lead, ids_far, route_far, mixer_far, cotangent_far, gate_far, up_far, down_far,
    saved_far, gain_far, weight_far, inverse_far, taps_far, grad_gate, grad_up, grad_down, acts,
    crossed, every, extended, head, ids, route, mixer, cotangent, saved, gain, weight, inverse, taps, home, table,
    blocks, sums, tokens, ids_in, route_in, relayed, more, held, sent, gate_t, up_t, down_t, gate, up, down, hidden_gate, hidden_up, active,
    grad_hg, grad_hu, partial, pair_in, row_out, row_in, total, slot_weight, *sems
):
    (load_sem, far_send, far_recv, row_send, row_recv, pair_send, pair_recv,
     home_send, home_recv, sum_send, sum_recv, back_send, back_recv,
     line_send, line_recv, side_send, side_recv, token_send, token_recv, relay_send,
     relay_recv) = sems[:21]
    mine = lax.axis_index("sp")
    place = lax.axis_index("tp")
    chips = groups // 2
    chip, core = place // 2, place % 2
    sibling = chip * 2 + 1 - core
    tok = mixer.shape[0]
    capacity, share = held.shape[3:]
    slots = experts * capacity

    def at_chip(step):
        return ((chip + step) % chips) * 2 + core

    loads = [
        pltpu.make_async_copy(source, target, load_sem.at[at])
        for at, (source, target) in enumerate(
            (
                (ids_far, ids), (route_far, route), (mixer_far, mixer), (cotangent_far, cotangent),
                (gate_far, gate), (up_far, up), (down_far, down), (saved_far, saved),
                (gain_far, gain), (weight_far, weight), (inverse_far, inverse),
                (taps_far, taps),
            )
        )
    ]
    for load in loads:
        load.start()
    barrier = pltpu.get_barrier_semaphore()

    def greet(step, carry):
        pl.semaphore_signal(barrier, inc=1, device_id=((mine + step) % experts, place),
                            device_id_type=pl.DeviceIdType.MESH)
        return carry

    lax.fori_loop(1, experts, greet, 0)

    def greet_group(step, carry):
        pl.semaphore_signal(barrier, inc=1, device_id=(mine, (place + step) % groups),
                            device_id_type=pl.DeviceIdType.MESH)
        return carry

    lax.fori_loop(1, groups, greet_group, 0)
    first = experts // 2
    base = mine // first * first
    columns = pl.ds(pl.multiple_of(place * share, share), share)
    for load in loads[:4]:
        load.wait()
    pl.semaphore_wait(barrier, experts + groups - 2)
    opposite = mate(mine, first, experts)
    crossing = [
        remote(source, target, token_send.at[at], token_recv.at[at], (opposite, place))
        for at, (source, target) in enumerate(
            (
                (ids, ids_in), (route, route_in), (mixer.at[:, columns], tokens.at[0]),
                (cotangent.at[:, columns], tokens.at[1]),
            )
        )
    ]
    crossing[0].start()
    crossing[1].start()

    def slot_table(chosen_ids, weights, low, count):
        expert = lax.broadcasted_iota(jnp.int32, (experts, tok), 0)
        hot = [(chosen_ids[k : k + 1] == expert).astype(jnp.float32) for k in range(ids.shape[0])]
        before = lax.broadcasted_iota(jnp.int32, (tok, tok), 0)
        after = lax.broadcasted_iota(jnp.int32, (tok, tok), 1)
        rank = jnp.dot(
            sum(hot).astype(jnp.bfloat16),
            (before < after).astype(jnp.float32).astype(jnp.bfloat16),
            preferred_element_type=jnp.float32,
        )
        slot = expert.astype(jnp.float32) * capacity + rank
        number = (lax.broadcasted_iota(jnp.int32, (count, tok), 0) + low).astype(jnp.float32)
        chosen = jnp.zeros((count, tok), jnp.float32)
        weighted = jnp.zeros((count, tok), jnp.float32)
        for k in range(ids.shape[0]):
            match = number == jnp.sum(hot[k] * slot, axis=0, keepdims=True)
            chosen = jnp.where(match, 1.0, chosen)
            weighted = jnp.where(match, weights[k : k + 1], weighted)
        return chosen.astype(jnp.bfloat16), jnp.sum(weighted, axis=1, keepdims=True)

    def pick(picks, values):
        return jnp.dot(picks, values, preferred_element_type=jnp.float32)

    every_slot, scale = slot_table(ids[...], route[...], 0, slots)
    table[...] = every_slot.reshape(experts, capacity, tok)
    slot_weight[...] = scale.reshape(experts, capacity, 1)
    near = table[pl.ds(base, first)].reshape(first * capacity, tok)
    near_scale = slot_weight[pl.ds(base, first)].reshape(first * capacity, 1)
    sent[:, 0] = pick(near, mixer[:, columns]).astype(jnp.bfloat16).reshape(first, capacity, share)
    sent[:, 1] = (
        (near_scale * pick(near, cotangent[:, columns]))
        .astype(jnp.bfloat16).reshape(first, capacity, share)
    )

    def far(step):
        peer = mate(mine, step, experts)
        return remote(sent.at[peer - base], held.at[step, place],
                      far_send.at[step], far_recv.at[step], (peer, place))

    def row(step, hop):
        block = held.at[step, place]
        return remote(block, block, row_send.at[step, hop], row_recv.at[step, hop],
                      (mine, at_chip(hop)))

    def pair(step, hop):
        block = held.at[step, at_chip(chips - hop)]
        return remote(block, block, pair_send.at[step, hop], pair_recv.at[step, hop],
                      (mine, sibling))

    def each(low, high, act):
        def body(step, carry):
            act(step)
            return carry

        lax.fori_loop(low, high, body, 0)

    def extra(step, hop):
        return remote(more.at[hop - 1, step - 1], held.at[step, at_chip(chips - hop)],
                      row_send.at[step, hop], row_recv.at[step, hop],
                      (mate(mine, step, experts), place))

    each(1, first, lambda step: far(step).start())
    for hop in range(1, chips):
        other = pl.ds(pl.multiple_of(at_chip(chips - hop) * share, share), share)
        for step in range(1, lead):
            peer = mate(mine, step, experts)
            picks = table[peer]
            more[hop - 1, step - 1, 0] = pick(picks, mixer[:, other]).astype(jnp.bfloat16)
            more[hop - 1, step - 1, 1] = (
                slot_weight[peer] * pick(picks, cotangent[:, other])
            ).astype(jnp.bfloat16)
            extra(step, hop).start()
    crossing[2].start()
    crossing[3].start()

    def relay(kind, step):
        peer = mate(mine, step, experts)
        return remote(relayed.at[peer - base, kind], held.at[step + first, place, kind],
                      relay_send.at[kind, step], relay_recv.at[kind, step], (peer, place))

    own = table[mine]
    own_scale = slot_weight[mine]
    for g in range(groups):
        span = slice(g * share, (g + 1) * share)
        held[0, g, 0] = jnp.dot(
            own, mixer[:, span], preferred_element_type=jnp.float32
        ).astype(jnp.bfloat16)
        held[0, g, 1] = (
            own_scale * jnp.dot(own, cotangent[:, span], preferred_element_type=jnp.float32)
        ).astype(jnp.bfloat16)

    across = experts // lead
    line, side = mine // lead, mine % lead

    def along(step, bit):
        peer = mate(line, bit, across) * lead + side
        return remote(acts.at[step], acts.at[step + bit], line_send.at[step + bit],
                      line_recv.at[step + bit], (peer, place))

    acts_order = sorted(range(1, across), key=lambda step: -(step & -step))

    def spread(step):
        bit = 1
        while bit < across:
            if step % (2 * bit) == 0:
                along(step, bit).start()
            bit = 2 * bit

    def reached(step):
        bit = 1
        while step % (2 * bit) == 0:
            bit = 2 * bit
        return along(step - bit, bit)

    def beside(step, hop):
        return remote(acts.at[step], crossed.at[hop - 1, step], side_send.at[step, hop],
                      side_recv.at[step, hop], (line * lead + mate(side, hop, lead), place))

    def cross(step):
        for hop in range(1, lead):
            beside(step, hop).start()

    def extend(step):
        reached(step).wait_recv()
        spread(step)

    def early_acts():
        spread(0)
        cross(0)

    def relay_acts():
        for step in acts_order:
            if step & (step - 1) == 0 and step > 1:
                extend(step)

    def later_acts():
        for step in acts_order:
            if step & (step - 1) or step == 1:
                extend(step)
            cross(step)

    def finish_acts():
        for step in range(1, across):
            reached(step).wait_send()
        for step in range(across):
            for hop in range(1, lead):
                beside(step, hop).wait()

    loads[7].wait()
    loads[8].wait()
    scaled = saved[...].astype(jnp.float32) * gain[...]
    acts[0] = (scaled * sigmoid(scaled)).astype(jnp.bfloat16)

    def greeted(step):
        far(step).wait_recv()
        pair(step, 0).start()

    def service(step):
        far(step).wait_recv()
        hand_on(step)

    def serve(step):
        relay(0, step - first).wait_recv()
        relay(1, step - first).wait_recv()
        hand_on(step)

    def hand_on(step):
        for hop in range(1, chips):
            row(step, hop).start()
        pair(step, 0).start()

    def settle(step):
        for hop in range(1, chips):
            row(step, hop).wait_recv()
            pair(step, hop).start()

    def complete(step):
        for hop in range(chips):
            pair(step, hop).wait_recv()

    def chunk(kind, low, high, g):
        return held[low:high, g, kind].reshape((high - low) * capacity, share)

    crossing[0].wait_recv()
    crossing[1].wait_recv()
    far_table, far_scale = slot_table(ids_in[...], route_in[...], base * capacity, first * capacity)

    def relay_kind(kind):
        crossing[kind + 2].wait_recv()
        value = pick(far_table, tokens[kind])
        if kind:
            value = far_scale * value
        relayed[:, kind] = value.astype(jnp.bfloat16).reshape(first, capacity, share)
        each(1, first, lambda step: relay(kind, step).start())
        held[first, place, kind] = relayed[mine - base, kind]

    def turn_weights():
        for load in loads[4:7]:
            load.wait()
        for g in range(groups):
            span = slice(g * share, (g + 1) * share)
            gate_t[:, span] = jnp.transpose(gate[span, :])
            up_t[:, span] = jnp.transpose(up[span, :])
            down_t[span, :] = jnp.transpose(down[:, span])

    def ahead(low, high):
        lines = slice(low * capacity, high * capacity)
        for matrix, result in ((gate, hidden_gate), (up, hidden_up)):
            value = None
            for g in range(groups):
                term = jnp.dot(
                    chunk(0, low, high, g), matrix[g * share : (g + 1) * share, :],
                    preferred_element_type=jnp.float32,
                )
                value = term if value is None else value + term
            result[lines, :] = value

    def back(low, high):
        lines = slice(low * capacity, high * capacity)
        value = None
        for g in range(groups):
            term = jnp.dot(
                chunk(1, low, high, g), down_t[g * share : (g + 1) * share, :],
                preferred_element_type=jnp.float32,
            )
            value = term if value is None else value + term
        hg = hidden_gate[lines, :]
        hu = hidden_up[lines, :]
        sigma = sigmoid(hg)
        swish = hg * sigma
        active[lines, :] = (swish * hu).astype(jnp.bfloat16)
        grad_hg[lines, :] = (value * hu * sigma * (1.0 + hg * (1.0 - sigma))).astype(jnp.bfloat16)
        grad_hu[lines, :] = (value * swish).astype(jnp.bfloat16)
        for g in range(groups):
            term = jnp.dot(
                grad_hg[lines, :], gate_t[:, g * share : (g + 1) * share],
                preferred_element_type=jnp.float32,
            ) + jnp.dot(
                grad_hu[lines, :], up_t[:, g * share : (g + 1) * share],
                preferred_element_type=jnp.float32,
            )
            partial[g, low:high] = term.astype(jnp.bfloat16).reshape(high - low, capacity, share)

    def weight_grads(g):
        span = pl.ds(pl.multiple_of(g * share, share), share)
        left = held[:, g, 0].reshape(slots, share)
        grad_gate[span, :] = lax.dot_general(
            left, grad_hg[...], CONTRACT_FIRST, preferred_element_type=jnp.float32
        ).astype(jnp.bfloat16)
        grad_up[span, :] = lax.dot_general(
            left, grad_hu[...], CONTRACT_FIRST, preferred_element_type=jnp.float32
        ).astype(jnp.bfloat16)
        grad_down[:, span] = lax.dot_general(
            active[...], held[:, g, 1].reshape(slots, share), CONTRACT_FIRST,
            preferred_element_type=jnp.float32,
        ).astype(jnp.bfloat16)

    def home_pair(step, hop):
        other = ((chip + hop) % chips) * 2 + 1 - core
        return remote(partial.at[other, step], pair_in.at[hop, step],
                      home_send.at[step, hop], home_recv.at[step, hop], (mine, sibling))

    def home_row(step, hop):
        return remote(row_out.at[hop, step], row_in.at[hop, step],
                      sum_send.at[step, hop], sum_recv.at[step, hop], (mine, at_chip(hop)))

    def home_far(step):
        owner = mate(mine, step, experts)
        return remote(total.at[step], home.at[mine],
                      back_send.at[step], back_recv.at[step], (owner, place))

    def start_pair(step):
        for hop in reversed(range(chips)):
            home_pair(step, hop).start()

    def add_pair(step, hop):
        home_pair(step, hop).wait_recv()
        return partial[at_chip(hop), step].astype(jnp.float32) + pair_in[hop, step].astype(
            jnp.float32
        )

    def send_rows(step):
        for hop in range(1, chips):
            row_out[hop, step] = add_pair(step, hop).astype(row_out.dtype)
            home_row(step, hop).start()

    def add_rows(step):
        value = add_pair(step, 0)
        for hop in range(1, chips):
            home_row(step, hop).wait_recv()
            value = value + row_in[hop, step].astype(jnp.float32)
        return value.astype(total.dtype)

    def send_home(step):
        total[step] = add_rows(step)
        home_far(step).start()

    second = 3 * experts // 4
    each(1, lead, greeted)
    turn_weights()
    each(lead, first, service)
    relay_kind(0)
    relay_kind(1)
    hand_on(first)
    each(1, first, settle)
    each(first + 1, second, serve)
    each(1, first, complete)
    ahead(0, first)
    each(second, experts, serve)
    back(0, first)
    each(0, first, start_pair)
    early_acts()
    each(first, second, settle)
    each(first, second, complete)
    ahead(first, second)
    back(first, second)
    each(first, second, start_pair)
    each(second, second + 1, settle)
    each(first, second, send_rows)
    each(second + 1, experts, settle)
    each(0, first // 2, send_rows)
    each(second, experts, complete)
    ahead(second, experts)
    back(second, experts)
    each(second, experts, start_pair)
    each(first, second, send_home)
    weight_grads(0)
    each(second, experts, send_rows)
    each(first // 2, first, send_rows)
    relay_acts()
    each(1, groups - 1, weight_grads)
    each(second, experts, send_home)
    home[mine] = add_rows(0)
    each(1, first // 2, send_home)
    weight_grads(groups - 1)
    each(first // 2, first, send_home)
    later_acts()

    def return_done(step):
        home_far(step).wait_recv()

    each(1, experts, return_done)
    loads[9].wait()
    loads[10].wait()
    loads[11].wait()
    tail_part(
        experts, groups, mine, place, table, home, cotangent[:, columns], saved, inverse, gain,
        weight, taps, every, extended, head, blocks, sums, *sems[21:],
    )

    def finish(step):
        for hop in range(chips):
            home_pair(step, hop).wait_send()
            if hop:
                home_row(step, hop).wait_send()

    def finish_far(step):
        home_far(step).wait_send()
        for hop in range(chips):
            pair(step, hop).wait_send()
            if hop:
                row(step, hop).wait_send()

    finish_acts()
    each(0, experts, finish)
    each(1, experts, finish_far)

    def finish_near(step):
        far(step).wait_send()
        relay(0, step).wait_send()
        relay(1, step).wait_send()

    each(1, first, finish_near)
    for copy in crossing:
        copy.wait_send()


def expert_blocks(
    ids, route, mixer, cotangent, gate, up, down, saved, gain, weight, inverse, taps, experts,
    groups,
):
    tok, width = mixer.shape
    ff = gate.shape[1]
    share = width // groups
    capacity = groups * max(1, 4 * tok // (experts * groups))
    chips = groups // 2
    slots = experts * capacity
    lead = line_width(experts)
    across = experts // lead
    half = jnp.bfloat16
    dma = pltpu.SemaphoreType.DMA
    vmem = pl.BlockSpec(memory_space=pltpu.VMEM)
    held = pltpu.VMEM((experts, groups, 2, capacity, share), half)
    sent = pltpu.VMEM((experts // 2, 2, capacity, share), half)
    kept = pltpu.VMEM((experts, capacity, share), half)
    blocks = pltpu.VMEM((chips, experts, capacity, share), half)
    channels = saved.shape[1]
    lanes = min(channels, 128)
    columns = width // experts
    reach = (taps.shape[0] + 6) // 8 * 8
    outs = tuple(jax.ShapeDtypeStruct(array.shape, half) for array in (gate, up, down)) + (
        jax.ShapeDtypeStruct((across,) + saved.shape, half),
        jax.ShapeDtypeStruct((lead - 1, across) + saved.shape, half),
        jax.ShapeDtypeStruct((experts, 2, tok // 2, columns), half),
        jax.ShapeDtypeStruct((channels // lanes, tok + reach, lanes), jnp.float32),
        jax.ShapeDtypeStruct((tok - reach, channels), half),
    )
    inputs = (ids, route, mixer, cotangent, gate, up, down, saved, gain, weight, inverse, taps)
    return pl.pallas_call(
        functools.partial(expert_kernel, experts, groups, lead),
        out_shape=outs,
        in_specs=[pl.BlockSpec(memory_space=pltpu.HBM)] * len(inputs),
        out_specs=[vmem] * len(outs),
        scratch_shapes=[
            pltpu.VMEM(array.shape, array.dtype)
            for array in (ids, route, mixer, cotangent, saved, gain, weight, inverse, taps)
        ]
        + [
            kept,
            pltpu.VMEM((experts, capacity, tok), half),
            pltpu.VMEM((experts, 2, tok // 2, columns), half),
            pltpu.VMEM((groups, 2, 8, tok), jnp.float32),
            pltpu.VMEM((2, tok, share), half),
            pltpu.VMEM(ids.shape, ids.dtype),
            pltpu.VMEM(route.shape, route.dtype),
            sent,
            pltpu.VMEM((chips - 1, lead - 1, 2, capacity, share), half),
        ]
        + [held, sent]
        + [pltpu.VMEM(array.shape[::-1], half) for array in (gate, up, down)]
        + [pltpu.VMEM(array.shape, half) for array in (gate, up, down)]
        + [pltpu.VMEM((slots, ff), jnp.float32)] * 2
        + [pltpu.VMEM((slots, ff), half)] * 3
        + [pltpu.VMEM((groups, experts, capacity, share), half)]
        + [blocks] * 3
        + [kept, pltpu.VMEM((experts, capacity, 1), jnp.float32)]
        + [dma((12,))]
        + [dma((experts,))] * 2
        + [dma((experts, chips))] * 8
        + [dma((experts,))] * 2
        + [dma((across,))] * 2
        + [dma((across, lead))] * 2
        + [dma((4,))] * 2
        + [dma((2, experts // 2))] * 2
        + [dma((chips,))] * 4
        + [dma((experts,))] * 4
        + [dma((groups,))] * 2
        + [dma] * 2,
        compiler_params=pltpu.CompilerParams(
            collective_id=0, has_side_effects=True, vmem_limit_bytes=42 * 2**20
        ),
        cost_estimate=pl.CostEstimate(flops=10**10, bytes_accessed=10**7, transcendentals=0),
    )(
        *(
            pltpu.with_memory_space_constraint(array, pltpu.HBM)
            for array in inputs
        )
    )


def convolve(taps, extended, at, lanes, low, rows):
    value = jnp.zeros((rows, lanes), jnp.float32)
    for tap in range(taps.shape[0]):
        value = value + taps[tap : tap + 1, at : at + lanes] * (
            extended[at // lanes, low + tap : low + tap + rows]
        )
    return value


def tail_part(
    experts, groups, mine, place, table, home, cotangent, saved, inverse, gain, weight,
    taps, every, extended, head, blocks, sums, *sems
):
    (row_send, row_recv, pair_send, pair_recv, far_send, far_recv, half_send, half_recv,
     sum_send, sum_recv, halo_send, halo_recv) = sems
    chips = groups // 2
    chip, core = place // 2, place % 2
    sibling = chip * 2 + 1 - core
    tok = saved.shape[0]
    channels = saved.shape[1]
    width = blocks.shape[-1]
    per = experts // groups
    half = tok // 2

    def at_chip(step):
        return ((chip + step) % chips) * 2 + core

    def share_at(owner):
        return blocks.at[pl.ds(owner * per, per)]

    def row(hop):
        return remote(share_at(place), share_at(place), row_send.at[hop], row_recv.at[hop],
                      (mine, at_chip(hop)))

    def pair(hop):
        owner = at_chip(chips - hop)
        return remote(share_at(owner), share_at(owner), pair_send.at[hop], pair_recv.at[hop],
                      (mine, sibling))

    share = lax.dot_general(
        table[...].reshape(-1, tok), home[...].reshape(-1, home.shape[-1]), CONTRACT_FIRST, preferred_element_type=jnp.float32
    )
    share = (share + cotangent.astype(jnp.float32)).astype(jnp.bfloat16)
    for part in range(per):
        piece = share[:, part * width : (part + 1) * width]
        blocks[place * per + part] = piece.reshape(2, half, width)
    def far(step):
        peer = mate(mine, step, experts)
        return remote(blocks.at[peer, core], every.at[step, core], far_send.at[step],
                      far_recv.at[step], (peer, place))

    def to_half(step):
        return remote(every.at[step, core], every.at[step, core],
                      half_send.at[step], half_recv.at[step], (mine, sibling))

    def send_share(owner):
        for part in range(per):
            peer = owner * per + part

            @pl.when(peer != mine)
            def _(peer=peer):
                far(mate(mine, peer, experts)).start()

    def product(owner):
        side = weight[:, pl.ds(pl.multiple_of(owner * per * width, per * width), per * width)]
        value = None
        for part in range(per):
            term = lax.dot_general(
                blocks[owner * per + part].reshape(tok, width),
                side[:, part * width : (part + 1) * width],
                CONTRACT_LAST,
                preferred_element_type=jnp.float32,
            )
            value = term if value is None else value + term
        return value

    for hop in range(1, chips):
        row(hop).start()
    pair(0).start()
    send_share(place)
    grad = product(place)
    pair(0).wait_recv()
    send_share(sibling)
    grad = grad + product(sibling)
    for hop in range(1, chips):
        row(hop).wait_recv()
        pair(hop).start()
        send_share(at_chip(chips - hop))
        grad = grad + product(at_chip(chips - hop))
    for hop in range(1, chips):
        pair(hop).wait_recv()
        other = ((chip + chips - hop) % chips) * 2 + 1 - core
        send_share(other)
        grad = grad + product(other)
    every[0] = blocks[mine]
    normalized = saved[...].astype(jnp.float32)
    scaled = normalized * gain[...]
    gate = sigmoid(scaled)
    grad = grad * gate * (1.0 + scaled * (1.0 - gate)) * gain[...]
    lanes = min(channels, 128)
    first = jnp.zeros((tok, lanes), jnp.float32)
    second = jnp.zeros((tok, lanes), jnp.float32)
    for at in range(0, channels, lanes):
        first = first + grad[:, at : at + lanes]
        second = second + grad[:, at : at + lanes] * normalized[:, at : at + lanes]
    sums[place, 0] = jnp.sum(jnp.transpose(first).reshape(lanes // 8, 8, tok), axis=0)
    sums[place, 1] = jnp.sum(jnp.transpose(second).reshape(lanes // 8, 8, tok), axis=0)

    def tell(step):
        return remote(sums.at[place], sums.at[place], sum_send.at[step], sum_recv.at[step],
                      (mine, (place + step) % groups))

    def start_tell(step, carry):
        tell(step).start()
        return carry

    def wait_tell(step, carry):
        tell(step).wait()
        return carry

    lax.fori_loop(1, groups, start_tell, 0)
    lax.fori_loop(1, groups, wait_tell, 0)
    count = channels * groups
    total = jnp.sum(sums[...], axis=0)

    def column(kind):
        flat = jnp.sum(total[kind], axis=0, keepdims=True) / count
        return jnp.transpose(jnp.broadcast_to(flat, (lanes, tok)))

    mean, slope = column(0), column(1)
    deviation = jnp.transpose(jnp.broadcast_to(inverse[...], (lanes, tok)))
    for at in range(0, channels, lanes):
        extended[at // lanes, 0:tok] = deviation * (
            grad[:, at : at + lanes] - mean - normalized[:, at : at + lanes] * slope
        )
    reach = extended.shape[1] - tok

    def halo():
        return remote(extended.at[:, pl.ds(0, reach)], extended.at[:, pl.ds(tok, reach)],
                      halo_send, halo_recv, ((mine + experts - 1) % experts, place))

    @pl.when(mine > 0)
    def _():
        halo().start()

    @pl.when(mine == experts - 1)
    def _():
        extended[:, tok : tok + reach] = jnp.zeros((channels // lanes, reach, lanes), jnp.float32)

    def forward(step, carry):
        far(step).wait_recv()
        to_half(step).start()
        return carry

    lax.fori_loop(1, experts, forward, 0)
    for at in range(0, channels, lanes):
        head[:, at : at + lanes] = convolve(
            taps, extended, at, lanes, 0, head.shape[0]
        ).astype(head.dtype)

    @pl.when(mine < experts - 1)
    def _():
        halo().wait_recv()

    def arrive(step, carry):
        to_half(step).wait_recv()
        return carry

    lax.fori_loop(1, experts, arrive, 0)
    @pl.when(mine > 0)
    def _():
        halo().wait_send()

    for hop in range(chips):
        pair(hop).wait_send()
        if hop:
            row(hop).wait_send()

    def finish(step, carry):
        far(step).wait_send()
        to_half(step).wait_send()
        return carry

    lax.fori_loop(1, experts, finish, 0)


def last_kernel(
    lead, every, acts, crossed, extended, head, taps, gate, up, down, result_far, proj_far, gate_far, up_far, down_far,
    result, proj, sems
):
    stores = [
        pltpu.make_async_copy(source, target, sems.at[at])
        for at, (source, target) in enumerate(
            (
                (gate, gate_far), (up, up_far), (down, down_far), (result, result_far.at[pl.ds(head.shape[0], result.shape[0])]),
                (proj, proj_far), (head, result_far.at[pl.ds(0, head.shape[0])]),
            )
        )
    ]
    for store in stores[:3]:
        store.start()
    stores[5].start()
    rows, channels = result.shape
    lanes = extended.shape[-1]
    for at in range(0, channels, lanes):
        value = convolve(taps, extended, at, lanes, head.shape[0], rows)
        result[:, at : at + lanes] = value.astype(result.dtype)
    stores[3].start()
    def product(hop, right):
        return lax.dot_general(
            every[:, hop].reshape(-1, every.shape[-1]),
            right.reshape(-1, channels),
            CONTRACT_FIRST,
            preferred_element_type=jnp.float32,
        )

    value = product(0, acts[...])
    for hop in range(1, lead):
        value = value + product(hop, crossed[hop - 1])
    proj[...] = value
    stores[4].start()
    for store in stores:
        store.wait()


def last_blocks(every, acts, crossed, extended, head, taps, gate, up, down):
    across, tok, channels = acts.shape
    lead = every.shape[0] // across
    every = every.reshape((across, lead) + every.shape[1:])
    vmem = pl.BlockSpec(memory_space=pltpu.VMEM)
    shapes = (
        jax.ShapeDtypeStruct((tok, channels), jnp.bfloat16),
        jax.ShapeDtypeStruct((every.shape[-1], channels), jnp.float32),
    )
    return pl.pallas_call(
        functools.partial(last_kernel, lead),
        out_shape=shapes
        + tuple(jax.ShapeDtypeStruct(array.shape, array.dtype) for array in (gate, up, down)),
        in_specs=[vmem] * 9,
        out_specs=[pl.BlockSpec(memory_space=pltpu.HBM)] * 5,
        scratch_shapes=[
            pltpu.VMEM((tok - head.shape[0], channels), jnp.bfloat16),
            pltpu.VMEM(shapes[1].shape, jnp.float32),
        ]
        + [pltpu.SemaphoreType.DMA((6,))],
        compiler_params=pltpu.CompilerParams(vmem_limit_bytes=16 * 2**20),
        cost_estimate=pl.CostEstimate(flops=10**9, bytes_accessed=10**7, transcendentals=0),
    )(every, acts, crossed, extended, head, taps, gate, up, down)


def shards(
    cotangent,
    mixer_out,
    expert_ids,
    route_weight,
    saved_normalized,
    inverse_deviation,
    channel_norm_gain,
    taps,
    proj_weight,
    gate_weight,
    up_weight,
    down_weight,
):
    experts = lax.axis_size("sp")
    groups = lax.axis_size("tp")
    grad_first, grad_third, grad_second, acts, crossed, every, extended, head = expert_blocks(
        jnp.transpose(expert_ids),
        jnp.transpose(route_weight),
        mixer_out,
        cotangent,
        gate_weight[0],
        up_weight[0],
        down_weight[0],
        saved_normalized,
        channel_norm_gain[None, :],
        proj_weight,
        inverse_deviation[None, :],
        taps,
        experts,
        groups,
    )
    result, grad_proj, grad_first, grad_third, grad_second = last_blocks(
        every, acts, crossed, extended, head, taps, grad_first, grad_third, grad_second
    )
    return (
        result,
        grad_proj,
        grad_first[None],
        grad_third[None],
        grad_second[None],
    )


def solution(mesh):
    return jax.shard_map(
        shards,
        mesh=mesh,
        in_specs=(
            P("sp", None),
            P("sp", None),
            P("sp", None),
            P("sp", None),
            P("sp", "tp"),
            P("sp"),
            P("tp"),
            P(None, "tp"),
            P("tp", None),
            P("sp", None, "tp"),
            P("sp", None, "tp"),
            P("sp", "tp", None),
        ),
        out_specs=(
            P("sp", "tp"),
            P("sp", "tp"),
            P("sp", None, "tp"),
            P("sp", None, "tp"),
            P("sp", "tp", None),
        ),
        check_vma=False,
    )
```

```python
import functools

import jax
import jax.numpy as jnp
from jax import lax
from jax.experimental import pallas as pl
from jax.experimental.pallas import tpu as pltpu
from jax.sharding import PartitionSpec as P


def line_width(experts):
    width = 1
    while 4 * width * width <= experts and experts % (2 * width) == 0:
        width = 2 * width
    return width


def sigmoid(value):
    return 1.0 / (1.0 + jnp.exp(-value))


def mate(index, step, count):
    if count & (count - 1):
        raise ValueError("count")
    value, bit = 0, 1
    while bit < count:
        value = value + bit * ((index // bit + step // bit) % 2)
        bit = 2 * bit
    return value


def remote(source, target, send_sem, recv_sem, device):
    return pltpu.make_async_remote_copy(
        src_ref=source,
        dst_ref=target,
        send_sem=send_sem,
        recv_sem=recv_sem,
        device_id=device,
        device_id_type=pl.DeviceIdType.MESH,
    )


CONTRACT_LAST = (((1,), (1,)), ((), ()))
CONTRACT_FIRST = (((0,), (0,)), ((), ()))


def expert_kernel(
    experts, groups, lead, ids_far, route_far, mixer_far, cotangent_far, gate_far, up_far, down_far,
    saved_far, gain_far, weight_far, inverse_far, taps_far, grad_gate, grad_up, grad_down, acts,
    crossed, every, extended, head, ids, route, mixer, cotangent, saved, gain, weight, inverse, taps, home, table,
    blocks, sums, tokens, ids_in, route_in, relayed, more, held, sent, gate_t, up_t, down_t, gate, up, down, hidden_gate, hidden_up, active,
    grad_hg, grad_hu, partial, pair_in, row_out, row_in, total, slot_weight, *sems
):
    (load_sem, far_send, far_recv, row_send, row_recv, pair_send, pair_recv,
     home_send, home_recv, sum_send, sum_recv, back_send, back_recv,
     line_send, line_recv, side_send, side_recv, token_send, token_recv, relay_send,
     relay_recv) = sems[:21]
    mine = lax.axis_index("sp")
    place = lax.axis_index("tp")
    chips = groups // 2
    chip, core = place // 2, place % 2
    sibling = chip * 2 + 1 - core
    tok = mixer.shape[0]
    capacity, share = held.shape[3:]
    slots = experts * capacity

    def at_chip(step):
        return ((chip + step) % chips) * 2 + core

    loads = [
        pltpu.make_async_copy(source, target, load_sem.at[at])
        for at, (source, target) in enumerate(
            (
                (ids_far, ids), (route_far, route), (mixer_far, mixer), (cotangent_far, cotangent),
                (gate_far, gate), (up_far, up), (down_far, down), (saved_far, saved),
                (gain_far, gain), (weight_far, weight), (inverse_far, inverse),
                (taps_far, taps),
            )
        )
    ]
    for load in loads:
        load.start()
    barrier = pltpu.get_barrier_semaphore()

    def greet(step, carry):
        pl.semaphore_signal(barrier, inc=1, device_id=((mine + step) % experts, place),
                            device_id_type=pl.DeviceIdType.MESH)
        return carry

    lax.fori_loop(1, experts, greet, 0)

    def greet_group(step, carry):
        pl.semaphore_signal(barrier, inc=1, device_id=(mine, (place + step) % groups),
                            device_id_type=pl.DeviceIdType.MESH)
        return carry

    lax.fori_loop(1, groups, greet_group, 0)
    first = experts // 2
    base = mine // first * first
    columns = pl.ds(pl.multiple_of(place * share, share), share)
    for load in loads[:4]:
        load.wait()
    pl.semaphore_wait(barrier, experts + groups - 2)
    opposite = mate(mine, first, experts)
    crossing = [
        remote(source, target, token_send.at[at], token_recv.at[at], (opposite, place))
        for at, (source, target) in enumerate(
            (
                (ids, ids_in), (route, route_in), (mixer.at[:, columns], tokens.at[0]),
                (cotangent.at[:, columns], tokens.at[1]),
            )
        )
    ]
    crossing[0].start()
    crossing[1].start()

    def slot_table(chosen_ids, weights, low, count):
        expert = lax.broadcasted_iota(jnp.int32, (experts, tok), 0)
        hot = [(chosen_ids[k : k + 1] == expert).astype(jnp.float32) for k in range(ids.shape[0])]
        before = lax.broadcasted_iota(jnp.int32, (tok, tok), 0)
        after = lax.broadcasted_iota(jnp.int32, (tok, tok), 1)
        rank = jnp.dot(
            sum(hot).astype(jnp.bfloat16),
            (before < after).astype(jnp.float32).astype(jnp.bfloat16),
            preferred_element_type=jnp.float32,
        )
        slot = expert.astype(jnp.float32) * capacity + rank
        number = (lax.broadcasted_iota(jnp.int32, (count, tok), 0) + low).astype(jnp.float32)
        chosen = jnp.zeros((count, tok), jnp.float32)
        weighted = jnp.zeros((count, tok), jnp.float32)
        for k in range(ids.shape[0]):
            match = number == jnp.sum(hot[k] * slot, axis=0, keepdims=True)
            chosen = jnp.where(match, 1.0, chosen)
            weighted = jnp.where(match, weights[k : k + 1], weighted)
        return chosen.astype(jnp.bfloat16), jnp.sum(weighted, axis=1, keepdims=True)

    def pick(picks, values):
        return jnp.dot(picks, values, preferred_element_type=jnp.float32)

    every_slot, scale = slot_table(ids[...], route[...], 0, slots)
    table[...] = every_slot.reshape(experts, capacity, tok)
    slot_weight[...] = scale.reshape(experts, capacity, 1)
    near = table[pl.ds(base, first)].reshape(first * capacity, tok)
    near_scale = slot_weight[pl.ds(base, first)].reshape(first * capacity, 1)
    sent[:, 0] = pick(near, mixer[:, columns]).astype(jnp.bfloat16).reshape(first, capacity, share)
    sent[:, 1] = (
        (near_scale * pick(near, cotangent[:, columns]))
        .astype(jnp.bfloat16).reshape(first, capacity, share)
    )

    def far(step):
        peer = mate(mine, step, experts)
        return remote(sent.at[peer - base], held.at[step, place],
                      far_send.at[step], far_recv.at[step], (peer, place))

    def row(step, hop):
        block = held.at[step, place]
        return remote(block, block, row_send.at[step, hop], row_recv.at[step, hop],
                      (mine, at_chip(hop)))

    def pair(step, hop):
        block = held.at[step, at_chip(chips - hop)]
        return remote(block, block, pair_send.at[step, hop], pair_recv.at[step, hop],
                      (mine, sibling))

    def each(low, high, act):
        def body(step, carry):
            act(step)
            return carry

        lax.fori_loop(low, high, body, 0)

    def extra(step, hop):
        return remote(more.at[hop - 1, step - 1], held.at[step, at_chip(chips - hop)],
                      row_send.at[step, hop], row_recv.at[step, hop],
                      (mate(mine, step, experts), place))

    each(1, first, lambda step: far(step).start())
    for hop in range(1, chips):
        other = pl.ds(pl.multiple_of(at_chip(chips - hop) * share, share), share)
        for step in range(1, lead):
            peer = mate(mine, step, experts)
            picks = table[peer]
            more[hop - 1, step - 1, 0] = pick(picks, mixer[:, other]).astype(jnp.bfloat16)
            more[hop - 1, step - 1, 1] = (
                slot_weight[peer] * pick(picks, cotangent[:, other])
            ).astype(jnp.bfloat16)
            extra(step, hop).start()
    crossing[2].start()
    crossing[3].start()

    def relay(kind, step):
        peer = mate(mine, step, experts)
        return remote(relayed.at[peer - base, kind], held.at[step + first, place, kind],
                      relay_send.at[kind, step], relay_recv.at[kind, step], (peer, place))

    own = table[mine]
    own_scale = slot_weight[mine]
    for g in range(groups):
        span = slice(g * share, (g + 1) * share)
        held[0, g, 0] = jnp.dot(
            own, mixer[:, span], preferred_element_type=jnp.float32
        ).astype(jnp.bfloat16)
        held[0, g, 1] = (
            own_scale * jnp.dot(own, cotangent[:, span], preferred_element_type=jnp.float32)
        ).astype(jnp.bfloat16)

    across = experts // lead
    line, side = mine // lead, mine % lead

    def along(step, bit):
        peer = mate(line, bit, across) * lead + side
        return remote(acts.at[step], acts.at[step + bit], line_send.at[step + bit],
                      line_recv.at[step + bit], (peer, place))

    acts_order = sorted(range(1, across), key=lambda step: -(step & -step))

    def spread(step):
        bit = 1
        while bit < across:
            if step % (2 * bit) == 0:
                along(step, bit).start()
            bit = 2 * bit

    def reached(step):
        bit = 1
        while step % (2 * bit) == 0:
            bit = 2 * bit
        return along(step - bit, bit)

    def beside(step, hop):
        return remote(acts.at[step], crossed.at[hop - 1, step], side_send.at[step, hop],
                      side_recv.at[step, hop], (line * lead + mate(side, hop, lead), place))

    def cross(step):
        for hop in range(1, lead):
            beside(step, hop).start()

    def extend(step):
        reached(step).wait_recv()
        spread(step)

    def early_acts():
        spread(0)
        cross(0)

    def relay_acts():
        for step in acts_order:
            if step & (step - 1) == 0 and step > 1:
                extend(step)

    def later_acts():
        for step in acts_order:
            if step & (step - 1) or step == 1:
                extend(step)
            cross(step)

    def finish_acts():
        for step in range(1, across):
            reached(step).wait_send()
        for step in range(across):
            for hop in range(1, lead):
                beside(step, hop).wait()

    loads[7].wait()
    loads[8].wait()
    scaled = saved[...].astype(jnp.float32) * gain[...]
    acts[0] = (scaled * sigmoid(scaled)).astype(jnp.bfloat16)

    def greeted(step):
        far(step).wait_recv()
        pair(step, 0).start()

    def service(step):
        far(step).wait_recv()
        hand_on(step)

    def serve(step):
        relay(0, step - first).wait_recv()
        relay(1, step - first).wait_recv()
        hand_on(step)

    def hand_on(step):
        for hop in range(1, chips):
            row(step, hop).start()
        pair(step, 0).start()

    def settle(step):
        for hop in range(1, chips):
            row(step, hop).wait_recv()
            pair(step, hop).start()

    def complete(step):
        for hop in range(chips):
            pair(step, hop).wait_recv()

    def chunk(kind, low, high, g):
        return held[low:high, g, kind].reshape((high - low) * capacity, share)

    crossing[0].wait_recv()
    crossing[1].wait_recv()
    far_table, far_scale = slot_table(ids_in[...], route_in[...], base * capacity, first * capacity)

    def relay_kind(kind):
        crossing[kind + 2].wait_recv()
        value = pick(far_table, tokens[kind])
        if kind:
            value = far_scale * value
        relayed[:, kind] = value.astype(jnp.bfloat16).reshape(first, capacity, share)
        each(1, first, lambda step: relay(kind, step).start())
        held[first, place, kind] = relayed[mine - base, kind]

    def turn_weights():
        for load in loads[4:7]:
            load.wait()
        for g in range(groups):
            span = slice(g * share, (g + 1) * share)
            gate_t[:, span] = jnp.transpose(gate[span, :])
            up_t[:, span] = jnp.transpose(up[span, :])
            down_t[span, :] = jnp.transpose(down[:, span])

    def ahead(low, high):
        lines = slice(low * capacity, high * capacity)
        for matrix, result in ((gate, hidden_gate), (up, hidden_up)):
            value = None
            for g in range(groups):
                term = jnp.dot(
                    chunk(0, low, high, g), matrix[g * share : (g + 1) * share, :],
                    preferred_element_type=jnp.float32,
                )
                value = term if value is None else value + term
            result[lines, :] = value

    def back(low, high):
        lines = slice(low * capacity, high * capacity)
        value = None
        for g in range(groups):
            term = jnp.dot(
                chunk(1, low, high, g), down_t[g * share : (g + 1) * share, :],
                preferred_element_type=jnp.float32,
            )
            value = term if value is None else value + term
        hg = hidden_gate[lines, :]
        hu = hidden_up[lines, :]
        sigma = sigmoid(hg)
        swish = hg * sigma
        active[lines, :] = (swish * hu).astype(jnp.bfloat16)
        grad_hg[lines, :] = (value * hu * sigma * (1.0 + hg * (1.0 - sigma))).astype(jnp.bfloat16)
        grad_hu[lines, :] = (value * swish).astype(jnp.bfloat16)
        for g in range(groups):
            term = jnp.dot(
                grad_hg[lines, :], gate_t[:, g * share : (g + 1) * share],
                preferred_element_type=jnp.float32,
            ) + jnp.dot(
                grad_hu[lines, :], up_t[:, g * share : (g + 1) * share],
                preferred_element_type=jnp.float32,
            )
            partial[g, low:high] = term.astype(jnp.bfloat16).reshape(high - low, capacity, share)

    def weight_grads(g):
        span = pl.ds(pl.multiple_of(g * share, share), share)
        left = held[:, g, 0].reshape(slots, share)
        grad_gate[span, :] = lax.dot_general(
            left, grad_hg[...], CONTRACT_FIRST, preferred_element_type=jnp.float32
        ).astype(jnp.bfloat16)
        grad_up[span, :] = lax.dot_general(
            left, grad_hu[...], CONTRACT_FIRST, preferred_element_type=jnp.float32
        ).astype(jnp.bfloat16)
        grad_down[:, span] = lax.dot_general(
            active[...], held[:, g, 1].reshape(slots, share), CONTRACT_FIRST,
            preferred_element_type=jnp.float32,
        ).astype(jnp.bfloat16)

    def home_pair(step, hop):
        other = ((chip + hop) % chips) * 2 + 1 - core
        return remote(partial.at[other, step], pair_in.at[hop, step],
                      home_send.at[step, hop], home_recv.at[step, hop], (mine, sibling))

    def home_row(step, hop):
        return remote(row_out.at[hop, step], row_in.at[hop, step],
                      sum_send.at[step, hop], sum_recv.at[step, hop], (mine, at_chip(hop)))

    def home_far(step):
        owner = mate(mine, step, experts)
        return remote(total.at[step], home.at[mine],
                      back_send.at[step], back_recv.at[step], (owner, place))

    def start_pair(step):
        for hop in reversed(range(chips)):
            home_pair(step, hop).start()

    def add_pair(step, hop):
        home_pair(step, hop).wait_recv()
        return partial[at_chip(hop), step].astype(jnp.float32) + pair_in[hop, step].astype(
            jnp.float32
        )

    def send_rows(step):
        for hop in range(1, chips):
            row_out[hop, step] = add_pair(step, hop).astype(row_out.dtype)
            home_row(step, hop).start()

    def add_rows(step):
        value = add_pair(step, 0)
        for hop in range(1, chips):
            home_row(step, hop).wait_recv()
            value = value + row_in[hop, step].astype(jnp.float32)
        return value.astype(total.dtype)

    def send_home(step):
        total[step] = add_rows(step)
        home_far(step).start()

    second = 3 * experts // 4
    each(1, lead, greeted)
    turn_weights()
    each(lead, first, service)
    relay_kind(0)
    relay_kind(1)
    hand_on(first)
    each(1, first, settle)
    each(first + 1, second, serve)
    each(1, first, complete)
    each(second, second + 1, serve)
    ahead(0, first)
    each(second + 1, experts, serve)
    back(0, first)
    each(0, first, start_pair)
    early_acts()
    each(first, second, settle)
    each(first, second, complete)
    ahead(first, second)
    back(first, second)
    each(first, second, start_pair)
    each(second, second + 1, settle)
    each(first, second, send_rows)
    each(second + 1, experts, settle)
    each(0, first // 2, send_rows)
    each(second, experts, complete)
    ahead(second, experts)
    back(second, experts)
    each(second, experts, start_pair)
    each(first, second, send_home)
    weight_grads(0)
    each(second, experts, send_rows)
    each(first // 2, first, send_rows)
    relay_acts()
    each(1, groups - 1, weight_grads)
    each(second, experts, send_home)
    home[mine] = add_rows(0)
    each(1, first // 2, send_home)
    weight_grads(groups - 1)
    each(first // 2, first, send_home)
    later_acts()

    def return_done(step):
        home_far(step).wait_recv()

    each(1, experts, return_done)
    loads[9].wait()
    loads[10].wait()
    loads[11].wait()
    tail_part(
        experts, groups, mine, place, table, home, cotangent[:, columns], saved, inverse, gain,
        weight, taps, every, extended, head, blocks, sums, *sems[21:],
    )

    def finish(step):
        for hop in range(chips):
            home_pair(step, hop).wait_send()
            if hop:
                home_row(step, hop).wait_send()

    def finish_far(step):
        home_far(step).wait_send()
        for hop in range(chips):
            pair(step, hop).wait_send()
            if hop:
                row(step, hop).wait_send()

    finish_acts()
    each(0, experts, finish)
    each(1, experts, finish_far)

    def finish_near(step):
        far(step).wait_send()
        relay(0, step).wait_send()
        relay(1, step).wait_send()

    each(1, first, finish_near)
    for copy in crossing:
        copy.wait_send()


def expert_blocks(
    ids, route, mixer, cotangent, gate, up, down, saved, gain, weight, inverse, taps, experts,
    groups,
):
    tok, width = mixer.shape
    ff = gate.shape[1]
    share = width // groups
    capacity = groups * max(1, 4 * tok // (experts * groups))
    chips = groups // 2
    slots = experts * capacity
    lead = line_width(experts)
    across = experts // lead
    half = jnp.bfloat16
    dma = pltpu.SemaphoreType.DMA
    vmem = pl.BlockSpec(memory_space=pltpu.VMEM)
    held = pltpu.VMEM((experts, groups, 2, capacity, share), half)
    sent = pltpu.VMEM((experts // 2, 2, capacity, share), half)
    kept = pltpu.VMEM((experts, capacity, share), half)
    blocks = pltpu.VMEM((chips, experts, capacity, share), half)
    channels = saved.shape[1]
    lanes = min(channels, 128)
    columns = width // experts
    reach = (taps.shape[0] + 6) // 8 * 8
    outs = tuple(jax.ShapeDtypeStruct(array.shape, half) for array in (gate, up, down)) + (
        jax.ShapeDtypeStruct((across,) + saved.shape, half),
        jax.ShapeDtypeStruct((lead - 1, across) + saved.shape, half),
        jax.ShapeDtypeStruct((experts, 2, tok // 2, columns), half),
        jax.ShapeDtypeStruct((channels // lanes, tok + reach, lanes), jnp.float32),
        jax.ShapeDtypeStruct((tok - reach, channels), half),
    )
    inputs = (ids, route, mixer, cotangent, gate, up, down, saved, gain, weight, inverse, taps)
    return pl.pallas_call(
        functools.partial(expert_kernel, experts, groups, lead),
        out_shape=outs,
        in_specs=[pl.BlockSpec(memory_space=pltpu.HBM)] * len(inputs),
        out_specs=[vmem] * len(outs),
        scratch_shapes=[
            pltpu.VMEM(array.shape, array.dtype)
            for array in (ids, route, mixer, cotangent, saved, gain, weight, inverse, taps)
        ]
        + [
            kept,
            pltpu.VMEM((experts, capacity, tok), half),
            pltpu.VMEM((experts, 2, tok // 2, columns), half),
            pltpu.VMEM((groups, 2, 8, tok), jnp.float32),
            pltpu.VMEM((2, tok, share), half),
            pltpu.VMEM(ids.shape, ids.dtype),
            pltpu.VMEM(route.shape, route.dtype),
            sent,
            pltpu.VMEM((chips - 1, lead - 1, 2, capacity, share), half),
        ]
        + [held, sent]
        + [pltpu.VMEM(array.shape[::-1], half) for array in (gate, up, down)]
        + [pltpu.VMEM(array.shape, half) for array in (gate, up, down)]
        + [pltpu.VMEM((slots, ff), jnp.float32)] * 2
        + [pltpu.VMEM((slots, ff), half)] * 3
        + [pltpu.VMEM((groups, experts, capacity, share), half)]
        + [blocks] * 3
        + [kept, pltpu.VMEM((experts, capacity, 1), jnp.float32)]
        + [dma((12,))]
        + [dma((experts,))] * 2
        + [dma((experts, chips))] * 8
        + [dma((experts,))] * 2
        + [dma((across,))] * 2
        + [dma((across, lead))] * 2
        + [dma((4,))] * 2
        + [dma((2, experts // 2))] * 2
        + [dma((chips,))] * 4
        + [dma((experts,))] * 4
        + [dma((groups,))] * 2
        + [dma] * 2,
        compiler_params=pltpu.CompilerParams(
            collective_id=0, has_side_effects=True, vmem_limit_bytes=42 * 2**20
        ),
        cost_estimate=pl.CostEstimate(flops=10**10, bytes_accessed=10**7, transcendentals=0),
    )(
        *(
            pltpu.with_memory_space_constraint(array, pltpu.HBM)
            for array in inputs
        )
    )


def convolve(taps, extended, at, lanes, low, rows):
    value = jnp.zeros((rows, lanes), jnp.float32)
    for tap in range(taps.shape[0]):
        value = value + taps[tap : tap + 1, at : at + lanes] * (
            extended[at // lanes, low + tap : low + tap + rows]
        )
    return value


def tail_part(
    experts, groups, mine, place, table, home, cotangent, saved, inverse, gain, weight,
    taps, every, extended, head, blocks, sums, *sems
):
    (row_send, row_recv, pair_send, pair_recv, far_send, far_recv, half_send, half_recv,
     sum_send, sum_recv, halo_send, halo_recv) = sems
    chips = groups // 2
    chip, core = place // 2, place % 2
    sibling = chip * 2 + 1 - core
    tok = saved.shape[0]
    channels = saved.shape[1]
    width = blocks.shape[-1]
    per = experts // groups
    half = tok // 2

    def at_chip(step):
        return ((chip + step) % chips) * 2 + core

    def share_at(owner):
        return blocks.at[pl.ds(owner * per, per)]

    def row(hop):
        return remote(share_at(place), share_at(place), row_send.at[hop], row_recv.at[hop],
                      (mine, at_chip(hop)))

    def pair(hop):
        owner = at_chip(chips - hop)
        return remote(share_at(owner), share_at(owner), pair_send.at[hop], pair_recv.at[hop],
                      (mine, sibling))

    share = lax.dot_general(
        table[...].reshape(-1, tok), home[...].reshape(-1, home.shape[-1]), CONTRACT_FIRST, preferred_element_type=jnp.float32
    )
    share = (share + cotangent.astype(jnp.float32)).astype(jnp.bfloat16)
    for part in range(per):
        piece = share[:, part * width : (part + 1) * width]
        blocks[place * per + part] = piece.reshape(2, half, width)
    def far(step):
        peer = mate(mine, step, experts)
        return remote(blocks.at[peer, core], every.at[step, core], far_send.at[step],
                      far_recv.at[step], (peer, place))

    def to_half(step):
        return remote(every.at[step, core], every.at[step, core],
                      half_send.at[step], half_recv.at[step], (mine, sibling))

    def send_share(owner):
        for part in range(per):
            peer = owner * per + part

            @pl.when(peer != mine)
            def _(peer=peer):
                far(mate(mine, peer, experts)).start()

    def product(owner):
        side = weight[:, pl.ds(pl.multiple_of(owner * per * width, per * width), per * width)]
        value = None
        for part in range(per):
            term = lax.dot_general(
                blocks[owner * per + part].reshape(tok, width),
                side[:, part * width : (part + 1) * width],
                CONTRACT_LAST,
                preferred_element_type=jnp.float32,
            )
            value = term if value is None else value + term
        return value

    for hop in range(1, chips):
        row(hop).start()
    pair(0).start()
    send_share(place)
    grad = product(place)
    pair(0).wait_recv()
    send_share(sibling)
    grad = grad + product(sibling)
    for hop in range(1, chips):
        row(hop).wait_recv()
        pair(hop).start()
        send_share(at_chip(chips - hop))
        grad = grad + product(at_chip(chips - hop))
    for hop in range(1, chips):
        pair(hop).wait_recv()
        other = ((chip + chips - hop) % chips) * 2 + 1 - core
        send_share(other)
        grad = grad + product(other)
    every[0] = blocks[mine]
    normalized = saved[...].astype(jnp.float32)
    scaled = normalized * gain[...]
    gate = sigmoid(scaled)
    grad = grad * gate * (1.0 + scaled * (1.0 - gate)) * gain[...]
    lanes = min(channels, 128)
    first = jnp.zeros((tok, lanes), jnp.float32)
    second = jnp.zeros((tok, lanes), jnp.float32)
    for at in range(0, channels, lanes):
        first = first + grad[:, at : at + lanes]
        second = second + grad[:, at : at + lanes] * normalized[:, at : at + lanes]
    sums[place, 0] = jnp.sum(jnp.transpose(first).reshape(lanes // 8, 8, tok), axis=0)
    sums[place, 1] = jnp.sum(jnp.transpose(second).reshape(lanes // 8, 8, tok), axis=0)

    def tell(step):
        return remote(sums.at[place], sums.at[place], sum_send.at[step], sum_recv.at[step],
                      (mine, (place + step) % groups))

    def start_tell(step, carry):
        tell(step).start()
        return carry

    def wait_tell(step, carry):
        tell(step).wait()
        return carry

    lax.fori_loop(1, groups, start_tell, 0)
    lax.fori_loop(1, groups, wait_tell, 0)
    count = channels * groups
    total = jnp.sum(sums[...], axis=0)

    def column(kind):
        flat = jnp.sum(total[kind], axis=0, keepdims=True) / count
        return jnp.transpose(jnp.broadcast_to(flat, (lanes, tok)))

    mean, slope = column(0), column(1)
    deviation = jnp.transpose(jnp.broadcast_to(inverse[...], (lanes, tok)))
    for at in range(0, channels, lanes):
        extended[at // lanes, 0:tok] = deviation * (
            grad[:, at : at + lanes] - mean - normalized[:, at : at + lanes] * slope
        )
    reach = extended.shape[1] - tok

    def halo():
        return remote(extended.at[:, pl.ds(0, reach)], extended.at[:, pl.ds(tok, reach)],
                      halo_send, halo_recv, ((mine + experts - 1) % experts, place))

    @pl.when(mine > 0)
    def _():
        halo().start()

    @pl.when(mine == experts - 1)
    def _():
        extended[:, tok : tok + reach] = jnp.zeros((channels // lanes, reach, lanes), jnp.float32)

    def forward(step, carry):
        far(step).wait_recv()
        to_half(step).start()
        return carry

    lax.fori_loop(1, experts, forward, 0)
    for at in range(0, channels, lanes):
        head[:, at : at + lanes] = convolve(
            taps, extended, at, lanes, 0, head.shape[0]
        ).astype(head.dtype)

    @pl.when(mine < experts - 1)
    def _():
        halo().wait_recv()

    def arrive(step, carry):
        to_half(step).wait_recv()
        return carry

    lax.fori_loop(1, experts, arrive, 0)
    @pl.when(mine > 0)
    def _():
        halo().wait_send()

    for hop in range(chips):
        pair(hop).wait_send()
        if hop:
            row(hop).wait_send()

    def finish(step, carry):
        far(step).wait_send()
        to_half(step).wait_send()
        return carry

    lax.fori_loop(1, experts, finish, 0)


def last_kernel(
    lead, every, acts, crossed, extended, head, taps, gate, up, down, result_far, proj_far, gate_far, up_far, down_far,
    result, proj, sems
):
    stores = [
        pltpu.make_async_copy(source, target, sems.at[at])
        for at, (source, target) in enumerate(
            (
                (gate, gate_far), (up, up_far), (down, down_far), (result, result_far.at[pl.ds(head.shape[0], result.shape[0])]),
                (proj, proj_far), (head, result_far.at[pl.ds(0, head.shape[0])]),
            )
        )
    ]
    for store in stores[:3]:
        store.start()
    stores[5].start()
    rows, channels = result.shape
    lanes = extended.shape[-1]
    for at in range(0, channels, lanes):
        value = convolve(taps, extended, at, lanes, head.shape[0], rows)
        result[:, at : at + lanes] = value.astype(result.dtype)
    stores[3].start()
    def product(hop, right):
        return lax.dot_general(
            every[:, hop].reshape(-1, every.shape[-1]),
            right.reshape(-1, channels),
            CONTRACT_FIRST,
            preferred_element_type=jnp.float32,
        )

    value = product(0, acts[...])
    for hop in range(1, lead):
        value = value + product(hop, crossed[hop - 1])
    proj[...] = value
    stores[4].start()
    for store in stores:
        store.wait()


def last_blocks(every, acts, crossed, extended, head, taps, gate, up, down):
    across, tok, channels = acts.shape
    lead = every.shape[0] // across
    every = every.reshape((across, lead) + every.shape[1:])
    vmem = pl.BlockSpec(memory_space=pltpu.VMEM)
    shapes = (
        jax.ShapeDtypeStruct((tok, channels), jnp.bfloat16),
        jax.ShapeDtypeStruct((every.shape[-1], channels), jnp.float32),
    )
    return pl.pallas_call(
        functools.partial(last_kernel, lead),
        out_shape=shapes
        + tuple(jax.ShapeDtypeStruct(array.shape, array.dtype) for array in (gate, up, down)),
        in_specs=[vmem] * 9,
        out_specs=[pl.BlockSpec(memory_space=pltpu.HBM)] * 5,
        scratch_shapes=[
            pltpu.VMEM((tok - head.shape[0], channels), jnp.bfloat16),
            pltpu.VMEM(shapes[1].shape, jnp.float32),
        ]
        + [pltpu.SemaphoreType.DMA((6,))],
        compiler_params=pltpu.CompilerParams(vmem_limit_bytes=16 * 2**20),
        cost_estimate=pl.CostEstimate(flops=10**9, bytes_accessed=10**7, transcendentals=0),
    )(every, acts, crossed, extended, head, taps, gate, up, down)


def shards(
    cotangent,
    mixer_out,
    expert_ids,
    route_weight,
    saved_normalized,
    inverse_deviation,
    channel_norm_gain,
    taps,
    proj_weight,
    gate_weight,
    up_weight,
    down_weight,
):
    experts = lax.axis_size("sp")
    groups = lax.axis_size("tp")
    grad_first, grad_third, grad_second, acts, crossed, every, extended, head = expert_blocks(
        jnp.transpose(expert_ids),
        jnp.transpose(route_weight),
        mixer_out,
        cotangent,
        gate_weight[0],
        up_weight[0],
        down_weight[0],
        saved_normalized,
        channel_norm_gain[None, :],
        proj_weight,
        inverse_deviation[None, :],
        taps,
        experts,
        groups,
    )
    result, grad_proj, grad_first, grad_third, grad_second = last_blocks(
        every, acts, crossed, extended, head, taps, grad_first, grad_third, grad_second
    )
    return (
        result,
        grad_proj,
        grad_first[None],
        grad_third[None],
        grad_second[None],
    )


def solution(mesh):
    return jax.shard_map(
        shards,
        mesh=mesh,
        in_specs=(
            P("sp", None),
            P("sp", None),
            P("sp", None),
            P("sp", None),
            P("sp", "tp"),
            P("sp"),
            P("tp"),
            P(None, "tp"),
            P("tp", None),
            P("sp", None, "tp"),
            P("sp", None, "tp"),
            P("sp", "tp", None),
        ),
        out_specs=(
            P("sp", "tp"),
            P("sp", "tp"),
            P("sp", None, "tp"),
            P("sp", None, "tp"),
            P("sp", "tp", None),
        ),
        check_vma=False,
    )
```
